32 devices in a mesh: grp: 2 (over y), sp: 4 (over z), tp: 4 (over x, core).
Axes of the slice: x: 2, y: 2, z: 4, core: 2. Of those that a mesh axis runs over, the one named last changes fastest.
Arguments:
- residual: bfloat16 [2048, 2048], P(('grp', 'sp')), parts along dimension 0, may hold values from -34 to 34
- queries: bfloat16 [2048, 1024], P(('grp', 'sp'), 'tp'), parts along dimension 0, may hold values from -400 to 400
- keys: bfloat16 [2048, 512], P(('grp', 'sp'), 'tp'), parts along dimension 0, may hold values from -8 to 8
- values: bfloat16 [2048, 512], P(('grp', 'sp'), 'tp'), parts along dimension 0, may hold values from -6 to 6
- segments: int32 [2048], P(('grp', 'sp')), parts along dimension 0, may hold values from 0 to 2, never falling along the last dimension, each value on 1 to 768 neighbouring positions
- routes: int32 [2048, 2], P(('grp', 'sp')), parts along dimension 0, may hold values from 0 to 3, all different within a row; in each aligned block of 256 rows (0 to 255, 256 to 511, ...) at most 256 rows name the same one
- route_weight: float32 [2048, 2], P(('grp', 'sp')), parts along dimension 0, may hold values from 0.3 to 3
- sinks: float32 [16], P('tp'), may hold values from 1 to 6
- out_weight: bfloat16 [1024, 2048], P('tp'), may hold values from -1 to 1
- norm_gain: float32 [2048], replicated, may hold values from 0.1 to 1.9
- expert_gate: bfloat16 [4, 2048, 1024], P('sp', None, 'tp'), may hold values from -0.125 to 0.125
- expert_up: bfloat16 [4, 2048, 1024], P('sp', None, 'tp'), may hold values from -0.125 to 0.125
- expert_down: bfloat16 [4, 1024, 2048], P('sp', None, 'tp'), may hold values from -0.1875 to 0.1875
- shared_gate: bfloat16 [2048, 1024], P(None, 'tp'), may hold values from -0.125 to 0.125
- shared_up: bfloat16 [2048, 1024], P(None, 'tp'), may hold values from -0.125 to 0.125
- shared_down: bfloat16 [1024, 2048], P(None, 'tp'), may hold values from -0.1875 to 0.1875
Outputs:
- mixed: bfloat16 [2048, 2048], P(('grp', 'sp'), 'tp'), parts along dimension 0
The draws below stay inside these ranges and needn't reach their ends.
There are 2 independent parts, one for each index of `grp`. The reference program is written for one: setup_inputs(seed, part) draws one part's arguments, and reference() takes and returns one part's arrays. A program takes and returns all parts, laid end to end along the dimension named above; an argument that names none is the same for every part. Nothing has to cross between parts.
Inputs may be any that keep to these rules, and one draw needn't show every extreme that they name: `routes`: each row names 2 different experts. In the rows of one device no expert is named by more than 256 rows, and in some device's rows an expert is named by exactly 256. `segments`: document numbers never fall along the positions; every document spans 1 to 768 positions and one spans exactly 768.
All inputs are finite; a program needn't handle non-finite values.
Results may differ from the reference program's by a relative error of at most 0.0065.
Values may be sent and summed in bfloat16 or wider, within the bound.
A program may use at most 64 MiB of HBM per device.

```python
import math
import jax
import jax.numpy as jnp
import numpy as np
from jax import lax

D = 2048
HEADS = 16
KV_HEADS = 8
HEAD_DIM = 64
WINDOW = 128
EFF = 1024
SFF = 1024
TOPK = 2
TOK = 256
TOKENS = 1024
EXPERTS = 4
CAP = 256
DOCS = 3
LONGEST = 768
N_SP = 4


def query_key_pair(key):
    query_seed = jax.random.fold_in(key, 101)
    key_seed = jax.random.fold_in(key, 202)
    queries = jnp.clip(jax.random.normal(query_seed, (TOKENS, HEADS * HEAD_DIM), jnp.float32), -6.0, 6.0)
    key_rows = jnp.clip(jax.random.normal(key_seed, (TOKENS, KV_HEADS * HEAD_DIM), jnp.float32), -6.0, 6.0)
    return (queries, key_rows)


def draw_queries(key, part):
    queries, key_rows = query_key_pair(key)
    return queries.astype(jnp.bfloat16)


def draw_keys(key, part):
    queries, key_rows = query_key_pair(key)
    return key_rows.astype(jnp.bfloat16)


def draw_residual(key, part):
    profile = jnp.exp(math.log(4.0) * jnp.arange(D, dtype=jnp.float32) / D)
    jitter = jnp.exp(jax.random.uniform(jax.random.fold_in(key, 11), (D,), jnp.float32, math.log(0.7), math.log(1.4)))
    base = jnp.clip(jax.random.normal(jax.random.fold_in(key, 14), (TOKENS, D), jnp.float32), -6.0, 6.0)
    return (base * profile * jitter).astype(jnp.bfloat16)


def level_of(own_key, shape, pieces, low, high):
    def one(dim, parts):
        heights = jax.random.uniform(jax.random.fold_in(jax.random.fold_in(own_key, 6), dim), (parts,), jnp.float32, low / len(pieces), high / len(pieces))
        return jnp.repeat(jnp.exp(heights), shape[dim] // parts).reshape((-1,) + (1,) * (len(shape) - dim - 1))

    factor_of = one(*pieces[0])
    for cut in pieces[1:]:
        factor_of = factor_of * one(*cut)
    return factor_of


def length_profile(amount, total, limit, skew):
    portions = [(1 << 20) // math.isqrt(grade ** skew) + 1 for grade in range(2, amount + 1)]
    rest, counts = total - limit - (amount - 1), [1] * (amount - 1)
    while rest > 0:
        movable = [i for i in range(amount - 1) if counts[i] < limit]
        whole, left = sum([portions[i] for i in movable]), rest
        for i in movable:
            addition = min(limit - counts[i], max(1, left * portions[i] // whole), rest)
            counts[i] = counts[i] + addition
            rest = rest - addition
    return np.array([limit] + counts)


def ragged(stream_key, count, total, reach, slope):
    if count == 2:
        one = jax.random.randint(stream_key, (), max(1, total - reach), min(reach, total - 1) + 1)
        return jnp.stack([one, total - one])
    sizes = jnp.asarray(length_profile(count, total, reach, slope), jnp.int32)
    twos = (count - 1) // 2
    source_of, taker = sizes[1:1 + 2 * twos:2], sizes[2:2 + 2 * twos:2]
    room = jnp.minimum(source_of - 1, reach - taker)
    passed = jax.random.randint(jax.random.fold_in(stream_key, 1), (twos,), 0, 1 << 20) % (room + 1)
    sizes = sizes.at[1:1 + 2 * twos:2].set(source_of - passed).at[2:2 + 2 * twos:2].set(taker + passed)
    return sizes[jax.random.permutation(jax.random.fold_in(stream_key, 2), count)]


def deal_out(key, own, number, rows, count, top, reach, lean):
    order = jax.random.permutation(key, count)
    heavy_load, usual = shares(count, rows * top, reach, lean, True), shares(count, rows * top, reach, lean, False)
    places = jnp.arange(count)

    def named(tallies, turn):
        used = int((tallies > 0).sum())
        fixed = max(1, used // 4)
        shifted = fixed + (places - fixed + turn * (used - fixed)) % max(1, count - fixed)
        return jnp.zeros((count,), jnp.int32).at[order[jnp.where(places < fixed, places, shifted)]].set(jnp.asarray(tallies, jnp.int32))

    tallies = jnp.where(number % 4 == 0, named(heavy_load, number // 4), named(usual, number - number // 4 - 1))
    mixed = jax.random.permutation(jax.random.fold_in(own, 3), count)
    source_of, taker = mixed[0:count // 2 * 2:2], mixed[1:count // 2 * 2:2]
    margin = jnp.minimum(tallies[source_of] - 1, reach - tallies[taker]) // 2
    margin = jnp.where((source_of == order[0]) | (taker == order[0]) | (tallies[taker] == 0), 0, jnp.maximum(margin, 0))
    shifted = jax.random.randint(jax.random.fold_in(own, 4), (count // 2,), 0, 1 << 20) % (margin + 1)
    tallies = tallies.at[source_of].add(-shifted).at[taker].add(shifted)
    members = jnp.searchsorted(jnp.cumsum(tallies), jnp.arange(rows * top), side="right").astype(jnp.int32)
    listing = members.reshape(top, rows).T
    listing = listing[jax.random.permutation(jax.random.fold_in(own, 1), rows)]
    turn = jax.random.randint(jax.random.fold_in(own, 2), (rows, 1), 0, top)
    return jnp.take_along_axis(listing, (jnp.arange(top)[None, :] + turn) % top, axis=1)


def shares(number_of, total, limit, skew, full):
    loads = [(1 << 20) // math.isqrt(grade ** skew) + 1 for grade in range(1, number_of + 1)]
    largest = limit if full else min(limit, max(-(-total // number_of), total * loads[0] // sum(loads)))
    least = 1 if total - largest >= number_of - 1 else 0
    counts, surplus = [largest] + [least] * (number_of - 1), total - largest - least * (number_of - 1)
    while surplus > 0:
        free = [i for i in range(1, number_of) if counts[i] < largest] or [i for i in range(1, number_of) if counts[i] < limit]
        mass, remaining = sum([loads[i] for i in free]), surplus
        for i in free:
            more = min(limit - counts[i], max(1, remaining * loads[i] // mass), surplus)
            counts[i] = counts[i] + more
            surplus = surplus - more
    return np.array(counts)


def centred(rng, extent, deviation, most, pieces=(), kind=jnp.bfloat16):
    array = jax.random.normal(rng, extent, jnp.float32) * deviation
    if len(pieces) > 0:
        array = level_of(rng, extent, pieces, -0.22, 0.18) * array
    return jnp.clip(array, min=-most, max=most).astype(kind)


def setup_inputs(seed: int = 0, part: int = 0) -> dict:
    key_of = jax.random.split(jax.random.key(seed), 17)
    part_keys = jax.random.split(jax.random.fold_in(key_of[16], part), 17)
    residual = draw_residual(jax.random.fold_in(jax.random.fold_in(key_of[16], part), 71), part)
    queries = draw_queries(jax.random.fold_in(jax.random.fold_in(key_of[16], part), 71), part)
    keys = draw_keys(jax.random.fold_in(jax.random.fold_in(key_of[16], part), 71), part)
    values = centred(part_keys[3], (TOKENS, KV_HEADS * HEAD_DIM), 1.0, 6.0, ((0, 4), (1, 4)))
    segments = jnp.searchsorted(jnp.cumsum(ragged(part_keys[4], DOCS, TOKENS, LONGEST, 2)), jnp.arange(TOKENS), side="right").astype(jnp.int32)
    routes_keys = jax.random.split(jax.random.fold_in(part_keys[5], 1), TOKENS // TOK)
    routes_turns = jax.random.permutation(jax.random.fold_in(part_keys[5], 3), TOKENS // TOK)
    routes = jax.vmap(lambda own, number: deal_out(jax.random.fold_in(part_keys[5], 2), own, number, TOK, EXPERTS, TOPK, CAP, 1))(routes_keys, routes_turns).reshape((TOKENS, TOPK))
    route_weight = jnp.clip(jnp.exp(math.log(3.0) - 2.3025851 * jax.random.uniform(part_keys[6], (TOKENS, TOPK), jnp.float32) ** level_of(part_keys[6], (TOKENS, TOPK), ((0, 4),), -0.2, 0.2)), 0.3, 3.0)
    sinks = jnp.clip(1.0 + 5.0 * jax.random.uniform(key_of[7], (HEADS,), jnp.float32) ** level_of(key_of[7], (HEADS,), ((0, 4),), -0.2, 0.2), 1.0, 6.0)
    out_weight = centred(key_of[8], (HEADS * HEAD_DIM, D), (HEADS * HEAD_DIM // 32) ** -0.5, 1.0, ((0, 4),))
    norm_gain = jnp.clip(1.0 + 0.18 * jax.random.normal(key_of[9], (D,), jnp.float32), 0.1, 1.9)
    expert_gate = centred(key_of[10], (EXPERTS, D, EFF), D ** -0.5, 0.125, ((0, 4), (2, 4)))
    expert_up = centred(key_of[11], (EXPERTS, D, EFF), D ** -0.5, 0.125, ((0, 4), (2, 4)))
    expert_down = centred(key_of[12], (EXPERTS, EFF, D), EFF ** -0.5, 0.1875, ((0, 4), (2, 4)))
    shared_gate = centred(key_of[13], (D, SFF), D ** -0.5, 0.125, ((1, 4),))
    shared_up = centred(key_of[14], (D, SFF), D ** -0.5, 0.125, ((1, 4),))
    shared_down = centred(key_of[15], (SFF, D), SFF ** -0.5, 0.1875, ((1, 4),))
    return {"residual": residual, "queries": queries, "keys": keys, "values": values, "segments": segments, "routes": routes, "route_weight": route_weight, "sinks": sinks, "out_weight": out_weight, "norm_gain": norm_gain, "expert_gate": expert_gate, "expert_up": expert_up, "expert_down": expert_down, "shared_gate": shared_gate, "shared_up": shared_up, "shared_down": shared_down}


epsilon = 1e-06

def banded(rows, fill):
    blocks = rows.shape[0] // WINDOW
    shaped = rows.reshape((blocks, WINDOW) + rows.shape[1:])
    before = jnp.concatenate([jnp.full_like(shaped[:1], fill), shaped[:-1]], axis=0)
    return jnp.concatenate([before, shaped], axis=1)

def attend(queries, keys, values, segments, sinks):
    blocks = TOKENS // WINDOW
    group_size = HEADS // KV_HEADS
    query_blocks = queries.astype(jnp.float32).reshape(blocks, WINDOW, KV_HEADS, group_size, HEAD_DIM)
    key_band = banded(keys, 0).astype(jnp.float32).reshape(blocks, 2 * WINDOW, KV_HEADS, HEAD_DIM)
    value_band = banded(values, 0).astype(jnp.float32).reshape(blocks, 2 * WINDOW, KV_HEADS, HEAD_DIM)
    segment_band = banded(segments, -1)
    query_segments = segments.reshape(blocks, WINDOW)
    scores = jnp.einsum('nqhgd,nkhd->nhgqk', query_blocks, key_band) * HEAD_DIM ** (-0.5)
    offsets = jnp.arange(WINDOW)[:, None] + WINDOW - jnp.arange(2 * WINDOW)[None, :]
    allowed = (offsets >= 0) & (offsets < WINDOW) & (query_segments[:, :, None] == segment_band[:, None, :])
    sink_logits = sinks.astype(jnp.float32).reshape(KV_HEADS, group_size)[None, :, :, None]
    masked = jnp.where(allowed[:, None, None], scores, -jnp.inf)
    top_score = jnp.maximum(lax.optimization_barrier(jnp.max(masked, axis=-1)), sink_logits)
    exp_terms = jnp.where(allowed[:, None, None], jnp.exp(scores - top_score[..., None]), 0.0)
    denominator = lax.optimization_barrier(jnp.sum(exp_terms, axis=-1)) + jnp.exp(sink_logits - top_score)
    probabilities = (exp_terms / denominator[..., None]).astype(jnp.bfloat16)
    attended = jnp.einsum('nhgqk,nkhd->nqhgd', probabilities.astype(jnp.float32), value_band)
    return attended.astype(jnp.bfloat16).reshape(TOKENS, HEADS * HEAD_DIM)

def block_slots(block_routes):
    flat_ids = block_routes.reshape(-1)
    one_hot = (flat_ids[:, None] == jnp.arange(EXPERTS, dtype=jnp.int32)[None, :]).astype(jnp.int32)
    rank_in = jnp.cumsum(one_hot, axis=0) - one_hot
    return flat_ids * CAP + lax.optimization_barrier(jnp.sum(rank_in * one_hot, axis=1))

def reference(residual, queries, keys, values, segments, routes, route_weight, sinks, out_weight, norm_gain, expert_gate, expert_up, expert_down, shared_gate, shared_up, shared_down):
    attended = attend(queries, keys, values, segments, sinks)
    projected = jnp.dot(attended, out_weight, preferred_element_type=jnp.float32)
    updated = (residual.astype(jnp.float32) + projected).astype(jnp.bfloat16)
    updated_f32 = updated.astype(jnp.float32)
    inv_rms = lax.rsqrt(lax.optimization_barrier(jnp.mean(updated_f32 * updated_f32, axis=-1, keepdims=True)) + epsilon)
    normed = (updated_f32 * inv_rms * norm_gain).astype(jnp.bfloat16)
    shared_pre = jnp.dot(normed, shared_gate, preferred_element_type=jnp.float32)
    shared_lin = jnp.dot(normed, shared_up, preferred_element_type=jnp.float32)
    shared_act = (jax.nn.silu(shared_pre) * shared_lin).astype(jnp.bfloat16)
    shared_out = jnp.dot(shared_act, shared_down, preferred_element_type=jnp.float32)
    slot_dest = jax.vmap(block_slots)(routes.reshape(N_SP, TOK, TOPK))
    block_ids = jnp.broadcast_to(jnp.arange(N_SP, dtype=jnp.int32)[:, None], slot_dest.shape)
    token_ids = block_ids * TOK + (jnp.arange(TOK * TOPK, dtype=jnp.int32) // TOPK)[None, :]
    slot_token = jnp.full((N_SP, EXPERTS * CAP), -1, jnp.int32).at[block_ids, slot_dest].set(token_ids)
    slot_weight = jnp.zeros((N_SP, EXPERTS * CAP), jnp.float32).at[block_ids, slot_dest].set(route_weight.reshape(N_SP, TOK * TOPK))
    per_token = slot_token.reshape(N_SP, EXPERTS, CAP).transpose(1, 0, 2).reshape(EXPERTS, N_SP * CAP)
    per_weight = slot_weight.reshape(N_SP, EXPERTS, CAP).transpose(1, 0, 2).reshape(EXPERTS, N_SP * CAP)

    def one_expert(accum, inputs):
        gate_mat, up_mat, down_mat, token_list, weight_list = inputs
        filled = token_list >= 0
        safe_token = jnp.where(filled, token_list, 0).astype(jnp.int32)
        rows_in = jnp.where(filled[:, None], normed[safe_token], jnp.zeros((), jnp.bfloat16))
        gate_pre = jnp.dot(rows_in, gate_mat, preferred_element_type=jnp.float32)
        up_lin = jnp.dot(rows_in, up_mat, preferred_element_type=jnp.float32)
        expert_act = (jax.nn.silu(gate_pre) * up_lin).astype(jnp.bfloat16)
        expert_out = jnp.dot(expert_act, down_mat, preferred_element_type=jnp.float32).astype(jnp.bfloat16)
        accum = accum.at[safe_token].add(expert_out.astype(jnp.float32) * weight_list[:, None])
        return (accum, None)
    routed, _ = lax.scan(one_expert, jnp.zeros((TOKENS, D), jnp.float32), (expert_gate, expert_up, expert_down, per_token, per_weight))
    return (updated_f32 + shared_out + routed).astype(jnp.bfloat16)
```

```python
import functools
import jax
import jax.numpy as jnp
from jax import lax
from jax.experimental import pallas as pl
from jax.experimental.pallas import tpu as pltpu
from jax.sharding import PartitionSpec as P

HEAD_DIM = 64
WINDOW = 128


epsilon = 1e-06


def passed_along(value, axis, steps):
    count = lax.axis_size(axis)
    leading, last = (max(0, -steps), min(count, count - steps))
    return lax.ppermute(value, axis, [(source, source + steps) for source in range(leading, last)])


def banded(prev_rows, own_rows, window_len):
    blocks = own_rows.shape[0] // window_len
    joined = jnp.concatenate([prev_rows, own_rows], axis=0)
    shaped = joined.reshape((blocks + 1, window_len) + own_rows.shape[1:])
    return jnp.concatenate([shaped[:-1], shaped[1:]], axis=1)


def shards(
    residual,
    queries,
    keys,
    values,
    segments,
    routes,
    route_weight,
    sinks,
    out_weight,
    norm_gain,
    expert_gate,
    expert_up,
    expert_down,
    shared_gate,
    shared_up,
    shared_down,
):
    rows_here = residual.shape[0]
    model_width = residual.shape[1]
    tp_count = lax.axis_size("tp")
    tp_index = lax.axis_index("tp")
    head_local = queries.shape[1] // HEAD_DIM
    kv_local = keys.shape[1] // HEAD_DIM
    group_size = head_local // kv_local
    window_len = WINDOW
    blocks = rows_here // window_len
    own_marks = (segments % 256 + 1).astype(jnp.bfloat16)
    prev_keys, prev_values, prev_marks = passed_along(
        (
            keys[rows_here - window_len :],
            values[rows_here - window_len :],
            own_marks[rows_here - window_len :],
        ),
        "sp",
        1,
    )
    key_band = banded(prev_keys, keys, window_len).reshape(
        blocks, 2 * window_len, kv_local, HEAD_DIM
    )
    value_band = banded(prev_values, values, window_len).reshape(
        blocks, 2 * window_len, kv_local, HEAD_DIM
    )
    mark_band = banded(prev_marks, own_marks, window_len).astype(jnp.float32)
    query_marks = own_marks.reshape(blocks, window_len).astype(jnp.float32)
    query_blocks = queries.reshape(blocks, window_len, kv_local, group_size, HEAD_DIM)
    scores = jnp.einsum(
        "nqhgd,nkhd->nhgqk", query_blocks, key_band, preferred_element_type=jnp.float32
    ) * HEAD_DIM ** (-0.5)
    offsets = jnp.arange(window_len)[:, None] + window_len - jnp.arange(2 * window_len)[None, :]
    allowed = (
        (offsets >= 0) & (offsets < window_len) & (query_marks[:, :, None] == mark_band[:, None, :])
    )
    sink_logits = sinks.reshape(kv_local, group_size)[None, :, :, None]
    masked = jnp.where(allowed[:, None, None], scores, -jnp.inf)
    top_score = jnp.maximum(jnp.max(masked, axis=-1), sink_logits)
    exp_terms = jnp.where(allowed[:, None, None], jnp.exp(scores - top_score[..., None]), 0.0)
    denominator = jnp.sum(exp_terms, axis=-1) + jnp.exp(sink_logits - top_score)
    probabilities = (exp_terms / denominator[..., None]).astype(jnp.bfloat16)
    attended = jnp.einsum(
        "nhgqk,nkhd->nqhgd", probabilities, value_band, preferred_element_type=jnp.float32
    )
    attended = attended.astype(jnp.bfloat16).reshape(rows_here, head_local * HEAD_DIM)
    partial_value = jnp.dot(attended, out_weight, preferred_element_type=jnp.float32)
    col_width = model_width // tp_count
    col_start = tp_index * col_width
    summed = lax.psum(partial_value, "tp")
    updated = (residual.astype(jnp.float32) + summed).astype(jnp.bfloat16)
    updated_f32 = updated.astype(jnp.float32)
    inv_rms = lax.rsqrt(jnp.mean(updated_f32 * updated_f32, axis=-1, keepdims=True) + epsilon)
    normed = (updated_f32 * inv_rms * norm_gain).astype(jnp.bfloat16)
    updated_cols = lax.dynamic_slice_in_dim(updated, col_start, col_width, 1)
    normed_cols = lax.dynamic_slice_in_dim(normed, col_start, col_width, 1)
    shared_pre = jnp.dot(normed, shared_gate, preferred_element_type=jnp.float32)
    shared_lin = jnp.dot(normed, shared_up, preferred_element_type=jnp.float32)
    shared_act = (jax.nn.silu(shared_pre) * shared_lin).astype(jnp.bfloat16)
    top_count = routes.shape[1]
    experts = lax.axis_size("sp")
    capacity = 2 * rows_here * top_count // experts
    flat_ids = routes.reshape(-1)
    one_hot = (flat_ids[:, None] == jnp.arange(experts, dtype=jnp.int32)[None, :]).astype(jnp.int32)
    rank_in = jnp.cumsum(one_hot, axis=0) - one_hot
    slot_dest = flat_ids * capacity + jnp.sum(rank_in * one_hot, axis=1)
    token_of = jnp.arange(rows_here * top_count, dtype=jnp.int32) // top_count
    slot_token = jnp.full((experts * capacity,), -1, jnp.int32).at[slot_dest].set(token_of)
    filled = slot_token >= 0
    safe_token = jnp.where(filled, slot_token, 0)
    outgoing = jnp.where(filled[:, None], normed_cols[safe_token], jnp.zeros((), jnp.bfloat16))
    pieces = lax.all_to_all(
        outgoing.reshape(experts, capacity, col_width),
        "sp",
        split_axis=0,
        concat_axis=0,
        tiled=True,
    )
    arrived = lax.all_gather(pieces, "tp", axis=2, tiled=True)
    expert_rows = arrived.reshape(-1, model_width)
    gate_pre = jnp.dot(expert_rows, expert_gate[0], preferred_element_type=jnp.float32)
    up_lin = jnp.dot(expert_rows, expert_up[0], preferred_element_type=jnp.float32)
    expert_act = (jax.nn.silu(gate_pre) * up_lin).astype(jnp.bfloat16)
    gathered_expert, gathered_shared = (
        lax.all_gather(expert_act, "tp", axis=1, tiled=True),
        lax.all_gather(shared_act, "tp", axis=1, tiled=True),
    )
    expert_out = jnp.dot(
        gathered_expert, expert_down[0], preferred_element_type=jnp.float32
    ).astype(jnp.bfloat16)
    returned = lax.all_to_all(
        expert_out.reshape(experts, capacity, col_width),
        "sp",
        split_axis=0,
        concat_axis=0,
        tiled=True,
    )
    returned = returned.reshape(experts * capacity, col_width)
    picked = returned[slot_dest].astype(jnp.float32).reshape(rows_here, top_count, col_width)
    routed = jnp.sum(picked * route_weight[:, :, None], axis=1)
    shared_cols = jnp.dot(gathered_shared, shared_down, preferred_element_type=jnp.float32)
    return (updated_cols.astype(jnp.float32) + shared_cols + routed).astype(jnp.bfloat16)


MESH = pl.DeviceIdType.MESH
PARTS = 4
ALONG = (0, 2)
OWN = (0, 1)
STEPS = (
    ("attend", 1),
    ("loaded", "res"),
    ("enter",),
    ("chip", 1),
    ("across", 1),
    ("hold", 1),
    ("halo",),
    ("attend", 0),
    ("publish", 2),
    ("send", "e", 0, 2, 0),
    ("weights", "m", 0),
    ("send", "m", 1, 2, 0),
    ("chip", 0),
    ("across", 0),
    ("rest",),
    ("publish", 3),
    ("weights", "m", 2),
    ("send", "m", 1, 3, 0),
    ("send", "m", 0, 3, 0),
    ("take", "m", 0, 2, 0),
    ("send", "e", 0, 3, 0),
    ("hold", 0),
    ("own_over", 2),
    ("send", "e", 0, 2, 1),
    ("send", "m", 1, 2, 1),
    ("take", "m", 0, 3, 0),
    ("loaded", "gain", "eg", "eu", "sg", "su", "ed", "sd"),
    ("publish", 0),
    ("send", "m", 0, 0, 0),
    ("take", "m", 2, 3, 0),
    ("send", "e", 0, 0, 0),
    ("publish", 1),
    ("send", "e", 0, 1, 0),
    ("weights", "e", 3),
    ("weights", "m", 3),
    ("send", "m", 0, 1, 0),
    ("take", "e", 2, 3, 0),
    ("take", "m", 0, 2, 1),
    ("send", "m", 1, 1, 0),
    ("take", "m", 3, 3, 0),
    ("take", "e", 1, 3, 0),
    ("take", "m", 0, 1, 0),
    ("take", "m", 0, 0, 0),
    ("take", "m", 0, 3, 1),
    ("own_over", 3),
    ("take", "m", 3, 2, 0),
    ("own_over", 0),
    ("send", "e", 0, 0, 1),
    ("take", "e", 3, 3, 0),
    ("take", "m", 2, 1, 0),
    ("take", "m", 3, 2, 1),
    ("take", "e", 1, 2, 1),
    ("compute_own", 1),
    ("take", "e", 1, 3, 1),
    ("own_over", 1),
    ("take", "e", 3, 2, 0),
    ("take", "e", 1, 2, 0),
    ("take", "m", 3, 1, 0),
    ("take", "m", 2, 0, 0),
    ("take", "m", 0, 0, 1),
    ("take", "m", 3, 3, 1),
    ("take", "e", 2, 1, 0),
    ("take", "e", 3, 1, 0),
    ("take", "e", 3, 3, 1),
    ("compute_own", 0),
    ("take", "m", 2, 3, 1),
    ("take", "e", 3, 2, 1),
    ("weights", "e", 2),
    ("send", "m", 0, 0, 1),
    ("take", "m", 3, 0, 0),
    ("send", "m", 0, 2, 0),
    ("compute", (3, 0), 1),
    ("take", "m", 3, 0, 1),
    ("take", "e", 2, 3, 1),
    ("take", "e", 3, 0, 0),
    ("relay", "b", 0, 1),
    ("send", "m", 0, 2, 1),
    ("take", "m", 2, 1, 1),
    ("take", "m", 2, 0, 1),
    ("weights", "e", 1),
    ("relay", "b", 1, 1),
    ("take", "m", 2, 2, 0),
    ("take", "m", 2, 2, 1),
    ("take", "e", 3, 1, 1),
    ("send", "m", 1, 0, 1),
    ("take", "e", 3, 0, 1),
    ("compute", (1, 3), 1),
    ("take", "e", 2, 0, 0),
    ("take", "e", 2, 0, 1),
    ("send", "m", 1, 0, 0),
    ("take", "e", 2, 1, 1),
    ("take", "m", 3, 1, 1),
    ("compute", (3, 3), 0),
    ("take", "e", 1, 1, 0),
    ("shared", 1),
    ("relay", "m", 3, 1),
    ("take", "m", 0, 1, 1),
    ("relay", "e", 3, 1),
    ("take", "e", 2, 2, 0),
    ("compute", (2, 2), 0),
    ("give", (3, 3), 1),
    ("own", 1),
    ("take", "e", 2, 2, 1),
    ("relay", "e", 3, 0),
    ("relay", "m", 0, 1),
    ("relay", "m", 3, 0),
    ("take", "e", 1, 0, 1),
    ("compute", (2, 2), 1),
    ("relay", "b", 0, 0),
    ("relay", "b", 1, 0),
    ("relay", "e", 1, 1),
    ("give", (3, 3), 0),
    ("take", "e", 1, 1, 1),
    ("relay", "m", 2, 0),
    ("take", "e", 1, 0, 0),
    ("relay", "e", 2, 0),
    ("compute", (1, 0), 0),
    ("give", (2, 2), 0),
    ("relay", "e", 2, 1),
    ("give", (2, 0), 1),
    ("relay", "m", 2, 1),
    ("shared", 0),
    ("own", 0),
    ("relay", "e", 1, 0),
    ("relay", "m", 0, 0),
    ("give", (1, 2), 1),
    ("give", (1, 0), 0),
    ("finish", 0),
    ("finish", 1),
)


def fused_kernel(
    dims,
    res_hbm,
    q_hbm,
    k_hbm,
    v_hbm,
    seg_hbm,
    routes_hbm,
    rw_hbm,
    sinks_ref,
    wo_hbm,
    gain_hbm,
    eg_hbm,
    eu_hbm,
    ed_hbm,
    sg_hbm,
    su_hbm,
    sd_hbm,
    out_ref,
    q_ref,
    k_ref,
    v_ref,
    seg_ref,
    routes_ref,
    rw_ref,
    gain_ref,
    res_v,
    wo_v,
    gu_v,
    sgu_v,
    dn_v,
    sdn_v,
    kh,
    vh,
    mh,
    marks_own,
    marks_v,
    wx,
    att,
    b1s,
    b1r,
    b2s,
    b2r,
    keep,
    upd,
    norm_v,
    act,
    ret,
    rin,
    acc,
    w_sem,
    halo_s,
    halo_r,
    x_s,
    x_r,
    b_s,
    b_r,
    c_s,
    c_r,
    u_s,
    u_r,
    a_s,
    a_r,
    e_s,
    e_r,
):
    rows, cols, width, window, hidden, heads, group = dims
    bf16, f32 = jnp.bfloat16, jnp.float32
    s = lax.axis_index("sp")
    t = lax.axis_index("tp")
    core = t % 2
    chip = t // 2
    mate = t + 1 - 2 * core
    over = t + 2 - 4 * chip
    diag = 3 - t
    side = s // 2
    middle = ((s + 1) // 2) % 2
    is_mid = middle == 1
    is_end = middle == 0
    inner = s + 1 - 2 * side
    outer = (s + 3 + 2 * side) % 4

    def index_of(block):
        end, mid = block
        b = end + middle * (mid - end)
        return b + side * (3 - 2 * b)

    def remote(src, dst, send, recv, sp, tp):
        return pltpu.make_async_remote_copy(
            src_ref=src,
            dst_ref=dst,
            send_sem=send,
            recv_sem=recv,
            device_id={"sp": sp, "tp": tp},
            device_id_type=MESH,
        )

    pending = []
    conditional = []

    def go(copy, when=None):
        if when is None:
            copy.start()
            pending.append(copy)
        else:

            @pl.when(when)
            def _():
                copy.start()

            conditional.append((when, copy))

    barrier = pltpu.get_barrier_semaphore()
    for sp, tp in ((s, mate), (s, over), (inner, t)):
        pl.semaphore_signal(barrier, inc=1, device_id={"sp": sp, "tp": tp}, device_id_type=MESH)

    @pl.when(is_mid)
    def _():
        pl.semaphore_signal(barrier, inc=1, device_id={"sp": outer, "tp": t}, device_id_type=MESH)

    own_cols = pl.ds(pl.multiple_of(t * cols, cols), cols)
    first_half = pl.ds(0, hidden)
    second_half = pl.ds(hidden, hidden)
    sources = dict(
        seg=(seg_hbm, seg_ref),
        k=(k_hbm, k_ref),
        q=(q_hbm, q_ref),
        v=(v_hbm, v_ref),
        routes=(routes_hbm, routes_ref),
        rw=(rw_hbm, rw_ref),
        wo=(wo_hbm, wo_v),
        res=(res_hbm.at[:, own_cols], res_v),
        gain=(gain_hbm, gain_ref),
        eg=(eg_hbm.at[0], gu_v.at[:, first_half]),
        eu=(eu_hbm.at[0], gu_v.at[:, second_half]),
        sg=(sg_hbm, sgu_v.at[:, first_half]),
        su=(su_hbm, sgu_v.at[:, second_half]),
        ed=(ed_hbm.at[0], dn_v),
        sd=(sd_hbm, sdn_v),
    )
    loads = {
        name: pltpu.make_async_copy(src, dst, w_sem.at[i])
        for i, (name, (src, dst)) in enumerate(sources.items())
    }
    early = ("seg", "k", "q", "v", "routes", "rw", "wo", "res", "gain")
    for name in early:
        loads[name].start()

    def loaded(*names):
        for name in names:
            loads[name].wait()

    tail = pl.ds(rows - window, window)
    up_sp = (s + 1) % 4
    halos = [
        remote(k_ref.at[tail], kh, halo_s.at[0], halo_r.at[0], up_sp, t),
        remote(v_ref.at[tail], vh, halo_s.at[1], halo_r.at[1], up_sp, t),
        remote(marks_v, mh, halo_s.at[2], halo_r.at[2], up_sp, t),
    ]

    @pl.when(s == 0)
    def _():
        kh[...] = jnp.zeros_like(kh)
        vh[...] = jnp.zeros_like(vh)
        mh[...] = jnp.full(mh.shape, -1.0, f32)

    loaded("seg")
    marks_own[...] = jnp.broadcast_to(seg_ref[...].astype(f32), marks_own.shape)
    marks_v[...] = marks_own[:, tail]

    def down_rows(row):
        return jnp.transpose(jnp.broadcast_to(row, (window, window)))

    q_pos = lax.broadcasted_iota(jnp.int32, (window, window), 0)
    k_pos = lax.broadcasted_iota(jnp.int32, (window, window), 1)

    def attend(n):
        here = pl.ds(n * window, window)
        if n == 0:
            k_prev, v_prev, m_prev = kh, vh, mh[0:1, :]
            before = slice(None)
        else:
            before = pl.ds((n - 1) * window, window)
            k_prev, v_prev, m_prev = k_ref, v_ref, marks_own[0:1, before]
        m_own = marks_own[0:1, here]
        marks = down_rows(m_own)
        ok_prev = (k_pos > q_pos) & (marks == m_prev)
        ok_own = (k_pos <= q_pos) & (marks == m_own)
        contract = (((1,), (1,)), ((), ()))
        every = range(heads)
        kv = [slice((h // group) * HEAD_DIM, (h // group + 1) * HEAD_DIM) for h in every]
        scores = []
        for h in every:
            qh = q_ref[here, h * HEAD_DIM : (h + 1) * HEAD_DIM]
            pair = [
                lax.dot_general(qh, k, contract, preferred_element_type=f32) * HEAD_DIM ** (-0.5)
                for k in (k_prev[before, kv[h]], k_ref[here, kv[h]])
            ]
            scores.append((jnp.where(ok_prev, pair[0], -jnp.inf), jnp.where(ok_own, pair[1], -jnp.inf)))
        tops = [
            jnp.maximum(jnp.max(jnp.maximum(*scores[h]), axis=-1, keepdims=True), sinks_ref[h])
            for h in every
        ]
        terms = [tuple(jnp.exp(score - tops[h]) for score in scores[h]) for h in every]
        totals = [
            jnp.sum(terms[h][0] + terms[h][1], axis=-1, keepdims=True)
            + jnp.exp(sinks_ref[h] - tops[h])
            for h in every
        ]
        for h in every:
            inverse = 1.0 / totals[h]
            p_prev, p_own = ((term * inverse).astype(bf16) for term in terms[h])
            got = jnp.dot(p_prev, v_prev[before, kv[h]], preferred_element_type=f32) + jnp.dot(
                p_own, v_ref[here, kv[h]], preferred_element_type=f32
            )
            att[here, h * HEAD_DIM : (h + 1) * HEAD_DIM] = got.astype(bf16)

    def project(n, chunk):
        where = pl.ds(pl.multiple_of(chunk * cols, cols), cols)
        return jnp.dot(
            att[pl.ds(n * window, window), :], wo_v[:, where], preferred_element_type=f32
        )

    part_rows = rows // PARTS
    per_half = window // part_rows

    def parts_of(n):
        return range(n * per_half, (n + 1) * per_half)

    def part_span(p):
        return pl.ds(p * part_rows, part_rows)

    first = {}
    second = {}

    def reduce_in_chip(n):
        for far in (1, 0):
            chunk = (over if far else t) + 1 - 2 * core
            b1s[n, far] = project(n, chunk).astype(bf16)
            copy = remote(
                b1s.at[n, far], b1r.at[n, far], b_s.at[n, far], b_r.at[n, far], s, mate
            )
            go(copy)
            first[n, far] = copy

    def reduce_across(n):
        mine = project(n, over)
        first[n, 1].wait_recv()
        mine = mine + b1r[n, 1].astype(f32)
        for i, p in enumerate(parts_of(n)):
            b2s[p] = mine[i * part_rows : (i + 1) * part_rows].astype(bf16)
            copy = remote(b2s.at[p], b2r.at[p], c_s.at[p], c_r.at[p], s, over)
            go(copy)
            second[p] = copy

    def hold(n):
        here = pl.ds(n * window, window)
        mine = project(n, t) + res_v[here, :].astype(f32)
        first[n, 0].wait_recv()
        keep[here, :] = mine + b1r[n, 0].astype(f32)

    def piece(b, chunk, p):
        return upd.at[b, chunk, part_span(p)]

    def share(kind, b, chunk, p, sp, tp):
        return remote(
            piece(b, chunk, p),
            piece(b, chunk, p),
            u_s.at[kind, b, p],
            u_r.at[b, chunk, p],
            sp,
            tp,
        )

    roles = dict(e=is_end, m=is_mid, b=None)

    def send_own(role, far, p, passed):
        chunk = over if passed else t
        go(share(far + 5 * passed, s, chunk, p, outer if far else inner, t), roles[role])

    def publish(p):
        second[p].wait_recv()
        upd[s, t, part_span(p), :] = (keep[part_span(p), :] + b2r[p].astype(f32)).astype(bf16)
        go(share(3, s, t, p, s, over))
        go(share(2, s, t, p, s, mate))

    def own_over(p):
        share(4, s, over, p, s, mate).wait_recv()
        go(share(4, s, over, p, s, mate))

    def onward(block):
        return inner if block == 0 else outer

    def take(role, block, p, passed):
        b = block + side * (3 - 2 * block)
        chunk = over if passed else t
        copies = []
        if role == "m" and (p in ALONG or not passed):
            copies.append(share(5 * passed, b, chunk, p, onward(block), t))
        if not passed and p not in ALONG:
            copies.append(share(3, b, chunk, p, s, over))
        copies.append(share(2 + 2 * passed, b, chunk, p, s, mate))

        @pl.when(roles[role])
        def _():
            share(0, b, chunk, p, s, mate).wait_recv()
            for copy in copies:
                copy.start()

        conditional.extend((roles[role], copy) for copy in copies)

    def normalize(block, n):
        b = index_of(block)
        for p in parts_of(n):
            share(2, b, mate, p, s, mate).wait_recv()
            share(4, b, diag, p, s, mate).wait_recv()
        step = 32

        def body(i, carry):
            here = pl.ds(pl.multiple_of(n * window + i * step, step), step)
            squares = jnp.zeros((step, 1), f32)
            for chunk in range(4):
                part = upd[b, chunk, here, :].astype(f32)
                squares = squares + jnp.sum(part * part, axis=-1, keepdims=True)
            inv = lax.rsqrt(squares / width + epsilon)
            for chunk in range(4):
                part = upd[b, chunk, here, :].astype(f32)
                span = slice(chunk * cols, (chunk + 1) * cols)
                norm_v[here, span] = (part * inv * gain_ref[0:1, span]).astype(bf16)
            return carry

        lax.fori_loop(0, window // step, body, 0)

    def slot_of(block):
        return 4 if block is None else index_of(block)

    def pass_on(slot, kind, chunk, tp, n):
        place = act.at[slot, chunk, pl.ds(n * window, window)]
        return remote(place, place, a_s.at[kind, slot, n], a_r.at[slot, chunk, n], s, tp)

    def activate(block, n):
        slot = slot_of(block)
        here = pl.ds(n * window, window)
        weight = sgu_v if block is None else gu_v
        both = jnp.dot(norm_v[here, :], weight[...], preferred_element_type=f32)
        gate, lin = both[:, :hidden], both[:, hidden:]
        act[slot, t, here, :] = (gate / (1.0 + jnp.exp(-gate)) * lin).astype(bf16)
        go(pass_on(slot, 0, t, over, n))
        go(pass_on(slot, 1, t, mate, n))

    def relay_act(role, block, n):
        if role == "b":
            copy = pass_on(s if block == 0 else 4, 2, over, mate, n)
            copy.wait_recv()
            go(copy)
        else:
            copy = pass_on(block + side * (3 - 2 * block), 2, over, mate, n)

            @pl.when(roles[role])
            def _():
                copy.wait_recv()
                copy.start()

            conditional.append((roles[role], copy))

    def contract_act(block, n):
        slot = slot_of(block)
        weight = sdn_v if block is None else dn_v
        pass_on(slot, 1, mate, mate, n).wait_recv()
        pass_on(slot, 2, diag, mate, n).wait_recv()
        total = None
        for chunk in range(4):
            part = jnp.dot(
                act[slot, chunk, pl.ds(n * window, window), :],
                weight[chunk * hidden : (chunk + 1) * hidden, :],
                preferred_element_type=f32,
            )
            total = part if total is None else total + part
        return total

    def weighted(block, n, total, other):
        here = pl.ds(n * window, window)
        listed = wx[index_of(block), :, here]
        place = lax.broadcasted_iota(jnp.int32, listed.shape, 0)
        column = down_rows(jnp.sum(jnp.where(place == s, listed, 0.0), axis=0, keepdims=True))
        return [
            column * total[:, c : c + window] + other(slice(c, c + window)).astype(f32)
            for c in range(0, cols, window)
        ]

    def back(flow, b, n, sp):
        here = pl.ds(n * window, window)
        return remote(
            ret.at[b, here], rin.at[flow, b, here], e_s.at[b, n], e_r.at[flow, b, n], sp, t
        )

    def give(block, n):
        b = index_of(block)
        here = pl.ds(n * window, window)
        if block[1] == 0:
            flow, sp = side + middle * (1 - 2 * side), inner + middle * (outer - inner)
        else:
            flow, sp = side, inner
        copy = back(flow, b, n, sp)
        total = contract_act(block, n)

        @pl.when(is_mid)
        def _():
            copy.wait_recv()

        sums = weighted(block, n, total, lambda c: rin[flow, b, here, c])
        for i, value in enumerate(sums):
            ret[b, here, i * window : (i + 1) * window] = value.astype(bf16)
        go(copy)

    def keep_own(n):
        here = pl.ds(n * window, window)
        sums = weighted(OWN, n, contract_act(OWN, n), lambda c: upd[s, t, here, c])
        for i, value in enumerate(sums):
            span = slice(i * window, (i + 1) * window)
            acc[here, span] = acc[here, span] + value

    def keep_shared(n):
        acc[pl.ds(n * window, window), :] = contract_act(None, n)

    def gather_in(n):
        here = pl.ds(n * window, window)
        back(1 - side, s, n, inner).wait_recv()

        @pl.when(is_mid)
        def _():
            back(side, s, n, outer).wait_recv()

        out_ref[here, :] = (
            acc[here, :] + rin[0, s, here, :].astype(f32) + rin[1, s, here, :].astype(f32)
        ).astype(bf16)

    def weights_on(kind, b, sp):
        return remote(wx.at[b], wx.at[b], x_s.at[kind], x_r.at[b], sp, t)

    def take_weights(role, block):
        copy = weights_on(2 + block, block + side * (3 - 2 * block), onward(block))

        @pl.when(roles[role])
        def _():
            copy.wait_recv()
            if role == "m":
                copy.start()

        if role == "m":
            conditional.append((is_mid, copy))

    def compute(block, n):
        normalize(block, n)
        activate(block, n)

    def compute_own(n):
        compute(OWN, n)
        activate(None, n)

    def enter():
        loaded("routes", "rw")
        wx[s] = jnp.zeros(wx.shape[1:], f32)
        for e in range(4):
            weight = jnp.zeros((1, rows), f32)
            for k in range(routes_ref.shape[0]):
                named = routes_ref[k : k + 1, :] == e
                weight = weight + jnp.where(named, rw_ref[k : k + 1, :], 0.0)
            wx[s, e : e + 1, :] = weight
        pl.semaphore_wait(barrier, 3 + middle)

        @pl.when(s < 3)
        def _():
            for copy in halos:
                copy.start()

        go(weights_on(0, s, inner))
        go(weights_on(1, s, outer), is_mid)
        loaded("wo")

    def load_rest():
        for name in loads:
            if name not in early:
                loads[name].start()

        @pl.when(is_end)
        def _():
            rin[side] = jnp.zeros(rin.shape[1:], bf16)

    def halo():
        @pl.when(s > 0)
        def _():
            for copy in halos:
                copy.wait_recv()

    steps = dict(
        attend=attend,
        enter=enter,
        rest=load_rest,
        halo=halo,
        chip=reduce_in_chip,
        across=reduce_across,
        hold=hold,
        loaded=loaded,
        publish=publish,
        send=send_own,
        own_over=own_over,
        take=take,
        weights=take_weights,
        compute=compute,
        compute_own=compute_own,
        relay=relay_act,
        give=give,
        shared=keep_shared,
        own=keep_own,
        finish=gather_in,
    )
    loaded("k", "q", "v")
    for name, *given in STEPS:
        steps[name](*given)

    for copy in pending:
        copy.wait_send()
    for when, copy in conditional:

        @pl.when(when)
        def _():
            copy.wait_send()

    @pl.when(s < 3)
    def _():
        for copy in halos:
            copy.wait_send()


def layer(
    residual,
    queries,
    keys,
    values,
    segments,
    routes,
    route_weight,
    sinks,
    out_weight,
    norm_gain,
    expert_gate,
    expert_up,
    expert_down,
    shared_gate,
    shared_up,
    shared_down,
):
    arguments = (
        residual,
        queries,
        keys,
        values,
        segments,
        routes,
        route_weight,
        sinks,
        out_weight,
        norm_gain,
        expert_gate,
        expert_up,
        expert_down,
        shared_gate,
        shared_up,
        shared_down,
    )
    rows, width = residual.shape
    n_sp, n_tp = lax.axis_size("sp"), lax.axis_size("tp")
    capacity = 2 * rows * routes.shape[1] // n_sp
    hidden = expert_gate.shape[2]
    if n_sp != 4 or n_tp != 4 or capacity < rows or rows != 2 * WINDOW or shared_gate.shape[1] != hidden:
        return shards(*arguments)
    cols = width // n_tp
    heads = queries.shape[1] // HEAD_DIM
    group = queries.shape[1] // keys.shape[1]
    kv_width = keys.shape[1]
    blocks = rows // WINDOW
    bf16, f32 = jnp.bfloat16, jnp.float32
    vmem = pl.BlockSpec(memory_space=pltpu.VMEM)
    anywhere = pl.BlockSpec(memory_space=pl.ANY)
    dma = pltpu.SemaphoreType.DMA
    piece = rows // PARTS
    return pl.pallas_call(
        functools.partial(fused_kernel, (rows, cols, width, WINDOW, hidden, heads, group)),
        out_shape=jax.ShapeDtypeStruct((rows, cols), bf16),
        in_specs=[anywhere] * 7 + [pl.BlockSpec(memory_space=pltpu.SMEM)] + [anywhere] * 8,
        out_specs=vmem,
        scratch_shapes=[
            pltpu.VMEM(queries.shape, bf16),
            pltpu.VMEM(keys.shape, bf16),
            pltpu.VMEM(values.shape, bf16),
            pltpu.VMEM((1, rows), jnp.int32),
            pltpu.VMEM(routes.shape[::-1], jnp.int32),
            pltpu.VMEM(routes.shape[::-1], f32),
            pltpu.VMEM((1, width), f32),
            pltpu.VMEM((rows, cols), bf16),
            pltpu.VMEM(out_weight.shape, bf16),
            pltpu.VMEM((width, 2 * hidden), bf16),
            pltpu.VMEM((width, 2 * hidden), bf16),
            pltpu.VMEM(expert_down.shape[1:], bf16),
            pltpu.VMEM(shared_down.shape, bf16),
            pltpu.VMEM((WINDOW, kv_width), bf16),
            pltpu.VMEM((WINDOW, kv_width), bf16),
            pltpu.VMEM((8, WINDOW), f32),
            pltpu.VMEM((8, rows), f32),
            pltpu.VMEM((8, WINDOW), f32),
            pltpu.VMEM((4, 8, rows), f32),
            pltpu.VMEM((rows, heads * HEAD_DIM), bf16),
            pltpu.VMEM((blocks, 2, WINDOW, cols), bf16),
            pltpu.VMEM((blocks, 2, WINDOW, cols), bf16),
            pltpu.VMEM((PARTS, piece, cols), bf16),
            pltpu.VMEM((PARTS, piece, cols), bf16),
            pltpu.VMEM((rows, cols), f32),
            pltpu.VMEM((4, 4, rows, cols), bf16),
            pltpu.VMEM((rows, width), bf16),
            pltpu.VMEM((5, 4, rows, hidden), bf16),
            pltpu.VMEM((4, rows, cols), bf16),
            pltpu.VMEM((2, 4, rows, cols), bf16),
            pltpu.VMEM((rows, cols), f32),
            dma((16,)),
            dma((3,)),
            dma((3,)),
            dma((6,)),
            dma((4,)),
            dma((blocks, 2)),
            dma((blocks, 2)),
            dma((PARTS,)),
            dma((PARTS,)),
            dma((7, 4, PARTS)),
            dma((4, 4, PARTS)),
            dma((3, 5, blocks)),
            dma((5, 4, blocks)),
            dma((4, blocks)),
            dma((2, 4, blocks)),
        ],
        compiler_params=pltpu.CompilerParams(collective_id=0, has_side_effects=True),
    )(
        residual,
        queries,
        keys,
        values,
        segments[None, :],
        routes.T,
        route_weight.T,
        sinks,
        out_weight,
        norm_gain[None, :],
        expert_gate,
        expert_up,
        expert_down,
        shared_gate,
        shared_up,
        shared_down,
    )


def solution(mesh):
    placed = (
        P(("grp", "sp"), None),
        P(("grp", "sp"), "tp"),
        P(("grp", "sp"), "tp"),
        P(("grp", "sp"), "tp"),
        P(("grp", "sp")),
        P(("grp", "sp"), None),
        P(("grp", "sp"), None),
        P("tp"),
        P("tp", None),
        P(),
        P("sp", None, "tp"),
        P("sp", None, "tp"),
        P("sp", None, "tp"),
        P(None, "tp"),
        P(None, "tp"),
        P(None, "tp"),
    )
    return jax.shard_map(
        layer, mesh=mesh, in_specs=placed, out_specs=P(("grp", "sp"), "tp"), check_vma=False
    )
```

```python
import functools
import math
import jax
import jax.numpy as jnp
from jax import lax
from jax.experimental import pallas as pl
from jax.experimental.pallas import tpu as pltpu
from jax.sharding import PartitionSpec as P

HEAD_DIM = 64
WINDOW = 128


epsilon = 1e-06


def passed_along(value, axis, steps):
    count = lax.axis_size(axis)
    leading, last = (max(0, -steps), min(count, count - steps))
    return lax.ppermute(value, axis, [(source, source + steps) for source in range(leading, last)])


def banded(prev_rows, own_rows, window_len):
    blocks = own_rows.shape[0] // window_len
    joined = jnp.concatenate([prev_rows, own_rows], axis=0)
    shaped = joined.reshape((blocks + 1, window_len) + own_rows.shape[1:])
    return jnp.concatenate([shaped[:-1], shaped[1:]], axis=1)


def shards(
    residual,
    queries,
    keys,
    values,
    segments,
    routes,
    route_weight,
    sinks,
    out_weight,
    norm_gain,
    expert_gate,
    expert_up,
    expert_down,
    shared_gate,
    shared_up,
    shared_down,
):
    rows_here = residual.shape[0]
    model_width = residual.shape[1]
    tp_count = lax.axis_size("tp")
    tp_index = lax.axis_index("tp")
    head_local = queries.shape[1] // HEAD_DIM
    kv_local = keys.shape[1] // HEAD_DIM
    group_size = head_local // kv_local
    window_len = WINDOW
    blocks = rows_here // window_len
    own_marks = (segments % 256 + 1).astype(jnp.bfloat16)
    prev_keys, prev_values, prev_marks = passed_along(
        (
            keys[rows_here - window_len :],
            values[rows_here - window_len :],
            own_marks[rows_here - window_len :],
        ),
        "sp",
        1,
    )
    key_band = banded(prev_keys, keys, window_len).reshape(
        blocks, 2 * window_len, kv_local, HEAD_DIM
    )
    value_band = banded(prev_values, values, window_len).reshape(
        blocks, 2 * window_len, kv_local, HEAD_DIM
    )
    mark_band = banded(prev_marks, own_marks, window_len).astype(jnp.float32)
    query_marks = own_marks.reshape(blocks, window_len).astype(jnp.float32)
    query_blocks = queries.reshape(blocks, window_len, kv_local, group_size, HEAD_DIM)
    scores = jnp.einsum(
        "nqhgd,nkhd->nhgqk", query_blocks, key_band, preferred_element_type=jnp.float32
    ) * HEAD_DIM ** (-0.5)
    offsets = jnp.arange(window_len)[:, None] + window_len - jnp.arange(2 * window_len)[None, :]
    allowed = (
        (offsets >= 0) & (offsets < window_len) & (query_marks[:, :, None] == mark_band[:, None, :])
    )
    sink_logits = sinks.reshape(kv_local, group_size)[None, :, :, None]
    masked = jnp.where(allowed[:, None, None], scores, -jnp.inf)
    top_score = jnp.maximum(jnp.max(masked, axis=-1), sink_logits)
    exp_terms = jnp.where(allowed[:, None, None], jnp.exp(scores - top_score[..., None]), 0.0)
    denominator = jnp.sum(exp_terms, axis=-1) + jnp.exp(sink_logits - top_score)
    probabilities = (exp_terms / denominator[..., None]).astype(jnp.bfloat16)
    attended = jnp.einsum(
        "nhgqk,nkhd->nqhgd", probabilities, value_band, preferred_element_type=jnp.float32
    )
    attended = attended.astype(jnp.bfloat16).reshape(rows_here, head_local * HEAD_DIM)
    partial_value = jnp.dot(attended, out_weight, preferred_element_type=jnp.float32)
    col_width = model_width // tp_count
    col_start = tp_index * col_width
    summed = lax.psum(partial_value, "tp")
    updated = (residual.astype(jnp.float32) + summed).astype(jnp.bfloat16)
    updated_f32 = updated.astype(jnp.float32)
    inv_rms = lax.rsqrt(jnp.mean(updated_f32 * updated_f32, axis=-1, keepdims=True) + epsilon)
    normed = (updated_f32 * inv_rms * norm_gain).astype(jnp.bfloat16)
    updated_cols = lax.dynamic_slice_in_dim(updated, col_start, col_width, 1)
    normed_cols = lax.dynamic_slice_in_dim(normed, col_start, col_width, 1)
    shared_pre = jnp.dot(normed, shared_gate, preferred_element_type=jnp.float32)
    shared_lin = jnp.dot(normed, shared_up, preferred_element_type=jnp.float32)
    shared_act = (jax.nn.silu(shared_pre) * shared_lin).astype(jnp.bfloat16)
    top_count = routes.shape[1]
    experts = lax.axis_size("sp")
    capacity = 2 * rows_here * top_count // experts
    flat_ids = routes.reshape(-1)
    one_hot = (flat_ids[:, None] == jnp.arange(experts, dtype=jnp.int32)[None, :]).astype(jnp.int32)
    rank_in = jnp.cumsum(one_hot, axis=0) - one_hot
    slot_dest = flat_ids * capacity + jnp.sum(rank_in * one_hot, axis=1)
    token_of = jnp.arange(rows_here * top_count, dtype=jnp.int32) // top_count
    slot_token = jnp.full((experts * capacity,), -1, jnp.int32).at[slot_dest].set(token_of)
    filled = slot_token >= 0
    safe_token = jnp.where(filled, slot_token, 0)
    outgoing = jnp.where(filled[:, None], normed_cols[safe_token], jnp.zeros((), jnp.bfloat16))
    pieces = lax.all_to_all(
        outgoing.reshape(experts, capacity, col_width),
        "sp",
        split_axis=0,
        concat_axis=0,
        tiled=True,
    )
    arrived = lax.all_gather(pieces, "tp", axis=2, tiled=True)
    expert_rows = arrived.reshape(-1, model_width)
    gate_pre = jnp.dot(expert_rows, expert_gate[0], preferred_element_type=jnp.float32)
    up_lin = jnp.dot(expert_rows, expert_up[0], preferred_element_type=jnp.float32)
    expert_act = (jax.nn.silu(gate_pre) * up_lin).astype(jnp.bfloat16)
    gathered_expert, gathered_shared = (
        lax.all_gather(expert_act, "tp", axis=1, tiled=True),
        lax.all_gather(shared_act, "tp", axis=1, tiled=True),
    )
    expert_out = jnp.dot(
        gathered_expert, expert_down[0], preferred_element_type=jnp.float32
    ).astype(jnp.bfloat16)
    returned = lax.all_to_all(
        expert_out.reshape(experts, capacity, col_width),
        "sp",
        split_axis=0,
        concat_axis=0,
        tiled=True,
    )
    returned = returned.reshape(experts * capacity, col_width)
    picked = returned[slot_dest].astype(jnp.float32).reshape(rows_here, top_count, col_width)
    routed = jnp.sum(picked * route_weight[:, :, None], axis=1)
    shared_cols = jnp.dot(gathered_shared, shared_down, preferred_element_type=jnp.float32)
    return (updated_cols.astype(jnp.float32) + shared_cols + routed).astype(jnp.bfloat16)


MESH = pl.DeviceIdType.MESH
PARTS = 4
OWN = (0, 1)
E, M, B = 0, 1, 2
ALONG = {
    (E, 1): (0, 1),
    (E, 2): (1,),
    (E, 3): (2,),
    (M, 0): (0, 1, 2, 3),
    (M, 2): (1, 2),
    (M, 3): (),
}


def fused_kernel(
    dims,
    res_hbm,
    q_hbm,
    k_hbm,
    v_hbm,
    seg_hbm,
    routes_hbm,
    rw_hbm,
    sinks_ref,
    wo_hbm,
    gain_hbm,
    eg_hbm,
    eu_hbm,
    ed_hbm,
    sg_hbm,
    su_hbm,
    sd_hbm,
    out_hbm,
    q_ref,
    k_ref,
    v_ref,
    seg_ref,
    routes_ref,
    rw_ref,
    gain_ref,
    res_v,
    wo_v,
    gu_v,
    sgu_v,
    dn_v,
    sdn_v,
    kh,
    vh,
    mh,
    marks_own,
    marks_v,
    wx,
    att,
    b1s,
    b1r,
    b2s,
    b2r,
    keep,
    upd,
    norm_v,
    norm_h,
    act,
    tot,
    ret,
    rin,
    acc,
    result,
    w_sem,
    sent_s,
    out_s,
    halo_r,
    x_r,
    b_r,
    c_r,
    u_r,
    m_r,
    a_r,
    e_r,
):
    rows, cols, width, window, hidden, heads, group = dims
    bf16, f32 = jnp.bfloat16, jnp.float32
    s = lax.axis_index("sp")
    t = lax.axis_index("tp")
    core = t % 2
    chip = t // 2
    mate = t + 1 - 2 * core
    over = t + 2 - 4 * chip
    diag = 3 - t
    side = s // 2
    middle = ((s + 1) // 2) % 2
    is_mid = middle == 1
    is_end = middle == 0
    inner = s + 1 - 2 * side
    outer = (s + 3 + 2 * side) % 4

    def index_of(block):
        end, mid = block
        b = end + middle * (mid - end)
        return b + side * (3 - 2 * b)

    roles = (is_end, is_mid, None)
    sent = [0, 0, 0]

    def remote(src, dst, recv, sp, tp, role=B):
        return pltpu.make_async_remote_copy(
            src_ref=src,
            dst_ref=dst,
            send_sem=sent_s.at[role],
            recv_sem=recv,
            device_id={"sp": sp, "tp": tp},
            device_id_type=MESH,
        )

    def count(copy, role):
        width_of = 2 if copy.src_ref.dtype == bf16 else 4
        sent[role] += math.prod(copy.src_ref.shape) * width_of

    def go(copy, role=B):
        if role == B:
            copy.start()
        else:

            @pl.when(roles[role])
            def _():
                copy.start()

        count(copy, role)

    barrier = pltpu.get_barrier_semaphore()
    for sp, tp in ((s, mate), (s, over), (inner, t)):
        pl.semaphore_signal(barrier, inc=1, device_id={"sp": sp, "tp": tp}, device_id_type=MESH)

    @pl.when(is_mid)
    def _():
        pl.semaphore_signal(barrier, inc=1, device_id={"sp": outer, "tp": t}, device_id_type=MESH)

    own_cols = pl.ds(pl.multiple_of(t * cols, cols), cols)
    first_half = pl.ds(0, hidden)
    second_half = pl.ds(hidden, hidden)
    sources = dict(
        seg=(seg_hbm, seg_ref),
        k=(k_hbm, k_ref),
        q=(q_hbm, q_ref),
        v=(v_hbm, v_ref),
        routes=(routes_hbm, routes_ref),
        rw=(rw_hbm, rw_ref),
        wo=(wo_hbm, wo_v),
        res=(res_hbm.at[:, own_cols], res_v),
        gain=(gain_hbm, gain_ref),
        eg=(eg_hbm.at[0], gu_v.at[:, first_half]),
        eu=(eu_hbm.at[0], gu_v.at[:, second_half]),
        sg=(sg_hbm, sgu_v.at[:, first_half]),
        su=(su_hbm, sgu_v.at[:, second_half]),
        ed=(ed_hbm.at[0], dn_v),
        sd=(sd_hbm, sdn_v),
    )
    loads = {
        name: pltpu.make_async_copy(src, dst, w_sem.at[i])
        for i, (name, (src, dst)) in enumerate(sources.items())
    }
    for load in loads.values():
        load.start()

    def loaded(*names):
        for name in names:
            loads[name].wait()

    tail = pl.ds(rows - window, window)
    up_sp = (s + 1) % 4
    halos = [
        remote(k_ref.at[tail], kh, halo_r.at[0], up_sp, t, 3),
        remote(v_ref.at[tail], vh, halo_r.at[1], up_sp, t, 3),
        remote(marks_v, mh, halo_r.at[2], up_sp, t, 3),
    ]

    @pl.when(s == 0)
    def _():
        kh[...] = jnp.zeros_like(kh)
        vh[...] = jnp.zeros_like(vh)
        mh[...] = jnp.full(mh.shape, -1.0, f32)

    loaded("seg")
    marks_own[...] = jnp.broadcast_to(seg_ref[...].astype(f32), marks_own.shape)
    marks_v[...] = marks_own[:, tail]

    def down_rows(row):
        return jnp.transpose(jnp.broadcast_to(row, (window, window)))

    q_pos = lax.broadcasted_iota(jnp.int32, (window, window), 0)
    k_pos = lax.broadcasted_iota(jnp.int32, (window, window), 1)

    def attend(n):
        here = pl.ds(n * window, window)
        if n == 0:
            k_prev, v_prev, m_prev = kh, vh, mh[0:1, :]
            before = slice(None)
        else:
            before = pl.ds((n - 1) * window, window)
            k_prev, v_prev, m_prev = k_ref, v_ref, marks_own[0:1, before]
        m_own = marks_own[0:1, here]
        marks = down_rows(m_own)
        ok_prev = (k_pos > q_pos) & (marks == m_prev)
        ok_own = (k_pos <= q_pos) & (marks == m_own)
        contract = (((1,), (1,)), ((), ()))
        every = range(heads)
        kv = [slice((h // group) * HEAD_DIM, (h // group + 1) * HEAD_DIM) for h in every]
        scores = []
        for h in every:
            qh = q_ref[here, h * HEAD_DIM : (h + 1) * HEAD_DIM]
            pair = [
                lax.dot_general(qh, k, contract, preferred_element_type=f32) * HEAD_DIM ** (-0.5)
                for k in (k_prev[before, kv[h]], k_ref[here, kv[h]])
            ]
            scores.append((jnp.where(ok_prev, pair[0], -jnp.inf), jnp.where(ok_own, pair[1], -jnp.inf)))
        tops = [
            jnp.maximum(jnp.max(jnp.maximum(*scores[h]), axis=-1, keepdims=True), sinks_ref[h])
            for h in every
        ]
        terms = [tuple(jnp.exp(score - tops[h]) for score in scores[h]) for h in every]
        totals = [
            jnp.sum(terms[h][0] + terms[h][1], axis=-1, keepdims=True)
            + jnp.exp(sinks_ref[h] - tops[h])
            for h in every
        ]
        for h in every:
            inverse = 1.0 / totals[h]
            p_prev, p_own = ((term * inverse).astype(bf16) for term in terms[h])
            got = jnp.dot(p_prev, v_prev[before, kv[h]], preferred_element_type=f32) + jnp.dot(
                p_own, v_ref[here, kv[h]], preferred_element_type=f32
            )
            att[here, h * HEAD_DIM : (h + 1) * HEAD_DIM] = got.astype(bf16)

    def project(n, chunk):
        where = pl.ds(pl.multiple_of(chunk * cols, cols), cols)
        return jnp.dot(
            att[pl.ds(n * window, window), :], wo_v[:, where], preferred_element_type=f32
        )

    part_rows = rows // PARTS
    per_half = window // part_rows

    def parts_of(n):
        return range(n * per_half, (n + 1) * per_half)

    def part_span(p):
        return pl.ds(p * part_rows, part_rows)

    first = {}
    second = {}

    def reduce_in_chip(n):
        for far in (1, 0):
            chunk = (over if far else t) + 1 - 2 * core
            b1s[n, far] = project(n, chunk).astype(bf16)
            copy = remote(
                b1s.at[n, far], b1r.at[n, far], b_r.at[n, far], s, mate
            )
            go(copy)
            first[n, far] = copy

    def reduce_across(n):
        mine = project(n, over)
        first[n, 1].wait_recv()
        mine = mine + b1r[n, 1].astype(f32)
        for i, p in enumerate(parts_of(n)):
            b2s[p] = mine[i * part_rows : (i + 1) * part_rows].astype(bf16)
            copy = remote(b2s.at[p], b2r.at[p], c_r.at[p], s, over)
            go(copy)
            second[p] = copy

    def hold(n):
        here = pl.ds(n * window, window)
        mine = project(n, t) + res_v[here, :].astype(f32)
        first[n, 0].wait_recv()
        keep[here, :] = mine + b1r[n, 0].astype(f32)

    def piece(b, chunk, p):
        return upd.at[b, chunk, part_span(p)]

    def share(passed, b, chunk, p, sp, tp, role=B):
        place = piece(b, chunk, p)
        return remote(place, place, u_r.at[b, passed, p], sp, tp, role)

    def to_mate(b, chunk, p, role=B):
        place = piece(b, chunk, p)
        return remote(place, place, m_r.at[b, p // per_half], s, mate, role)

    def send_own(role, far, p, passed):
        wanted = (M, 0) if role == E else (E, 1) if far else (M, 2)
        if passed and p not in ALONG[wanted]:
            return
        chunk = over if passed else t
        go(share(passed, s, chunk, p, outer if far else inner, t, role), role)

    def publish(p):
        second[p].wait_recv()
        upd[s, t, part_span(p), :] = (keep[part_span(p), :] + b2r[p].astype(f32)).astype(bf16)
        go(share(1, s, t, p, s, over))
        go(to_mate(s, t, p))

    def own_over(p):
        share(1, s, over, p, s, over).wait_recv()
        go(to_mate(s, over, p))

    def onward(block):
        return inner if block == 0 else outer

    def take(role, block, p, passed):
        b = block + side * (3 - 2 * block)
        chunk = over if passed else t
        copies = []
        if role == M and (not passed or p in ALONG[(M, 3) if block == 0 else (E, block)]):
            copies.append(share(passed, b, chunk, p, onward(block), t, role))
        if not passed and p not in ALONG[role, block]:
            copies.append(share(1, b, chunk, p, s, over, role))
        copies.append(to_mate(b, chunk, p, role))

        @pl.when(roles[role])
        def _():
            share(passed, b, chunk, p, s, mate).wait_recv()
            for copy in copies:
                copy.start()

        for copy in copies:
            count(copy, role)

    def normalize(block, n, rows_out):
        b = index_of(block)
        landed = upd.at[b, pl.ds(0, 2), pl.ds(n * window, window)]
        remote(landed, landed, m_r.at[b, n], s, mate).wait_recv()
        step = 32

        def body(i, carry):
            here = pl.ds(pl.multiple_of(n * window + i * step, step), step)
            squares = jnp.zeros((step, 1), f32)
            for chunk in range(4):
                part = upd[b, chunk, here, :].astype(f32)
                squares = squares + jnp.sum(part * part, axis=-1, keepdims=True)
            inv = lax.rsqrt(squares / width + epsilon)
            for chunk in range(4):
                part = upd[b, chunk, here, :].astype(f32)
                span = slice(chunk * cols, (chunk + 1) * cols)
                rows_out[here, span] = (part * inv * gain_ref[0:1, span]).astype(bf16)
            return carry

        lax.fori_loop(0, window // step, body, 0)

    def slot_of(block):
        return 4 if block is None else index_of(block)

    def pass_on(slot, chunk, tp, n, role=B):
        place = act.at[slot, chunk, pl.ds(n * window, window)]
        flow = 0 if tp is over else 1
        return remote(place, place, a_r.at[slot, flow, n], s, tp, role)

    def activate(block, n, normed):
        slot = slot_of(block)
        here = pl.ds(n * window, window)
        weight = sgu_v if block is None else gu_v
        both = jnp.dot(normed[here, :], weight[...], preferred_element_type=f32)
        gate, lin = both[:, :hidden], both[:, hidden:]
        act[slot, t, here, :] = (gate / (1.0 + jnp.exp(-gate)) * lin).astype(bf16)
        go(pass_on(slot, t, over, n))
        go(pass_on(slot, t, mate, n))

    def relay_act(role, block, n):
        if role == B:
            slot = s if block == 0 else 4
            pass_on(slot, over, over, n).wait_recv()
            go(pass_on(slot, over, mate, n))
        else:
            slot = block + side * (3 - 2 * block)
            copy = pass_on(slot, over, mate, n, role)

            @pl.when(roles[role])
            def _():
                pass_on(slot, over, over, n).wait_recv()
                copy.start()

            count(copy, role)

    def contract_act(block, n):
        slot = slot_of(block)
        weight = sdn_v if block is None else dn_v
        landed = act.at[slot, pl.ds(0, 2), pl.ds(n * window, window)]
        remote(landed, landed, a_r.at[slot, 1, n], s, mate).wait_recv()
        total = None
        for chunk in range(4):
            part = jnp.dot(
                act[slot, chunk, pl.ds(n * window, window), :],
                weight[chunk * hidden : (chunk + 1) * hidden, :],
                preferred_element_type=f32,
            )
            total = part if total is None else total + part
        return total

    def weighted(block, n, place, other):
        here = pl.ds(n * window, window)
        total = contract_act(block, n)
        listed = wx[index_of(block), :, here]
        row = lax.broadcasted_iota(jnp.int32, listed.shape, 0)
        column = down_rows(jnp.sum(jnp.where(row == s, listed, 0.0), axis=0, keepdims=True))
        for c in range(0, cols, window):
            value = column * total[:, c : c + window]
            if other is not None:
                value = value + other(slice(c, c + window))
            place[here, c : c + window] = value

    def back(place, b, p, sp, role=B):
        here = part_span(p)
        return remote(ret.at[b, here], rin.at[place, here], e_r.at[place, p], sp, t, role)

    def give(block, n):
        weighted(block, n, tot.at[index_of(block)], None)

    def pass_back(role, block, p):
        b = block + side * (3 - 2 * block)
        here = part_span(p)
        place = 4 if (role, block) == (E, 1) else b
        copy = back(place, b, p, outer if (role, block) == (M, 0) else inner, role)

        @pl.when(roles[role])
        def _():
            value = tot[b, here, :]
            if role == M:
                back(b, b, p, inner).wait_recv()
                value = value + rin[b, here, :].astype(f32)
            ret[b, here, :] = value.astype(bf16)
            copy.start()

        count(copy, role)

    def keep_own(n):
        here = pl.ds(n * window, window)
        weighted(OWN, n, acc, lambda c: upd[s, t, here, c].astype(f32) + acc[here, c])

    def keep_shared(n):
        acc[pl.ds(n * window, window), :] = contract_act(None, n)

    def gather_in(p):
        here = part_span(p)
        back(s, s, p, inner).wait_recv()

        @pl.when(is_mid)
        def _():
            back(4, s, p, outer).wait_recv()

        result[here, :] = (
            acc[here, :] + rin[s, here, :].astype(f32) + rin[4, here, :].astype(f32)
        ).astype(bf16)
        stores[p].start()

    stores = [
        pltpu.make_async_copy(
            result.at[part_span(p)], out_hbm.at[part_span(p)], out_s.at[p]
        )
        for p in range(PARTS)
    ]

    def weights_on(b, sp, role=B):
        return remote(wx.at[b], wx.at[b], x_r.at[b], sp, t, role)

    def take_weights(role, block):
        copy = weights_on(block + side * (3 - 2 * block), onward(block), M)

        @pl.when(roles[role])
        def _():
            copy.wait_recv()
            if role == M:
                copy.start()

        if role == M:
            count(copy, M)

    def compute(block, n):
        normalize(block, n, norm_v)
        activate(block, n, norm_v)

    def norm_own(n):
        normalize(OWN, n, norm_h)

    def act_own(n):
        activate(OWN, n, norm_h)

    def act_shared(n):
        activate(None, n, norm_h)

    def enter():
        loaded("routes", "rw")
        wx[s] = jnp.zeros(wx.shape[1:], f32)
        for e in range(4):
            weight = jnp.zeros((1, rows), f32)
            for k in range(routes_ref.shape[0]):
                named = routes_ref[k : k + 1, :] == e
                weight = weight + jnp.where(named, rw_ref[k : k + 1, :], 0.0)
            wx[s, e : e + 1, :] = weight
        pl.semaphore_wait(barrier, 3 + middle)

        @pl.when(s < 3)
        def _():
            for copy in halos:
                copy.start()

        go(weights_on(s, inner))
        go(weights_on(s, outer, M), M)
        loaded("wo")

    def clear():
        @pl.when(is_end)
        def _():
            rin[4] = jnp.zeros(rin.shape[1:], bf16)

    def halo():
        @pl.when(s > 0)
        def _():
            for copy in halos:
                copy.wait_recv()

    loaded("k", "q", "v")
    attend(1)
    enter()
    reduce_in_chip(1)
    loaded("res")
    reduce_across(1)
    hold(1)
    take_weights(M, 2)
    halo()
    attend(0)
    reduce_in_chip(0)
    take_weights(M, 0)
    reduce_across(0)
    publish(2)
    clear()
    send_own(E, 0, 2, 0)
    send_own(M, 0, 2, 0)
    loaded("gain", "eg", "eu", "sg", "su", "ed", "sd")
    send_own(M, 1, 2, 0)
    hold(0)
    publish(3)
    send_own(E, 0, 3, 0)
    send_own(M, 0, 3, 0)
    send_own(M, 1, 3, 0)
    take(M, 0, 2, 0)
    take_weights(M, 3)
    publish(0)
    take(M, 2, 2, 0)
    take(M, 0, 3, 0)
    take(M, 2, 3, 0)
    take(M, 0, 0, 0)
    take(M, 3, 2, 0)
    send_own(E, 0, 0, 0)
    publish(1)
    take(M, 0, 1, 0)
    send_own(E, 0, 1, 0)
    take(E, 1, 2, 0)
    own_over(2)
    take(M, 3, 3, 0)
    send_own(M, 0, 0, 0)
    send_own(E, 0, 2, 1)
    own_over(3)
    own_over(0)
    send_own(E, 0, 0, 1)
    take(E, 2, 2, 0)
    take(M, 3, 0, 0)
    take(E, 2, 3, 0)
    take(M, 3, 1, 0)
    take(M, 0, 2, 1)
    take_weights(E, 1)
    take_weights(E, 3)
    take(M, 2, 3, 1)
    send_own(M, 0, 1, 0)
    take(M, 3, 2, 1)
    send_own(M, 0, 2, 1)
    take(E, 1, 3, 0)
    take(M, 2, 0, 0)
    own_over(1)
    send_own(M, 0, 1, 1)
    norm_own(1)
    take(E, 2, 2, 1)
    send_own(E, 0, 3, 1)
    take_weights(E, 2)
    take(E, 1, 2, 1)
    send_own(M, 1, 1, 1)
    take(E, 3, 3, 0)
    take(E, 2, 3, 1)
    take(M, 3, 3, 1)
    take(E, 3, 0, 0)
    send_own(M, 1, 0, 1)
    take(M, 0, 0, 1)
    take(E, 3, 1, 0)
    take(M, 0, 3, 1)
    compute((2, 3), 1)
    take(E, 3, 2, 0)
    norm_own(0)
    take(E, 3, 2, 1)
    take(M, 2, 2, 1)
    take(E, 3, 3, 1)
    take(E, 3, 0, 1)
    take(M, 2, 1, 0)
    take(M, 2, 1, 1)
    take(E, 1, 3, 1)
    take(E, 2, 0, 0)
    send_own(M, 1, 1, 0)
    take(M, 3, 1, 1)
    compute((3, 0), 1)
    take(E, 3, 1, 1)
    send_own(M, 1, 0, 0)
    compute((1, 2), 1)
    relay_act(E, 2, 1)
    take(M, 3, 0, 1)
    send_own(E, 0, 1, 1)
    compute((3, 3), 0)
    relay_act(M, 3, 1)
    give((2, 3), 1)
    pass_back(E, 2, 3)
    pass_back(E, 2, 2)
    take(E, 2, 0, 1)
    act_shared(0)
    relay_act(M, 2, 1)
    relay_act(E, 3, 1)
    take(M, 2, 0, 1)
    take(E, 2, 1, 0)
    take(E, 2, 1, 1)
    take(E, 1, 1, 1)
    act_own(1)
    take(M, 0, 1, 1)
    give((3, 2), 1)
    pass_back(E, 3, 3)
    relay_act(M, 3, 0)
    compute((2, 0), 0)
    relay_act(E, 3, 0)
    pass_back(E, 3, 2)
    pass_back(M, 2, 2)
    take(E, 1, 0, 0)
    relay_act(M, 0, 1)
    take(E, 1, 0, 1)
    take(E, 1, 1, 0)
    give((3, 3), 0)
    pass_back(E, 3, 1)
    relay_act(E, 1, 1)
    pass_back(M, 3, 3)
    pass_back(E, 3, 0)
    compute((1, 2), 0)
    pass_back(M, 3, 2)
    give((1, 0), 1)
    pass_back(E, 1, 2)
    relay_act(E, 2, 0)
    relay_act(M, 0, 0)
    relay_act(B, 1, 0)
    pass_back(M, 3, 1)
    act_own(0)
    give((2, 0), 0)
    pass_back(E, 2, 1)
    pass_back(M, 0, 3)
    relay_act(E, 1, 0)
    pass_back(M, 3, 0)
    pass_back(E, 2, 0)
    act_shared(1)
    relay_act(M, 2, 0)
    pass_back(M, 0, 2)
    pass_back(M, 2, 3)
    give((1, 2), 0)
    pass_back(E, 1, 3)
    pass_back(M, 0, 1)
    pass_back(M, 2, 1)
    pass_back(E, 1, 1)
    keep_shared(0)
    relay_act(B, 0, 0)
    pass_back(M, 0, 0)
    pass_back(M, 2, 0)
    relay_act(B, 1, 1)
    pass_back(E, 1, 0)
    relay_act(B, 0, 1)
    keep_shared(1)
    keep_own(0)
    keep_own(1)
    gather_in(3)
    gather_in(1)
    gather_in(2)
    gather_in(0)

    def settle(size, sem):
        for unit in (upd.at[0], upd.at[0, 0], piece(0, 0, 0), wx.at[0]):
            of_one = math.prod(unit.shape) * (4 if unit.dtype == f32 else 2)
            for _ in range(size // of_one):
                pltpu.make_async_copy(unit, unit, sem).wait()
            size = size % of_one

    settle(sent[B], sent_s.at[B])

    @pl.when(is_end)
    def _():
        settle(sent[E], sent_s.at[E])

    @pl.when(is_mid)
    def _():
        settle(sent[M], sent_s.at[M])

    @pl.when(s < 3)
    def _():
        for copy in halos:
            copy.wait_send()

    for store in stores:
        store.wait()


def layer(
    residual,
    queries,
    keys,
    values,
    segments,
    routes,
    route_weight,
    sinks,
    out_weight,
    norm_gain,
    expert_gate,
    expert_up,
    expert_down,
    shared_gate,
    shared_up,
    shared_down,
):
    arguments = (
        residual,
        queries,
        keys,
        values,
        segments,
        routes,
        route_weight,
        sinks,
        out_weight,
        norm_gain,
        expert_gate,
        expert_up,
        expert_down,
        shared_gate,
        shared_up,
        shared_down,
    )
    rows, width = residual.shape
    n_sp, n_tp = lax.axis_size("sp"), lax.axis_size("tp")
    capacity = 2 * rows * routes.shape[1] // n_sp
    hidden = expert_gate.shape[2]
    if n_sp != 4 or n_tp != 4 or capacity < rows or rows != 2 * WINDOW or shared_gate.shape[1] != hidden:
        return shards(*arguments)
    cols = width // n_tp
    heads = queries.shape[1] // HEAD_DIM
    group = queries.shape[1] // keys.shape[1]
    kv_width = keys.shape[1]
    blocks = rows // WINDOW
    bf16, f32 = jnp.bfloat16, jnp.float32
    vmem = pl.BlockSpec(memory_space=pltpu.VMEM)
    anywhere = pl.BlockSpec(memory_space=pl.ANY)
    dma = pltpu.SemaphoreType.DMA
    piece = rows // PARTS
    return pl.pallas_call(
        functools.partial(fused_kernel, (rows, cols, width, WINDOW, hidden, heads, group)),
        out_shape=jax.ShapeDtypeStruct((rows, cols), bf16),
        in_specs=[anywhere] * 7 + [pl.BlockSpec(memory_space=pltpu.SMEM)] + [anywhere] * 8,
        out_specs=anywhere,
        scratch_shapes=[
            pltpu.VMEM(queries.shape, bf16),
            pltpu.VMEM(keys.shape, bf16),
            pltpu.VMEM(values.shape, bf16),
            pltpu.VMEM((1, rows), jnp.int32),
            pltpu.VMEM(routes.shape[::-1], jnp.int32),
            pltpu.VMEM(routes.shape[::-1], f32),
            pltpu.VMEM((1, width), f32),
            pltpu.VMEM((rows, cols), bf16),
            pltpu.VMEM(out_weight.shape, bf16),
            pltpu.VMEM((width, 2 * hidden), bf16),
            pltpu.VMEM((width, 2 * hidden), bf16),
            pltpu.VMEM(expert_down.shape[1:], bf16),
            pltpu.VMEM(shared_down.shape, bf16),
            pltpu.VMEM((WINDOW, kv_width), bf16),
            pltpu.VMEM((WINDOW, kv_width), bf16),
            pltpu.VMEM((8, WINDOW), f32),
            pltpu.VMEM((8, rows), f32),
            pltpu.VMEM((8, WINDOW), f32),
            pltpu.VMEM((4, 8, rows), f32),
            pltpu.VMEM((rows, heads * HEAD_DIM), bf16),
            pltpu.VMEM((blocks, 2, WINDOW, cols), bf16),
            pltpu.VMEM((blocks, 2, WINDOW, cols), bf16),
            pltpu.VMEM((PARTS, piece, cols), bf16),
            pltpu.VMEM((PARTS, piece, cols), bf16),
            pltpu.VMEM((rows, cols), f32),
            pltpu.VMEM((4, 4, rows, cols), bf16),
            pltpu.VMEM((rows, width), bf16),
            pltpu.VMEM((rows, width), bf16),
            pltpu.VMEM((5, 4, rows, hidden), bf16),
            pltpu.VMEM((4, rows, cols), f32),
            pltpu.VMEM((4, rows, cols), bf16),
            pltpu.VMEM((5, rows, cols), bf16),
            pltpu.VMEM((rows, cols), f32),
            pltpu.VMEM((rows, cols), bf16),
            dma((len(arguments) - 1,)),
            dma((4,)),
            dma((PARTS,)),
            dma((3,)),
            dma((4,)),
            dma((blocks, 2)),
            dma((PARTS,)),
            dma((4, 2, PARTS)),
            dma((4, blocks)),
            dma((5, 2, blocks)),
            dma((5, PARTS)),
        ],
        compiler_params=pltpu.CompilerParams(collective_id=0, has_side_effects=True),
    )(
        residual,
        queries,
        keys,
        values,
        segments[None, :],
        routes.T,
        route_weight.T,
        sinks,
        out_weight,
        norm_gain[None, :],
        expert_gate,
        expert_up,
        expert_down,
        shared_gate,
        shared_up,
        shared_down,
    )


def solution(mesh):
    placed = (
        P(("grp", "sp"), None),
        P(("grp", "sp"), "tp"),
        P(("grp", "sp"), "tp"),
        P(("grp", "sp"), "tp"),
        P(("grp", "sp")),
        P(("grp", "sp"), None),
        P(("grp", "sp"), None),
        P("tp"),
        P("tp", None),
        P(),
        P("sp", None, "tp"),
        P("sp", None, "tp"),
        P("sp", None, "tp"),
        P(None, "tp"),
        P(None, "tp"),
        P(None, "tp"),
    )
    return jax.shard_map(
        layer, mesh=mesh, in_specs=placed, out_specs=P(("grp", "sp"), "tp"), check_vma=False
    )
```

```python
import functools
import math
import jax
import jax.numpy as jnp
from jax import lax
from jax.experimental import pallas as pl
from jax.experimental.pallas import tpu as pltpu
from jax.sharding import PartitionSpec as P

HEAD_DIM = 64
WINDOW = 128


epsilon = 1e-06


def passed_along(value, axis, steps):
    count = lax.axis_size(axis)
    leading, last = (max(0, -steps), min(count, count - steps))
    return lax.ppermute(value, axis, [(source, source + steps) for source in range(leading, last)])


def banded(prev_rows, own_rows, window_len):
    blocks = own_rows.shape[0] // window_len
    joined = jnp.concatenate([prev_rows, own_rows], axis=0)
    shaped = joined.reshape((blocks + 1, window_len) + own_rows.shape[1:])
    return jnp.concatenate([shaped[:-1], shaped[1:]], axis=1)


def shards(
    residual,
    queries,
    keys,
    values,
    segments,
    routes,
    route_weight,
    sinks,
    out_weight,
    norm_gain,
    expert_gate,
    expert_up,
    expert_down,
    shared_gate,
    shared_up,
    shared_down,
):
    rows_here = residual.shape[0]
    model_width = residual.shape[1]
    tp_count = lax.axis_size("tp")
    tp_index = lax.axis_index("tp")
    head_local = queries.shape[1] // HEAD_DIM
    kv_local = keys.shape[1] // HEAD_DIM
    group_size = head_local // kv_local
    window_len = WINDOW
    blocks = rows_here // window_len
    own_marks = (segments % 256 + 1).astype(jnp.bfloat16)
    prev_keys, prev_values, prev_marks = passed_along(
        (
            keys[rows_here - window_len :],
            values[rows_here - window_len :],
            own_marks[rows_here - window_len :],
        ),
        "sp",
        1,
    )
    key_band = banded(prev_keys, keys, window_len).reshape(
        blocks, 2 * window_len, kv_local, HEAD_DIM
    )
    value_band = banded(prev_values, values, window_len).reshape(
        blocks, 2 * window_len, kv_local, HEAD_DIM
    )
    mark_band = banded(prev_marks, own_marks, window_len).astype(jnp.float32)
    query_marks = own_marks.reshape(blocks, window_len).astype(jnp.float32)
    query_blocks = queries.reshape(blocks, window_len, kv_local, group_size, HEAD_DIM)
    scores = jnp.einsum(
        "nqhgd,nkhd->nhgqk", query_blocks, key_band, preferred_element_type=jnp.float32
    ) * HEAD_DIM ** (-0.5)
    offsets = jnp.arange(window_len)[:, None] + window_len - jnp.arange(2 * window_len)[None, :]
    allowed = (
        (offsets >= 0) & (offsets < window_len) & (query_marks[:, :, None] == mark_band[:, None, :])
    )
    sink_logits = sinks.reshape(kv_local, group_size)[None, :, :, None]
    masked = jnp.where(allowed[:, None, None], scores, -jnp.inf)
    top_score = jnp.maximum(jnp.max(masked, axis=-1), sink_logits)
    exp_terms = jnp.where(allowed[:, None, None], jnp.exp(scores - top_score[..., None]), 0.0)
    denominator = jnp.sum(exp_terms, axis=-1) + jnp.exp(sink_logits - top_score)
    probabilities = (exp_terms / denominator[..., None]).astype(jnp.bfloat16)
    attended = jnp.einsum(
        "nhgqk,nkhd->nqhgd", probabilities, value_band, preferred_element_type=jnp.float32
    )
    attended = attended.astype(jnp.bfloat16).reshape(rows_here, head_local * HEAD_DIM)
    partial_value = jnp.dot(attended, out_weight, preferred_element_type=jnp.float32)
    col_width = model_width // tp_count
    col_start = tp_index * col_width
    summed = lax.psum(partial_value, "tp")
    updated = (residual.astype(jnp.float32) + summed).astype(jnp.bfloat16)
    updated_f32 = updated.astype(jnp.float32)
    inv_rms = lax.rsqrt(jnp.mean(updated_f32 * updated_f32, axis=-1, keepdims=True) + epsilon)
    normed = (updated_f32 * inv_rms * norm_gain).astype(jnp.bfloat16)
    updated_cols = lax.dynamic_slice_in_dim(updated, col_start, col_width, 1)
    normed_cols = lax.dynamic_slice_in_dim(normed, col_start, col_width, 1)
    shared_pre = jnp.dot(normed, shared_gate, preferred_element_type=jnp.float32)
    shared_lin = jnp.dot(normed, shared_up, preferred_element_type=jnp.float32)
    shared_act = (jax.nn.silu(shared_pre) * shared_lin).astype(jnp.bfloat16)
    top_count = routes.shape[1]
    experts = lax.axis_size("sp")
    capacity = 2 * rows_here * top_count // experts
    flat_ids = routes.reshape(-1)
    one_hot = (flat_ids[:, None] == jnp.arange(experts, dtype=jnp.int32)[None, :]).astype(jnp.int32)
    rank_in = jnp.cumsum(one_hot, axis=0) - one_hot
    slot_dest = flat_ids * capacity + jnp.sum(rank_in * one_hot, axis=1)
    token_of = jnp.arange(rows_here * top_count, dtype=jnp.int32) // top_count
    slot_token = jnp.full((experts * capacity,), -1, jnp.int32).at[slot_dest].set(token_of)
    filled = slot_token >= 0
    safe_token = jnp.where(filled, slot_token, 0)
    outgoing = jnp.where(filled[:, None], normed_cols[safe_token], jnp.zeros((), jnp.bfloat16))
    pieces = lax.all_to_all(
        outgoing.reshape(experts, capacity, col_width),
        "sp",
        split_axis=0,
        concat_axis=0,
        tiled=True,
    )
    arrived = lax.all_gather(pieces, "tp", axis=2, tiled=True)
    expert_rows = arrived.reshape(-1, model_width)
    gate_pre = jnp.dot(expert_rows, expert_gate[0], preferred_element_type=jnp.float32)
    up_lin = jnp.dot(expert_rows, expert_up[0], preferred_element_type=jnp.float32)
    expert_act = (jax.nn.silu(gate_pre) * up_lin).astype(jnp.bfloat16)
    gathered_expert, gathered_shared = (
        lax.all_gather(expert_act, "tp", axis=1, tiled=True),
        lax.all_gather(shared_act, "tp", axis=1, tiled=True),
    )
    expert_out = jnp.dot(
        gathered_expert, expert_down[0], preferred_element_type=jnp.float32
    ).astype(jnp.bfloat16)
    returned = lax.all_to_all(
        expert_out.reshape(experts, capacity, col_width),
        "sp",
        split_axis=0,
        concat_axis=0,
        tiled=True,
    )
    returned = returned.reshape(experts * capacity, col_width)
    picked = returned[slot_dest].astype(jnp.float32).reshape(rows_here, top_count, col_width)
    routed = jnp.sum(picked * route_weight[:, :, None], axis=1)
    shared_cols = jnp.dot(gathered_shared, shared_down, preferred_element_type=jnp.float32)
    return (updated_cols.astype(jnp.float32) + shared_cols + routed).astype(jnp.bfloat16)


MESH = pl.DeviceIdType.MESH
PARTS = 4
OWN = (0, 1)
E, M, B = 0, 1, 2
ALONG = {
    (E, 1): (0, 1),
    (E, 2): (1,),
    (E, 3): (2,),
    (M, 0): (0, 1, 2, 3),
    (M, 2): (1, 2),
    (M, 3): (),
}


def fused_kernel(
    dims,
    res_hbm,
    q_hbm,
    k_hbm,
    v_hbm,
    seg_hbm,
    routes_hbm,
    rw_hbm,
    sinks_ref,
    wo_hbm,
    gain_hbm,
    eg_hbm,
    eu_hbm,
    ed_hbm,
    sg_hbm,
    su_hbm,
    sd_hbm,
    result,
    q_ref,
    k_ref,
    v_ref,
    seg_ref,
    routes_ref,
    rw_ref,
    gain_ref,
    res_v,
    wo_v,
    gu_v,
    sgu_v,
    dn_v,
    sdn_v,
    kh,
    vh,
    mh,
    marks_own,
    marks_v,
    wx,
    att,
    b1s,
    b1r,
    b2s,
    b2r,
    keep,
    upd,
    norm_v,
    norm_h,
    act,
    tot,
    ret,
    rin,
    acc,
    w_sem,
    sent_s,
    halo_r,
    x_r,
    b_r,
    c_r,
    u_r,
    m_r,
    a_r,
    e_r,
):
    rows, cols, width, window, hidden, heads, group = dims
    bf16, f32 = jnp.bfloat16, jnp.float32
    s = lax.axis_index("sp")
    t = lax.axis_index("tp")
    core = t % 2
    chip = t // 2
    mate = t + 1 - 2 * core
    over = t + 2 - 4 * chip
    diag = 3 - t
    side = s // 2
    middle = ((s + 1) // 2) % 2
    is_mid = middle == 1
    is_end = middle == 0
    inner = s + 1 - 2 * side
    outer = (s + 3 + 2 * side) % 4

    def index_of(block):
        end, mid = block
        b = end + middle * (mid - end)
        return b + side * (3 - 2 * b)

    roles = (is_end, is_mid, None)
    sent = [0, 0, 0]

    def remote(src, dst, recv, sp, tp, role=B):
        return pltpu.make_async_remote_copy(
            src_ref=src,
            dst_ref=dst,
            send_sem=sent_s.at[role],
            recv_sem=recv,
            device_id={"sp": sp, "tp": tp},
            device_id_type=MESH,
        )

    def count(copy, role):
        width_of = 2 if copy.src_ref.dtype == bf16 else 4
        sent[role] += math.prod(copy.src_ref.shape) * width_of

    def go(copy, role=B):
        if role == B:
            copy.start()
        else:

            @pl.when(roles[role])
            def _():
                copy.start()

        count(copy, role)

    barrier = pltpu.get_barrier_semaphore()
    for sp, tp in ((s, mate), (s, over), (inner, t)):
        pl.semaphore_signal(barrier, inc=1, device_id={"sp": sp, "tp": tp}, device_id_type=MESH)

    @pl.when(is_mid)
    def _():
        pl.semaphore_signal(barrier, inc=1, device_id={"sp": outer, "tp": t}, device_id_type=MESH)

    own_cols = pl.ds(pl.multiple_of(t * cols, cols), cols)
    first_half = pl.ds(0, hidden)
    second_half = pl.ds(hidden, hidden)
    sources = dict(
        seg=(seg_hbm, seg_ref),
        k=(k_hbm, k_ref),
        q=(q_hbm, q_ref),
        v=(v_hbm, v_ref),
        routes=(routes_hbm, routes_ref),
        rw=(rw_hbm, rw_ref),
        wo=(wo_hbm, wo_v),
        res=(res_hbm.at[:, own_cols], res_v),
        gain=(gain_hbm, gain_ref),
        eg=(eg_hbm.at[0], gu_v.at[:, first_half]),
        eu=(eu_hbm.at[0], gu_v.at[:, second_half]),
        sg=(sg_hbm, sgu_v.at[:, first_half]),
        su=(su_hbm, sgu_v.at[:, second_half]),
        ed=(ed_hbm.at[0], dn_v),
        sd=(sd_hbm, sdn_v),
    )
    loads = {
        name: pltpu.make_async_copy(src, dst, w_sem.at[i])
        for i, (name, (src, dst)) in enumerate(sources.items())
    }
    for load in loads.values():
        load.start()

    def loaded(*names):
        for name in names:
            loads[name].wait()

    tail = pl.ds(rows - window, window)
    up_sp = (s + 1) % 4
    halos = [
        remote(k_ref.at[tail], kh, halo_r.at[0], up_sp, t, 3),
        remote(v_ref.at[tail], vh, halo_r.at[1], up_sp, t, 3),
        remote(marks_v, mh, halo_r.at[2], up_sp, t, 3),
    ]

    @pl.when(s == 0)
    def _():
        kh[...] = jnp.zeros_like(kh)
        vh[...] = jnp.zeros_like(vh)
        mh[...] = jnp.full(mh.shape, -1.0, f32)

    loaded("seg")
    marks_own[...] = jnp.broadcast_to(seg_ref[...].astype(f32), marks_own.shape)
    marks_v[...] = marks_own[:, tail]

    def down_rows(row):
        return jnp.transpose(jnp.broadcast_to(row, (window, window)))

    q_pos = lax.broadcasted_iota(jnp.int32, (window, window), 0)
    k_pos = lax.broadcasted_iota(jnp.int32, (window, window), 1)

    def attend(n):
        here = pl.ds(n * window, window)
        if n == 0:
            k_prev, v_prev, m_prev = kh, vh, mh[0:1, :]
            before = slice(None)
        else:
            before = pl.ds((n - 1) * window, window)
            k_prev, v_prev, m_prev = k_ref, v_ref, marks_own[0:1, before]
        m_own = marks_own[0:1, here]
        marks = down_rows(m_own)
        ok_prev = (k_pos > q_pos) & (marks == m_prev)
        ok_own = (k_pos <= q_pos) & (marks == m_own)
        contract = (((1,), (1,)), ((), ()))
        every = range(heads)
        kv = [slice((h // group) * HEAD_DIM, (h // group + 1) * HEAD_DIM) for h in every]
        scores = []
        for h in every:
            qh = q_ref[here, h * HEAD_DIM : (h + 1) * HEAD_DIM]
            pair = [
                lax.dot_general(qh, k, contract, preferred_element_type=f32) * HEAD_DIM ** (-0.5)
                for k in (k_prev[before, kv[h]], k_ref[here, kv[h]])
            ]
            scores.append((jnp.where(ok_prev, pair[0], -jnp.inf), jnp.where(ok_own, pair[1], -jnp.inf)))
        tops = [
            jnp.maximum(jnp.max(jnp.maximum(*scores[h]), axis=-1, keepdims=True), sinks_ref[h])
            for h in every
        ]
        terms = [tuple(jnp.exp(score - tops[h]) for score in scores[h]) for h in every]
        totals = [
            jnp.sum(terms[h][0] + terms[h][1], axis=-1, keepdims=True)
            + jnp.exp(sinks_ref[h] - tops[h])
            for h in every
        ]
        for h in every:
            inverse = 1.0 / totals[h]
            p_prev, p_own = ((term * inverse).astype(bf16) for term in terms[h])
            got = jnp.dot(p_prev, v_prev[before, kv[h]], preferred_element_type=f32) + jnp.dot(
                p_own, v_ref[here, kv[h]], preferred_element_type=f32
            )
            att[here, h * HEAD_DIM : (h + 1) * HEAD_DIM] = got.astype(bf16)

    def project(n, chunk):
        where = pl.ds(pl.multiple_of(chunk * cols, cols), cols)
        return jnp.dot(
            att[pl.ds(n * window, window), :], wo_v[:, where], preferred_element_type=f32
        )

    part_rows = rows // PARTS
    per_half = window // part_rows

    def parts_of(n):
        return range(n * per_half, (n + 1) * per_half)

    def part_span(p):
        return pl.ds(p * part_rows, part_rows)

    first = {}
    second = {}

    def reduce_in_chip(n):
        for far in (1, 0):
            chunk = (over if far else t) + 1 - 2 * core
            b1s[n, far] = project(n, chunk).astype(bf16)
            copy = remote(
                b1s.at[n, far], b1r.at[n, far], b_r.at[n, far], s, mate
            )
            go(copy)
            first[n, far] = copy

    def reduce_across(n):
        mine = project(n, over)
        first[n, 1].wait_recv()
        mine = mine + b1r[n, 1].astype(f32)
        for i, p in enumerate(parts_of(n)):
            b2s[p] = mine[i * part_rows : (i + 1) * part_rows].astype(bf16)
            copy = remote(b2s.at[p], b2r.at[p], c_r.at[p], s, over)
            go(copy)
            second[p] = copy

    def hold(n):
        here = pl.ds(n * window, window)
        mine = project(n, t) + res_v[here, :].astype(f32)
        first[n, 0].wait_recv()
        keep[here, :] = mine + b1r[n, 0].astype(f32)

    def piece(b, chunk, p):
        return upd.at[b, chunk, part_span(p)]

    def share(passed, b, chunk, p, sp, tp, role=B):
        place = piece(b, chunk, p)
        return remote(place, place, u_r.at[b, passed, p], sp, tp, role)

    def to_mate(b, chunk, p, role=B):
        place = piece(b, chunk, p)
        return remote(place, place, m_r.at[b, p // per_half], s, mate, role)

    def send_own(role, far, p, passed):
        wanted = (M, 0) if role == E else (E, 1) if far else (M, 2)
        if passed and p not in ALONG[wanted]:
            return
        chunk = over if passed else t
        go(share(passed, s, chunk, p, outer if far else inner, t, role), role)

    def publish(p):
        second[p].wait_recv()
        upd[s, t, part_span(p), :] = (keep[part_span(p), :] + b2r[p].astype(f32)).astype(bf16)
        go(share(1, s, t, p, s, over))
        go(to_mate(s, t, p))

    def own_over(p):
        share(1, s, over, p, s, over).wait_recv()
        go(to_mate(s, over, p))

    def onward(block):
        return inner if block == 0 else outer

    def take(role, block, p, passed):
        b = block + side * (3 - 2 * block)
        chunk = over if passed else t
        copies = []
        if role == M and (not passed or p in ALONG[(M, 3) if block == 0 else (E, block)]):
            copies.append(share(passed, b, chunk, p, onward(block), t, role))
        if not passed and p not in ALONG[role, block]:
            copies.append(share(1, b, chunk, p, s, over, role))
        copies.append(to_mate(b, chunk, p, role))

        @pl.when(roles[role])
        def _():
            share(passed, b, chunk, p, s, mate).wait_recv()
            for copy in copies:
                copy.start()

        for copy in copies:
            count(copy, role)

    def normalize(block, n, rows_out):
        b = index_of(block)
        landed = upd.at[b, pl.ds(0, 2), pl.ds(n * window, window)]
        remote(landed, landed, m_r.at[b, n], s, mate).wait_recv()
        step = 32

        def body(i, carry):
            here = pl.ds(pl.multiple_of(n * window + i * step, step), step)
            squares = jnp.zeros((step, 1), f32)
            for chunk in range(4):
                part = upd[b, chunk, here, :].astype(f32)
                squares = squares + jnp.sum(part * part, axis=-1, keepdims=True)
            inv = lax.rsqrt(squares / width + epsilon)
            for chunk in range(4):
                part = upd[b, chunk, here, :].astype(f32)
                span = slice(chunk * cols, (chunk + 1) * cols)
                rows_out[here, span] = (part * inv * gain_ref[0:1, span]).astype(bf16)
            return carry

        lax.fori_loop(0, window // step, body, 0)

    def slot_of(block):
        return 4 if block is None else index_of(block)

    def pass_on(slot, chunk, tp, n, role=B):
        place = act.at[slot, chunk, pl.ds(n * window, window)]
        flow = 0 if tp is over else 1
        return remote(place, place, a_r.at[slot, flow, n], s, tp, role)

    def activate(block, n, normed):
        slot = slot_of(block)
        here = pl.ds(n * window, window)
        weight = sgu_v if block is None else gu_v
        both = jnp.dot(normed[here, :], weight[...], preferred_element_type=f32)
        gate, lin = both[:, :hidden], both[:, hidden:]
        act[slot, t, here, :] = (gate / (1.0 + jnp.exp(-gate)) * lin).astype(bf16)
        go(pass_on(slot, t, over, n))
        go(pass_on(slot, t, mate, n))

    def relay_act(role, block, n):
        if role == B:
            slot = s if block == 0 else 4
            pass_on(slot, over, over, n).wait_recv()
            go(pass_on(slot, over, mate, n))
        else:
            slot = block + side * (3 - 2 * block)
            copy = pass_on(slot, over, mate, n, role)

            @pl.when(roles[role])
            def _():
                pass_on(slot, over, over, n).wait_recv()
                copy.start()

            count(copy, role)

    def contract_act(block, n):
        slot = slot_of(block)
        weight = sdn_v if block is None else dn_v
        landed = act.at[slot, pl.ds(0, 2), pl.ds(n * window, window)]
        remote(landed, landed, a_r.at[slot, 1, n], s, mate).wait_recv()
        total = None
        for chunk in range(4):
            part = jnp.dot(
                act[slot, chunk, pl.ds(n * window, window), :],
                weight[chunk * hidden : (chunk + 1) * hidden, :],
                preferred_element_type=f32,
            )
            total = part if total is None else total + part
        return total

    def weighted(block, n, place, other):
        here = pl.ds(n * window, window)
        total = contract_act(block, n)
        listed = wx[index_of(block), :, here]
        row = lax.broadcasted_iota(jnp.int32, listed.shape, 0)
        column = down_rows(jnp.sum(jnp.where(row == s, listed, 0.0), axis=0, keepdims=True))
        for c in range(0, cols, window):
            value = column * total[:, c : c + window]
            if other is not None:
                value = value + other(slice(c, c + window))
            place[here, c : c + window] = value

    def back(place, b, p, sp, role=B):
        here = part_span(p)
        return remote(ret.at[b, here], rin.at[place, here], e_r.at[place, p], sp, t, role)

    def give(block, n):
        weighted(block, n, tot.at[index_of(block)], None)

    def pass_back(role, block, p):
        b = block + side * (3 - 2 * block)
        here = part_span(p)
        place = 4 if (role, block) == (E, 1) else b
        copy = back(place, b, p, outer if (role, block) == (M, 0) else inner, role)

        @pl.when(roles[role])
        def _():
            value = tot[b, here, :]
            if role == M:
                back(b, b, p, inner).wait_recv()
                value = value + rin[b, here, :].astype(f32)
            ret[b, here, :] = value.astype(bf16)
            copy.start()

        count(copy, role)

    def keep_own(n):
        here = pl.ds(n * window, window)
        weighted(OWN, n, acc, lambda c: upd[s, t, here, c].astype(f32) + acc[here, c])

    def keep_shared(n):
        acc[pl.ds(n * window, window), :] = contract_act(None, n)

    def gather_in(p):
        here = part_span(p)
        back(s, s, p, inner).wait_recv()

        @pl.when(is_mid)
        def _():
            back(4, s, p, outer).wait_recv()

        result[here, :] = (
            acc[here, :] + rin[s, here, :].astype(f32) + rin[4, here, :].astype(f32)
        ).astype(bf16)

    def weights_on(b, sp, role=B):
        return remote(wx.at[b], wx.at[b], x_r.at[b], sp, t, role)

    def take_weights(role, block):
        copy = weights_on(block + side * (3 - 2 * block), onward(block), M)

        @pl.when(roles[role])
        def _():
            copy.wait_recv()
            if role == M:
                copy.start()

        if role == M:
            count(copy, M)

    def compute(block, n):
        normalize(block, n, norm_v)
        activate(block, n, norm_v)

    def norm_own(n):
        normalize(OWN, n, norm_h)

    def act_own(n):
        activate(OWN, n, norm_h)

    def act_shared(n):
        activate(None, n, norm_h)

    def enter():
        loaded("routes", "rw")
        wx[s] = jnp.zeros(wx.shape[1:], f32)
        for e in range(4):
            weight = jnp.zeros((1, rows), f32)
            for k in range(routes_ref.shape[0]):
                named = routes_ref[k : k + 1, :] == e
                weight = weight + jnp.where(named, rw_ref[k : k + 1, :], 0.0)
            wx[s, e : e + 1, :] = weight
        pl.semaphore_wait(barrier, 3 + middle)

        @pl.when(s < 3)
        def _():
            for copy in halos:
                copy.start()

        go(weights_on(s, inner))
        go(weights_on(s, outer, M), M)
        loaded("wo")

    def clear():
        @pl.when(is_end)
        def _():
            rin[4] = jnp.zeros(rin.shape[1:], bf16)

    def halo():
        @pl.when(s > 0)
        def _():
            for copy in halos:
                copy.wait_recv()

    loaded("k", "q", "v")
    attend(1)
    enter()
    reduce_in_chip(1)
    loaded("res")
    reduce_across(1)
    hold(1)
    take_weights(M, 2)
    halo()
    attend(0)
    reduce_in_chip(0)
    take_weights(M, 0)
    reduce_across(0)
    publish(2)
    clear()
    send_own(E, 0, 2, 0)
    send_own(M, 0, 2, 0)
    loaded("gain", "eg", "eu", "sg", "su", "ed", "sd")
    send_own(M, 1, 2, 0)
    hold(0)
    publish(3)
    send_own(E, 0, 3, 0)
    send_own(M, 0, 3, 0)
    send_own(M, 1, 3, 0)
    take(M, 0, 2, 0)
    take_weights(M, 3)
    publish(0)
    take(M, 2, 2, 0)
    take(M, 0, 3, 0)
    take(M, 2, 3, 0)
    take(M, 0, 0, 0)
    take(M, 3, 2, 0)
    send_own(E, 0, 0, 0)
    publish(1)
    take(M, 0, 1, 0)
    send_own(E, 0, 1, 0)
    take(E, 1, 2, 0)
    own_over(2)
    take(M, 3, 3, 0)
    send_own(M, 0, 0, 0)
    send_own(E, 0, 2, 1)
    own_over(3)
    own_over(0)
    send_own(E, 0, 0, 1)
    take(E, 2, 2, 0)
    take(M, 3, 0, 0)
    take(E, 2, 3, 0)
    take(M, 3, 1, 0)
    take(M, 0, 2, 1)
    take_weights(E, 1)
    take_weights(E, 3)
    take(M, 2, 3, 1)
    send_own(M, 0, 1, 0)
    take(M, 3, 2, 1)
    send_own(M, 0, 2, 1)
    take(E, 1, 3, 0)
    take(M, 2, 0, 0)
    own_over(1)
    send_own(M, 0, 1, 1)
    norm_own(1)
    take(E, 2, 2, 1)
    send_own(E, 0, 3, 1)
    take_weights(E, 2)
    take(E, 1, 2, 1)
    send_own(M, 1, 1, 1)
    take(E, 3, 3, 0)
    take(E, 2, 3, 1)
    take(M, 3, 3, 1)
    take(E, 3, 0, 0)
    send_own(M, 1, 0, 1)
    take(M, 0, 0, 1)
    take(E, 3, 1, 0)
    take(M, 0, 3, 1)
    compute((2, 3), 1)
    take(E, 3, 2, 0)
    norm_own(0)
    take(E, 3, 2, 1)
    take(M, 2, 2, 1)
    take(E, 3, 3, 1)
    take(E, 3, 0, 1)
    take(M, 2, 1, 0)
    take(M, 2, 1, 1)
    take(E, 1, 3, 1)
    take(E, 2, 0, 0)
    send_own(M, 1, 1, 0)
    take(M, 3, 1, 1)
    compute((3, 0), 1)
    take(E, 3, 1, 1)
    send_own(M, 1, 0, 0)
    compute((1, 2), 1)
    relay_act(E, 2, 1)
    take(M, 3, 0, 1)
    send_own(E, 0, 1, 1)
    compute((3, 3), 0)
    relay_act(M, 3, 1)
    give((2, 3), 1)
    pass_back(E, 2, 3)
    pass_back(E, 2, 2)
    take(E, 2, 0, 1)
    act_shared(0)
    relay_act(M, 2, 1)
    relay_act(E, 3, 1)
    take(M, 2, 0, 1)
    take(E, 2, 1, 0)
    take(E, 2, 1, 1)
    take(E, 1, 1, 1)
    act_own(1)
    take(M, 0, 1, 1)
    give((3, 2), 1)
    pass_back(E, 3, 3)
    relay_act(M, 3, 0)
    compute((2, 0), 0)
    relay_act(E, 3, 0)
    pass_back(E, 3, 2)
    pass_back(M, 2, 2)
    take(E, 1, 0, 0)
    relay_act(M, 0, 1)
    take(E, 1, 0, 1)
    take(E, 1, 1, 0)
    give((3, 3), 0)
    pass_back(E, 3, 1)
    relay_act(E, 1, 1)
    pass_back(M, 3, 3)
    pass_back(E, 3, 0)
    compute((1, 2), 0)
    pass_back(M, 3, 2)
    give((1, 0), 1)
    pass_back(E, 1, 2)
    relay_act(E, 2, 0)
    relay_act(M, 0, 0)
    relay_act(B, 1, 0)
    pass_back(M, 3, 1)
    act_own(0)
    give((2, 0), 0)
    pass_back(E, 2, 1)
    pass_back(M, 0, 3)
    relay_act(E, 1, 0)
    pass_back(M, 3, 0)
    pass_back(E, 2, 0)
    act_shared(1)
    relay_act(M, 2, 0)
    pass_back(M, 0, 2)
    pass_back(M, 2, 3)
    give((1, 2), 0)
    pass_back(E, 1, 3)
    pass_back(M, 0, 1)
    pass_back(M, 2, 1)
    pass_back(E, 1, 1)
    keep_shared(0)
    relay_act(B, 0, 0)
    pass_back(M, 0, 0)
    pass_back(M, 2, 0)
    relay_act(B, 1, 1)
    pass_back(E, 1, 0)
    relay_act(B, 0, 1)
    keep_shared(1)
    keep_own(0)
    keep_own(1)
    gather_in(3)
    gather_in(1)
    gather_in(2)
    gather_in(0)

    def settle(size, sem):
        for unit in (upd.at[0], upd.at[0, 0], piece(0, 0, 0), wx.at[0]):
            of_one = math.prod(unit.shape) * (4 if unit.dtype == f32 else 2)
            for _ in range(size // of_one):
                pltpu.make_async_copy(unit, unit, sem).wait()
            size = size % of_one

    settle(sent[B], sent_s.at[B])

    @pl.when(is_end)
    def _():
        settle(sent[E], sent_s.at[E])

    @pl.when(is_mid)
    def _():
        settle(sent[M], sent_s.at[M])

    @pl.when(s < 3)
    def _():
        for copy in halos:
            copy.wait_send()


def layer(
    residual,
    queries,
    keys,
    values,
    segments,
    routes,
    route_weight,
    sinks,
    out_weight,
    norm_gain,
    expert_gate,
    expert_up,
    expert_down,
    shared_gate,
    shared_up,
    shared_down,
):
    arguments = (
        residual,
        queries,
        keys,
        values,
        segments,
        routes,
        route_weight,
        sinks,
        out_weight,
        norm_gain,
        expert_gate,
        expert_up,
        expert_down,
        shared_gate,
        shared_up,
        shared_down,
    )
    rows, width = residual.shape
    n_sp, n_tp = lax.axis_size("sp"), lax.axis_size("tp")
    capacity = 2 * rows * routes.shape[1] // n_sp
    hidden = expert_gate.shape[2]
    if n_sp != 4 or n_tp != 4 or capacity < rows or rows != 2 * WINDOW or shared_gate.shape[1] != hidden:
        return shards(*arguments)
    cols = width // n_tp
    heads = queries.shape[1] // HEAD_DIM
    group = queries.shape[1] // keys.shape[1]
    kv_width = keys.shape[1]
    blocks = rows // WINDOW
    bf16, f32 = jnp.bfloat16, jnp.float32
    vmem = pl.BlockSpec(memory_space=pltpu.VMEM)
    anywhere = pl.BlockSpec(memory_space=pl.ANY)
    dma = pltpu.SemaphoreType.DMA
    piece = rows // PARTS
    return pl.pallas_call(
        functools.partial(fused_kernel, (rows, cols, width, WINDOW, hidden, heads, group)),
        out_shape=pltpu.VMEM((rows, cols), bf16),
        in_specs=[anywhere] * 7 + [pl.BlockSpec(memory_space=pltpu.SMEM)] + [anywhere] * 8,
        out_specs=vmem,
        scratch_shapes=[
            pltpu.VMEM(queries.shape, bf16),
            pltpu.VMEM(keys.shape, bf16),
            pltpu.VMEM(values.shape, bf16),
            pltpu.VMEM((1, rows), jnp.int32),
            pltpu.VMEM(routes.shape[::-1], jnp.int32),
            pltpu.VMEM(routes.shape[::-1], f32),
            pltpu.VMEM((1, width), f32),
            pltpu.VMEM((rows, cols), bf16),
            pltpu.VMEM(out_weight.shape, bf16),
            pltpu.VMEM((width, 2 * hidden), bf16),
            pltpu.VMEM((width, 2 * hidden), bf16),
            pltpu.VMEM(expert_down.shape[1:], bf16),
            pltpu.VMEM(shared_down.shape, bf16),
            pltpu.VMEM((WINDOW, kv_width), bf16),
            pltpu.VMEM((WINDOW, kv_width), bf16),
            pltpu.VMEM((8, WINDOW), f32),
            pltpu.VMEM((8, rows), f32),
            pltpu.VMEM((8, WINDOW), f32),
            pltpu.VMEM((4, 8, rows), f32),
            pltpu.VMEM((rows, heads * HEAD_DIM), bf16),
            pltpu.VMEM((blocks, 2, WINDOW, cols), bf16),
            pltpu.VMEM((blocks, 2, WINDOW, cols), bf16),
            pltpu.VMEM((PARTS, piece, cols), bf16),
            pltpu.VMEM((PARTS, piece, cols), bf16),
            pltpu.VMEM((rows, cols), f32),
            pltpu.VMEM((4, 4, rows, cols), bf16),
            pltpu.VMEM((rows, width), bf16),
            pltpu.VMEM((rows, width), bf16),
            pltpu.VMEM((5, 4, rows, hidden), bf16),
            pltpu.VMEM((4, rows, cols), f32),
            pltpu.VMEM((4, rows, cols), bf16),
            pltpu.VMEM((5, rows, cols), bf16),
            pltpu.VMEM((rows, cols), f32),
            dma((len(arguments) - 1,)),
            dma((4,)),
            dma((3,)),
            dma((4,)),
            dma((blocks, 2)),
            dma((PARTS,)),
            dma((4, 2, PARTS)),
            dma((4, blocks)),
            dma((5, 2, blocks)),
            dma((5, PARTS)),
        ],
        compiler_params=pltpu.CompilerParams(collective_id=0, has_side_effects=True),
    )(
        residual,
        queries,
        keys,
        values,
        segments[None, :],
        routes.T,
        route_weight.T,
        sinks,
        out_weight,
        norm_gain[None, :],
        expert_gate,
        expert_up,
        expert_down,
        shared_gate,
        shared_up,
        shared_down,
    )


def solution(mesh):
    placed = (
        P(("grp", "sp"), None),
        P(("grp", "sp"), "tp"),
        P(("grp", "sp"), "tp"),
        P(("grp", "sp"), "tp"),
        P(("grp", "sp")),
        P(("grp", "sp"), None),
        P(("grp", "sp"), None),
        P("tp"),
        P("tp", None),
        P(),
        P("sp", None, "tp"),
        P("sp", None, "tp"),
        P("sp", None, "tp"),
        P(None, "tp"),
        P(None, "tp"),
        P(None, "tp"),
    )
    return jax.shard_map(
        layer, mesh=mesh, in_specs=placed, out_specs=P(("grp", "sp"), "tp"), check_vma=False
    )
```

```python
import functools
import math
import jax
import jax.numpy as jnp
from jax import lax
from jax.experimental import pallas as pl
from jax.experimental.pallas import tpu as pltpu
from jax.sharding import PartitionSpec as P

HEAD_DIM = 64
WINDOW = 128


epsilon = 1e-06


def passed_along(value, axis, steps):
    count = lax.axis_size(axis)
    leading, last = (max(0, -steps), min(count, count - steps))
    return lax.ppermute(value, axis, [(source, source + steps) for source in range(leading, last)])


def banded(prev_rows, own_rows, window_len):
    blocks = own_rows.shape[0] // window_len
    joined = jnp.concatenate([prev_rows, own_rows], axis=0)
    shaped = joined.reshape((blocks + 1, window_len) + own_rows.shape[1:])
    return jnp.concatenate([shaped[:-1], shaped[1:]], axis=1)


def shards(
    residual,
    queries,
    keys,
    values,
    segments,
    routes,
    route_weight,
    sinks,
    out_weight,
    norm_gain,
    expert_gate,
    expert_up,
    expert_down,
    shared_gate,
    shared_up,
    shared_down,
):
    rows_here = residual.shape[0]
    model_width = residual.shape[1]
    tp_count = lax.axis_size("tp")
    tp_index = lax.axis_index("tp")
    head_local = queries.shape[1] // HEAD_DIM
    kv_local = keys.shape[1] // HEAD_DIM
    group_size = head_local // kv_local
    window_len = WINDOW
    blocks = rows_here // window_len
    own_marks = (segments % 256 + 1).astype(jnp.bfloat16)
    prev_keys, prev_values, prev_marks = passed_along(
        (
            keys[rows_here - window_len :],
            values[rows_here - window_len :],
            own_marks[rows_here - window_len :],
        ),
        "sp",
        1,
    )
    key_band = banded(prev_keys, keys, window_len).reshape(
        blocks, 2 * window_len, kv_local, HEAD_DIM
    )
    value_band = banded(prev_values, values, window_len).reshape(
        blocks, 2 * window_len, kv_local, HEAD_DIM
    )
    mark_band = banded(prev_marks, own_marks, window_len).astype(jnp.float32)
    query_marks = own_marks.reshape(blocks, window_len).astype(jnp.float32)
    query_blocks = queries.reshape(blocks, window_len, kv_local, group_size, HEAD_DIM)
    scores = jnp.einsum(
        "nqhgd,nkhd->nhgqk", query_blocks, key_band, preferred_element_type=jnp.float32
    ) * HEAD_DIM ** (-0.5)
    offsets = jnp.arange(window_len)[:, None] + window_len - jnp.arange(2 * window_len)[None, :]
    allowed = (
        (offsets >= 0) & (offsets < window_len) & (query_marks[:, :, None] == mark_band[:, None, :])
    )
    sink_logits = sinks.reshape(kv_local, group_size)[None, :, :, None]
    masked = jnp.where(allowed[:, None, None], scores, -jnp.inf)
    top_score = jnp.maximum(jnp.max(masked, axis=-1), sink_logits)
    exp_terms = jnp.where(allowed[:, None, None], jnp.exp(scores - top_score[..., None]), 0.0)
    denominator = jnp.sum(exp_terms, axis=-1) + jnp.exp(sink_logits - top_score)
    probabilities = (exp_terms / denominator[..., None]).astype(jnp.bfloat16)
    attended = jnp.einsum(
        "nhgqk,nkhd->nqhgd", probabilities, value_band, preferred_element_type=jnp.float32
    )
    attended = attended.astype(jnp.bfloat16).reshape(rows_here, head_local * HEAD_DIM)
    partial_value = jnp.dot(attended, out_weight, preferred_element_type=jnp.float32)
    col_width = model_width // tp_count
    col_start = tp_index * col_width
    summed = lax.psum(partial_value, "tp")
    updated = (residual.astype(jnp.float32) + summed).astype(jnp.bfloat16)
    updated_f32 = updated.astype(jnp.float32)
    inv_rms = lax.rsqrt(jnp.mean(updated_f32 * updated_f32, axis=-1, keepdims=True) + epsilon)
    normed = (updated_f32 * inv_rms * norm_gain).astype(jnp.bfloat16)
    updated_cols = lax.dynamic_slice_in_dim(updated, col_start, col_width, 1)
    normed_cols = lax.dynamic_slice_in_dim(normed, col_start, col_width, 1)
    shared_pre = jnp.dot(normed, shared_gate, preferred_element_type=jnp.float32)
    shared_lin = jnp.dot(normed, shared_up, preferred_element_type=jnp.float32)
    shared_act = (jax.nn.silu(shared_pre) * shared_lin).astype(jnp.bfloat16)
    top_count = routes.shape[1]
    experts = lax.axis_size("sp")
    capacity = 2 * rows_here * top_count // experts
    flat_ids = routes.reshape(-1)
    one_hot = (flat_ids[:, None] == jnp.arange(experts, dtype=jnp.int32)[None, :]).astype(jnp.int32)
    rank_in = jnp.cumsum(one_hot, axis=0) - one_hot
    slot_dest = flat_ids * capacity + jnp.sum(rank_in * one_hot, axis=1)
    token_of = jnp.arange(rows_here * top_count, dtype=jnp.int32) // top_count
    slot_token = jnp.full((experts * capacity,), -1, jnp.int32).at[slot_dest].set(token_of)
    filled = slot_token >= 0
    safe_token = jnp.where(filled, slot_token, 0)
    outgoing = jnp.where(filled[:, None], normed_cols[safe_token], jnp.zeros((), jnp.bfloat16))
    pieces = lax.all_to_all(
        outgoing.reshape(experts, capacity, col_width),
        "sp",
        split_axis=0,
        concat_axis=0,
        tiled=True,
    )
    arrived = lax.all_gather(pieces, "tp", axis=2, tiled=True)
    expert_rows = arrived.reshape(-1, model_width)
    gate_pre = jnp.dot(expert_rows, expert_gate[0], preferred_element_type=jnp.float32)
    up_lin = jnp.dot(expert_rows, expert_up[0], preferred_element_type=jnp.float32)
    expert_act = (jax.nn.silu(gate_pre) * up_lin).astype(jnp.bfloat16)
    gathered_expert, gathered_shared = (
        lax.all_gather(expert_act, "tp", axis=1, tiled=True),
        lax.all_gather(shared_act, "tp", axis=1, tiled=True),
    )
    expert_out = jnp.dot(
        gathered_expert, expert_down[0], preferred_element_type=jnp.float32
    ).astype(jnp.bfloat16)
    returned = lax.all_to_all(
        expert_out.reshape(experts, capacity, col_width),
        "sp",
        split_axis=0,
        concat_axis=0,
        tiled=True,
    )
    returned = returned.reshape(experts * capacity, col_width)
    picked = returned[slot_dest].astype(jnp.float32).reshape(rows_here, top_count, col_width)
    routed = jnp.sum(picked * route_weight[:, :, None], axis=1)
    shared_cols = jnp.dot(gathered_shared, shared_down, preferred_element_type=jnp.float32)
    return (updated_cols.astype(jnp.float32) + shared_cols + routed).astype(jnp.bfloat16)


MESH = pl.DeviceIdType.MESH
PARTS = 4
OWN = (0, 1)
E, M, B = 0, 1, 2
ALONG = {
    (E, 1): (0, 1, 3),
    (E, 2): (0,),
    (E, 3): (1,),
    (M, 0): (0, 1, 2, 3),
    (M, 2): (0, 3),
    (M, 3): (2, 3),
}


def fused_kernel(
    dims,
    res_hbm,
    q_hbm,
    k_hbm,
    v_hbm,
    seg_hbm,
    routes_hbm,
    rw_hbm,
    sinks_ref,
    wo_hbm,
    gain_hbm,
    eg_hbm,
    eu_hbm,
    ed_hbm,
    sg_hbm,
    su_hbm,
    sd_hbm,
    result,
    q_ref,
    k_ref,
    v_ref,
    seg_ref,
    routes_ref,
    rw_ref,
    gain_ref,
    res_v,
    wo_v,
    gu_v,
    sgu_v,
    dn_v,
    sdn_v,
    kh,
    vh,
    mh,
    marks_own,
    marks_v,
    wx,
    att,
    b1s,
    b1r,
    b2s,
    b2r,
    keep,
    upd,
    norm_v,
    norm_h,
    act,
    tot,
    ret,
    rin,
    acc,
    w_sem,
    sent_s,
    halo_r,
    x_r,
    b_r,
    c_r,
    u_r,
    m_r,
    a_r,
    e_r,
):
    rows, cols, width, window, hidden, heads, group = dims
    bf16, f32 = jnp.bfloat16, jnp.float32
    s = lax.axis_index("sp")
    t = lax.axis_index("tp")
    core = t % 2
    chip = t // 2
    mate = t + 1 - 2 * core
    over = t + 2 - 4 * chip
    diag = 3 - t
    side = s // 2
    middle = ((s + 1) // 2) % 2
    is_mid = middle == 1
    is_end = middle == 0
    inner = s + 1 - 2 * side
    outer = (s + 3 + 2 * side) % 4

    def index_of(block):
        end, mid = block
        b = end + middle * (mid - end)
        return b + side * (3 - 2 * b)

    roles = (is_end, is_mid, None)
    sent = [0, 0, 0]

    def remote(src, dst, recv, sp, tp, role=B):
        return pltpu.make_async_remote_copy(
            src_ref=src,
            dst_ref=dst,
            send_sem=sent_s.at[role],
            recv_sem=recv,
            device_id={"sp": sp, "tp": tp},
            device_id_type=MESH,
        )

    def count(copy, role):
        width_of = 2 if copy.src_ref.dtype == bf16 else 4
        sent[role] += math.prod(copy.src_ref.shape) * width_of

    def go(copy, role=B):
        if role == B:
            copy.start()
        else:

            @pl.when(roles[role])
            def _():
                copy.start()

        count(copy, role)

    barrier = pltpu.get_barrier_semaphore()
    for sp, tp in ((s, mate), (s, over), (inner, t)):
        pl.semaphore_signal(barrier, inc=1, device_id={"sp": sp, "tp": tp}, device_id_type=MESH)

    @pl.when(is_mid)
    def _():
        pl.semaphore_signal(barrier, inc=1, device_id={"sp": outer, "tp": t}, device_id_type=MESH)

    own_cols = pl.ds(pl.multiple_of(t * cols, cols), cols)
    first_half = pl.ds(0, hidden)
    second_half = pl.ds(hidden, hidden)
    sources = dict(
        seg=(seg_hbm, seg_ref),
        k=(k_hbm, k_ref),
        q=(q_hbm, q_ref),
        v=(v_hbm, v_ref),
        routes=(routes_hbm, routes_ref),
        rw=(rw_hbm, rw_ref),
        wo=(wo_hbm, wo_v),
        res=(res_hbm.at[:, own_cols], res_v),
        gain=(gain_hbm, gain_ref),
        eg=(eg_hbm.at[0], gu_v.at[:, first_half]),
        eu=(eu_hbm.at[0], gu_v.at[:, second_half]),
        sg=(sg_hbm, sgu_v.at[:, first_half]),
        su=(su_hbm, sgu_v.at[:, second_half]),
        ed=(ed_hbm.at[0], dn_v),
        sd=(sd_hbm, sdn_v),
    )
    loads = {
        name: pltpu.make_async_copy(src, dst, w_sem.at[i])
        for i, (name, (src, dst)) in enumerate(sources.items())
    }
    for load in loads.values():
        load.start()

    def loaded(*names):
        for name in names:
            loads[name].wait()

    tail = pl.ds(rows - window, window)
    up_sp = (s + 1) % 4
    halos = [
        remote(k_ref.at[tail], kh, halo_r.at[0], up_sp, t, 3),
        remote(v_ref.at[tail], vh, halo_r.at[1], up_sp, t, 3),
        remote(marks_v, mh, halo_r.at[2], up_sp, t, 3),
    ]

    @pl.when(s == 0)
    def _():
        kh[...] = jnp.zeros_like(kh)
        vh[...] = jnp.zeros_like(vh)
        mh[...] = jnp.full(mh.shape, -1.0, f32)

    loaded("seg")
    marks_own[...] = jnp.broadcast_to(seg_ref[...].astype(f32), marks_own.shape)
    marks_v[...] = marks_own[:, tail]

    def down_rows(row):
        return jnp.transpose(jnp.broadcast_to(row, (window, window)))

    q_pos = lax.broadcasted_iota(jnp.int32, (window, window), 0)
    k_pos = lax.broadcasted_iota(jnp.int32, (window, window), 1)

    def attend(n):
        here = pl.ds(n * window, window)
        if n == 0:
            k_prev, v_prev, m_prev = kh, vh, mh[0:1, :]
            before = slice(None)
        else:
            before = pl.ds((n - 1) * window, window)
            k_prev, v_prev, m_prev = k_ref, v_ref, marks_own[0:1, before]
        m_own = marks_own[0:1, here]
        marks = down_rows(m_own)
        ok_prev = (k_pos > q_pos) & (marks == m_prev)
        ok_own = (k_pos <= q_pos) & (marks == m_own)
        contract = (((1,), (1,)), ((), ()))
        every = range(heads)
        kv = [slice((h // group) * HEAD_DIM, (h // group + 1) * HEAD_DIM) for h in every]
        scores = []
        for h in every:
            qh = q_ref[here, h * HEAD_DIM : (h + 1) * HEAD_DIM]
            pair = [
                lax.dot_general(qh, k, contract, preferred_element_type=f32) * HEAD_DIM ** (-0.5)
                for k in (k_prev[before, kv[h]], k_ref[here, kv[h]])
            ]
            scores.append((jnp.where(ok_prev, pair[0], -jnp.inf), jnp.where(ok_own, pair[1], -jnp.inf)))
        tops = [
            jnp.maximum(jnp.max(jnp.maximum(*scores[h]), axis=-1, keepdims=True), sinks_ref[h])
            for h in every
        ]
        terms = [tuple(jnp.exp(score - tops[h]) for score in scores[h]) for h in every]
        totals = [
            jnp.sum(terms[h][0] + terms[h][1], axis=-1, keepdims=True)
            + jnp.exp(sinks_ref[h] - tops[h])
            for h in every
        ]
        for h in every:
            inverse = 1.0 / totals[h]
            p_prev, p_own = ((term * inverse).astype(bf16) for term in terms[h])
            got = jnp.dot(p_prev, v_prev[before, kv[h]], preferred_element_type=f32) + jnp.dot(
                p_own, v_ref[here, kv[h]], preferred_element_type=f32
            )
            att[here, h * HEAD_DIM : (h + 1) * HEAD_DIM] = got.astype(bf16)

    def project(n, chunk):
        where = pl.ds(pl.multiple_of(chunk * cols, cols), cols)
        return jnp.dot(
            att[pl.ds(n * window, window), :], wo_v[:, where], preferred_element_type=f32
        )

    part_rows = rows // PARTS
    per_half = window // part_rows

    def parts_of(n):
        return range(n * per_half, (n + 1) * per_half)

    def part_span(p):
        return pl.ds(p * part_rows, part_rows)

    first = {}
    second = {}

    def reduce_in_chip(n):
        for far in (1, 0):
            chunk = (over if far else t) + 1 - 2 * core
            b1s[n, far] = project(n, chunk).astype(bf16)
            copy = remote(
                b1s.at[n, far], b1r.at[n, far], b_r.at[n, far], s, mate
            )
            go(copy)
            first[n, far] = copy

    def reduce_across(n):
        mine = project(n, over)
        first[n, 1].wait_recv()
        mine = mine + b1r[n, 1].astype(f32)
        for i, p in enumerate(parts_of(n)):
            b2s[p] = mine[i * part_rows : (i + 1) * part_rows].astype(bf16)
            copy = remote(b2s.at[p], b2r.at[p], c_r.at[p], s, over)
            go(copy)
            second[p] = copy

    def hold(n):
        here = pl.ds(n * window, window)
        mine = project(n, t) + res_v[here, :].astype(f32)
        first[n, 0].wait_recv()
        keep[here, :] = mine + b1r[n, 0].astype(f32)

    def piece(b, chunk, p):
        return upd.at[b, chunk, part_span(p)]

    def share(passed, b, chunk, p, sp, tp, role=B):
        place = piece(b, chunk, p)
        return remote(place, place, u_r.at[b, passed, p], sp, tp, role)

    def to_mate(b, chunk, p, role=B):
        place = piece(b, chunk, p)
        return remote(place, place, m_r.at[b, p // per_half], s, mate, role)

    def send_own(role, far, p, passed):
        wanted = (M, 0) if role == E else (E, 1) if far else (M, 2)
        if passed and p not in ALONG[wanted]:
            return
        chunk = over if passed else t
        go(share(passed, s, chunk, p, outer if far else inner, t, role), role)

    def publish(p):
        second[p].wait_recv()
        upd[s, t, part_span(p), :] = (keep[part_span(p), :] + b2r[p].astype(f32)).astype(bf16)
        go(share(1, s, t, p, s, over))
        go(to_mate(s, t, p))

    def own_over(p):
        share(1, s, over, p, s, over).wait_recv()
        go(to_mate(s, over, p))

    def onward(block):
        return inner if block == 0 else outer

    def take(role, block, p, passed):
        b = block + side * (3 - 2 * block)
        chunk = over if passed else t
        copies = []
        if role == M and (not passed or p in ALONG[(M, 3) if block == 0 else (E, block)]):
            copies.append(share(passed, b, chunk, p, onward(block), t, role))
        if not passed and p not in ALONG[role, block]:
            copies.append(share(1, b, chunk, p, s, over, role))
        copies.append(to_mate(b, chunk, p, role))

        @pl.when(roles[role])
        def _():
            share(passed, b, chunk, p, s, mate).wait_recv()
            for copy in copies:
                copy.start()

        for copy in copies:
            count(copy, role)

    def normalize(block, n, rows_out):
        b = index_of(block)
        landed = upd.at[b, pl.ds(0, 2), pl.ds(n * window, window)]
        remote(landed, landed, m_r.at[b, n], s, mate).wait_recv()
        step = 32

        def body(i, carry):
            here = pl.ds(pl.multiple_of(n * window + i * step, step), step)
            squares = jnp.zeros((step, 1), f32)
            for chunk in range(4):
                part = upd[b, chunk, here, :].astype(f32)
                squares = squares + jnp.sum(part * part, axis=-1, keepdims=True)
            inv = lax.rsqrt(squares / width + epsilon)
            for chunk in range(4):
                part = upd[b, chunk, here, :].astype(f32)
                span = slice(chunk * cols, (chunk + 1) * cols)
                rows_out[here, span] = (part * inv * gain_ref[0:1, span]).astype(bf16)
            return carry

        lax.fori_loop(0, window // step, body, 0)

    def slot_of(block):
        return 4 if block is None else index_of(block)

    def pass_on(slot, chunk, tp, n, role=B):
        place = act.at[slot, chunk, pl.ds(n * window, window)]
        flow = 0 if tp is over else 1
        return remote(place, place, a_r.at[slot, flow, n], s, tp, role)

    def activate(block, n, normed):
        slot = slot_of(block)
        here = pl.ds(n * window, window)
        weight = sgu_v if block is None else gu_v
        both = jnp.dot(normed[here, :], weight[...], preferred_element_type=f32)
        gate, lin = both[:, :hidden], both[:, hidden:]
        act[slot, t, here, :] = (gate / (1.0 + jnp.exp(-gate)) * lin).astype(bf16)
        go(pass_on(slot, t, over, n))
        go(pass_on(slot, t, mate, n))

    def relay_act(role, block, n):
        if role == B:
            slot = s if block == 0 else 4
            pass_on(slot, over, over, n).wait_recv()
            go(pass_on(slot, over, mate, n))
        else:
            slot = block + side * (3 - 2 * block)
            copy = pass_on(slot, over, mate, n, role)

            @pl.when(roles[role])
            def _():
                pass_on(slot, over, over, n).wait_recv()
                copy.start()

            count(copy, role)

    def contract_act(block, n):
        slot = slot_of(block)
        weight = sdn_v if block is None else dn_v
        landed = act.at[slot, pl.ds(0, 2), pl.ds(n * window, window)]
        remote(landed, landed, a_r.at[slot, 1, n], s, mate).wait_recv()
        total = None
        for chunk in range(4):
            part = jnp.dot(
                act[slot, chunk, pl.ds(n * window, window), :],
                weight[chunk * hidden : (chunk + 1) * hidden, :],
                preferred_element_type=f32,
            )
            total = part if total is None else total + part
        return total

    def weighted(block, n, place, other):
        here = pl.ds(n * window, window)
        total = contract_act(block, n)
        listed = wx[index_of(block), :, here]
        row = lax.broadcasted_iota(jnp.int32, listed.shape, 0)
        column = down_rows(jnp.sum(jnp.where(row == s, listed, 0.0), axis=0, keepdims=True))
        for c in range(0, cols, window):
            value = column * total[:, c : c + window]
            if other is not None:
                value = value + other(slice(c, c + window))
            place[here, c : c + window] = value

    def back(place, b, p, sp, role=B):
        here = part_span(p)
        return remote(ret.at[b, here], rin.at[place, here], e_r.at[place, p], sp, t, role)

    def give(block, n):
        weighted(block, n, tot.at[index_of(block)], None)

    def pass_back(role, block, p):
        b = block + side * (3 - 2 * block)
        here = part_span(p)
        place = 4 if (role, block) == (E, 1) else b
        copy = back(place, b, p, outer if (role, block) == (M, 0) else inner, role)

        @pl.when(roles[role])
        def _():
            value = tot[b, here, :]
            if role == M:
                back(b, b, p, inner).wait_recv()
                value = value + rin[b, here, :].astype(f32)
            ret[b, here, :] = value.astype(bf16)
            copy.start()

        count(copy, role)

    def keep_own(n):
        here = pl.ds(n * window, window)
        weighted(OWN, n, acc, lambda c: upd[s, t, here, c].astype(f32) + acc[here, c])

    def keep_shared(n):
        acc[pl.ds(n * window, window), :] = contract_act(None, n)

    def gather_in(p):
        here = part_span(p)
        back(s, s, p, inner).wait_recv()

        @pl.when(is_mid)
        def _():
            back(4, s, p, outer).wait_recv()

        result[here, :] = (
            acc[here, :] + rin[s, here, :].astype(f32) + rin[4, here, :].astype(f32)
        ).astype(bf16)

    def weights_on(b, sp, role=B):
        return remote(wx.at[b], wx.at[b], x_r.at[b], sp, t, role)

    def take_weights(role, block):
        copy = weights_on(block + side * (3 - 2 * block), onward(block), M)

        @pl.when(roles[role])
        def _():
            copy.wait_recv()
            if role == M:
                copy.start()

        if role == M:
            count(copy, M)

    def compute(block, n):
        normalize(block, n, norm_v)
        activate(block, n, norm_v)

    def norm_own(n):
        normalize(OWN, n, norm_h)

    def act_own(n):
        activate(OWN, n, norm_h)

    def act_shared(n):
        activate(None, n, norm_h)

    def enter():
        loaded("routes", "rw")
        wx[s] = jnp.zeros(wx.shape[1:], f32)
        for e in range(4):
            weight = jnp.zeros((1, rows), f32)
            for k in range(routes_ref.shape[0]):
                named = routes_ref[k : k + 1, :] == e
                weight = weight + jnp.where(named, rw_ref[k : k + 1, :], 0.0)
            wx[s, e : e + 1, :] = weight
        pl.semaphore_wait(barrier, 3 + middle)

        @pl.when(s < 3)
        def _():
            for copy in halos:
                copy.start()

        go(weights_on(s, inner))
        go(weights_on(s, outer, M), M)
        loaded("wo")

    def clear():
        @pl.when(is_end)
        def _():
            rin[4] = jnp.zeros(rin.shape[1:], bf16)

    def halo():
        @pl.when(s > 0)
        def _():
            for copy in halos:
                copy.wait_recv()

    loaded("k", "q", "v")
    attend(1)
    enter()
    reduce_in_chip(1)
    reduce_across(1)
    clear()
    halo()
    attend(0)
    loaded("res")
    take_weights(M, 0)
    reduce_in_chip(0)
    hold(1)
    reduce_across(0)
    publish(2)
    send_own(M, 0, 2, 0)
    take_weights(M, 2)
    send_own(E, 0, 2, 0)
    send_own(M, 1, 2, 0)
    hold(0)
    publish(3)
    loaded("gain", "eg", "eu", "sg", "su", "ed", "sd")
    send_own(M, 0, 3, 0)
    send_own(E, 0, 3, 0)
    send_own(M, 1, 3, 0)
    take(M, 0, 2, 0)
    take_weights(M, 3)
    take(M, 2, 2, 0)
    publish(0)
    send_own(E, 0, 0, 0)
    take(M, 0, 3, 0)
    take(M, 2, 3, 0)
    take(M, 0, 0, 0)
    publish(1)
    take(M, 3, 2, 0)
    take(M, 0, 1, 0)
    send_own(M, 0, 1, 0)
    send_own(E, 0, 1, 0)
    send_own(M, 0, 0, 0)
    own_over(3)
    send_own(E, 0, 3, 1)
    take(M, 3, 3, 0)
    take(E, 1, 2, 0)
    take(M, 2, 2, 1)
    take_weights(E, 3)
    take(M, 3, 0, 0)
    own_over(0)
    own_over(2)
    send_own(M, 0, 3, 1)
    take(E, 2, 2, 0)
    send_own(E, 0, 2, 1)
    take(M, 0, 3, 1)
    take(E, 2, 3, 0)
    send_own(M, 0, 0, 1)
    take(M, 3, 1, 0)
    take(M, 0, 2, 1)
    take(E, 3, 2, 0)
    take(E, 1, 3, 0)
    take(E, 2, 2, 1)
    take(M, 2, 1, 0)
    send_own(M, 1, 3, 1)
    send_own(E, 0, 0, 1)
    take(E, 3, 3, 0)
    take(E, 2, 3, 1)
    own_over(1)
    take(E, 3, 0, 0)
    send_own(E, 0, 1, 1)
    compute((2, 0), 1)
    take(E, 3, 2, 1)
    norm_own(1)
    take(E, 1, 2, 1)
    norm_own(0)
    take(E, 3, 3, 1)
    take(M, 3, 1, 1)
    take(M, 2, 0, 0)
    take(E, 2, 1, 0)
    take(M, 2, 3, 1)
    compute((3, 2), 1)
    take(M, 0, 1, 1)
    take(M, 2, 1, 1)
    relay_act(M, 0, 1)
    take(M, 3, 0, 1)
    take_weights(E, 2)
    take(M, 2, 0, 1)
    take(E, 3, 1, 0)
    act_shared(0)
    take(M, 0, 0, 1)
    take(M, 3, 3, 1)
    take(E, 1, 3, 1)
    take(E, 3, 0, 1)
    relay_act(E, 2, 1)
    send_own(M, 1, 1, 1)
    take(E, 3, 1, 1)
    send_own(M, 1, 0, 0)
    send_own(M, 1, 1, 0)
    give((2, 0), 1)
    pass_back(E, 2, 3)
    take_weights(E, 1)
    compute((3, 3), 0)
    take(M, 3, 2, 1)
    pass_back(E, 2, 2)
    take(E, 2, 0, 0)
    take(E, 2, 1, 1)
    take(E, 2, 0, 1)
    send_own(M, 1, 0, 1)
    relay_act(E, 3, 1)
    relay_act(M, 2, 1)
    compute((1, 3), 1)
    give((3, 2), 1)
    pass_back(E, 3, 3)
    pass_back(E, 3, 2)
    compute((2, 0), 0)
    take(E, 1, 0, 0)
    relay_act(E, 3, 0)
    pass_back(M, 2, 3)
    act_shared(1)
    relay_act(M, 3, 0)
    relay_act(B, 1, 0)
    give((3, 3), 0)
    pass_back(E, 3, 0)
    pass_back(E, 3, 1)
    relay_act(M, 3, 1)
    take(E, 1, 1, 1)
    take(E, 1, 1, 0)
    relay_act(E, 1, 1)
    take(E, 1, 0, 1)
    give((1, 3), 1)
    relay_act(M, 0, 0)
    relay_act(E, 2, 0)
    pass_back(E, 1, 3)
    pass_back(M, 3, 3)
    compute((1, 2), 0)
    keep_shared(0)
    pass_back(M, 3, 2)
    relay_act(B, 1, 1)
    pass_back(M, 3, 0)
    give((2, 0), 0)
    pass_back(E, 2, 0)
    pass_back(E, 2, 1)
    pass_back(E, 1, 2)
    pass_back(M, 0, 3)
    pass_back(M, 3, 1)
    act_own(1)
    relay_act(M, 2, 0)
    relay_act(E, 1, 0)
    pass_back(M, 0, 2)
    pass_back(M, 2, 2)
    act_own(0)
    give((1, 2), 0)
    pass_back(M, 0, 0)
    pass_back(E, 1, 0)
    pass_back(M, 2, 0)
    pass_back(M, 0, 1)
    relay_act(B, 0, 1)
    pass_back(E, 1, 1)
    pass_back(M, 2, 1)
    keep_shared(1)
    relay_act(B, 0, 0)
    keep_own(1)
    keep_own(0)
    gather_in(2)
    gather_in(0)
    gather_in(3)
    gather_in(1)

    def settle(size, sem):
        for unit in (upd.at[0], upd.at[0, 0], piece(0, 0, 0), wx.at[0]):
            of_one = math.prod(unit.shape) * (4 if unit.dtype == f32 else 2)
            for _ in range(size // of_one):
                pltpu.make_async_copy(unit, unit, sem).wait()
            size = size % of_one

    settle(sent[B], sent_s.at[B])

    @pl.when(is_end)
    def _():
        settle(sent[E], sent_s.at[E])

    @pl.when(is_mid)
    def _():
        settle(sent[M], sent_s.at[M])

    @pl.when(s < 3)
    def _():
        for copy in halos:
            copy.wait_send()


def layer(
    residual,
    queries,
    keys,
    values,
    segments,
    routes,
    route_weight,
    sinks,
    out_weight,
    norm_gain,
    expert_gate,
    expert_up,
    expert_down,
    shared_gate,
    shared_up,
    shared_down,
):
    arguments = (
        residual,
        queries,
        keys,
        values,
        segments,
        routes,
        route_weight,
        sinks,
        out_weight,
        norm_gain,
        expert_gate,
        expert_up,
        expert_down,
        shared_gate,
        shared_up,
        shared_down,
    )
    rows, width = residual.shape
    n_sp, n_tp = lax.axis_size("sp"), lax.axis_size("tp")
    capacity = 2 * rows * routes.shape[1] // n_sp
    hidden = expert_gate.shape[2]
    if n_sp != 4 or n_tp != 4 or capacity < rows or rows != 2 * WINDOW or shared_gate.shape[1] != hidden:
        return shards(*arguments)
    cols = width // n_tp
    heads = queries.shape[1] // HEAD_DIM
    group = queries.shape[1] // keys.shape[1]
    kv_width = keys.shape[1]
    blocks = rows // WINDOW
    bf16, f32 = jnp.bfloat16, jnp.float32
    vmem = pl.BlockSpec(memory_space=pltpu.VMEM)
    anywhere = pl.BlockSpec(memory_space=pl.ANY)
    dma = pltpu.SemaphoreType.DMA
    piece = rows // PARTS
    return pl.pallas_call(
        functools.partial(fused_kernel, (rows, cols, width, WINDOW, hidden, heads, group)),
        out_shape=pltpu.VMEM((rows, cols), bf16),
        in_specs=[anywhere] * 7 + [pl.BlockSpec(memory_space=pltpu.SMEM)] + [anywhere] * 8,
        out_specs=vmem,
        scratch_shapes=[
            pltpu.VMEM(queries.shape, bf16),
            pltpu.VMEM(keys.shape, bf16),
            pltpu.VMEM(values.shape, bf16),
            pltpu.VMEM((1, rows), jnp.int32),
            pltpu.VMEM(routes.shape[::-1], jnp.int32),
            pltpu.VMEM(routes.shape[::-1], f32),
            pltpu.VMEM((1, width), f32),
            pltpu.VMEM((rows, cols), bf16),
            pltpu.VMEM(out_weight.shape, bf16),
            pltpu.VMEM((width, 2 * hidden), bf16),
            pltpu.VMEM((width, 2 * hidden), bf16),
            pltpu.VMEM(expert_down.shape[1:], bf16),
            pltpu.VMEM(shared_down.shape, bf16),
            pltpu.VMEM((WINDOW, kv_width), bf16),
            pltpu.VMEM((WINDOW, kv_width), bf16),
            pltpu.VMEM((8, WINDOW), f32),
            pltpu.VMEM((8, rows), f32),
            pltpu.VMEM((8, WINDOW), f32),
            pltpu.VMEM((4, 8, rows), f32),
            pltpu.VMEM((rows, heads * HEAD_DIM), bf16),
            pltpu.VMEM((blocks, 2, WINDOW, cols), bf16),
            pltpu.VMEM((blocks, 2, WINDOW, cols), bf16),
            pltpu.VMEM((PARTS, piece, cols), bf16),
            pltpu.VMEM((PARTS, piece, cols), bf16),
            pltpu.VMEM((rows, cols), f32),
            pltpu.VMEM((4, 4, rows, cols), bf16),
            pltpu.VMEM((rows, width), bf16),
            pltpu.VMEM((rows, width), bf16),
            pltpu.VMEM((5, 4, rows, hidden), bf16),
            pltpu.VMEM((4, rows, cols), f32),
            pltpu.VMEM((4, rows, cols), bf16),
            pltpu.VMEM((5, rows, cols), bf16),
            pltpu.VMEM((rows, cols), f32),
            dma((len(arguments) - 1,)),
            dma((4,)),
            dma((3,)),
            dma((4,)),
            dma((blocks, 2)),
            dma((PARTS,)),
            dma((4, 2, PARTS)),
            dma((4, blocks)),
            dma((5, 2, blocks)),
            dma((5, PARTS)),
        ],
        compiler_params=pltpu.CompilerParams(collective_id=0, has_side_effects=True),
    )(
        residual,
        queries,
        keys,
        values,
        segments[None, :],
        routes.T,
        route_weight.T,
        sinks,
        out_weight,
        norm_gain[None, :],
        expert_gate,
        expert_up,
        expert_down,
        shared_gate,
        shared_up,
        shared_down,
    )


def solution(mesh):
    placed = (
        P(("grp", "sp"), None),
        P(("grp", "sp"), "tp"),
        P(("grp", "sp"), "tp"),
        P(("grp", "sp"), "tp"),
        P(("grp", "sp")),
        P(("grp", "sp"), None),
        P(("grp", "sp"), None),
        P("tp"),
        P("tp", None),
        P(),
        P("sp", None, "tp"),
        P("sp", None, "tp"),
        P("sp", None, "tp"),
        P(None, "tp"),
        P(None, "tp"),
        P(None, "tp"),
    )
    return jax.shard_map(
        layer, mesh=mesh, in_specs=placed, out_specs=P(("grp", "sp"), "tp"), check_vma=False
    )
```

```python
import functools
import math
import jax
import jax.numpy as jnp
from jax import lax
from jax.experimental import pallas as pl
from jax.experimental.pallas import tpu as pltpu
from jax.sharding import PartitionSpec as P

HEAD_DIM = 64
WINDOW = 128


epsilon = 1e-06


def passed_along(value, axis, steps):
    count = lax.axis_size(axis)
    leading, last = (max(0, -steps), min(count, count - steps))
    return lax.ppermute(value, axis, [(source, source + steps) for source in range(leading, last)])


def banded(prev_rows, own_rows, window_len):
    blocks = own_rows.shape[0] // window_len
    joined = jnp.concatenate([prev_rows, own_rows], axis=0)
    shaped = joined.reshape((blocks + 1, window_len) + own_rows.shape[1:])
    return jnp.concatenate([shaped[:-1], shaped[1:]], axis=1)


def shards(
    residual,
    queries,
    keys,
    values,
    segments,
    routes,
    route_weight,
    sinks,
    out_weight,
    norm_gain,
    expert_gate,
    expert_up,
    expert_down,
    shared_gate,
    shared_up,
    shared_down,
):
    rows_here = residual.shape[0]
    model_width = residual.shape[1]
    tp_count = lax.axis_size("tp")
    tp_index = lax.axis_index("tp")
    head_local = queries.shape[1] // HEAD_DIM
    kv_local = keys.shape[1] // HEAD_DIM
    group_size = head_local // kv_local
    window_len = WINDOW
    blocks = rows_here // window_len
    own_marks = (segments % 256 + 1).astype(jnp.bfloat16)
    prev_keys, prev_values, prev_marks = passed_along(
        (
            keys[rows_here - window_len :],
            values[rows_here - window_len :],
            own_marks[rows_here - window_len :],
        ),
        "sp",
        1,
    )
    key_band = banded(prev_keys, keys, window_len).reshape(
        blocks, 2 * window_len, kv_local, HEAD_DIM
    )
    value_band = banded(prev_values, values, window_len).reshape(
        blocks, 2 * window_len, kv_local, HEAD_DIM
    )
    mark_band = banded(prev_marks, own_marks, window_len).astype(jnp.float32)
    query_marks = own_marks.reshape(blocks, window_len).astype(jnp.float32)
    query_blocks = queries.reshape(blocks, window_len, kv_local, group_size, HEAD_DIM)
    scores = jnp.einsum(
        "nqhgd,nkhd->nhgqk", query_blocks, key_band, preferred_element_type=jnp.float32
    ) * HEAD_DIM ** (-0.5)
    offsets = jnp.arange(window_len)[:, None] + window_len - jnp.arange(2 * window_len)[None, :]
    allowed = (
        (offsets >= 0) & (offsets < window_len) & (query_marks[:, :, None] == mark_band[:, None, :])
    )
    sink_logits = sinks.reshape(kv_local, group_size)[None, :, :, None]
    masked = jnp.where(allowed[:, None, None], scores, -jnp.inf)
    top_score = jnp.maximum(jnp.max(masked, axis=-1), sink_logits)
    exp_terms = jnp.where(allowed[:, None, None], jnp.exp(scores - top_score[..., None]), 0.0)
    denominator = jnp.sum(exp_terms, axis=-1) + jnp.exp(sink_logits - top_score)
    probabilities = (exp_terms / denominator[..., None]).astype(jnp.bfloat16)
    attended = jnp.einsum(
        "nhgqk,nkhd->nqhgd", probabilities, value_band, preferred_element_type=jnp.float32
    )
    attended = attended.astype(jnp.bfloat16).reshape(rows_here, head_local * HEAD_DIM)
    partial_value = jnp.dot(attended, out_weight, preferred_element_type=jnp.float32)
    col_width = model_width // tp_count
    col_start = tp_index * col_width
    summed = lax.psum(partial_value, "tp")
    updated = (residual.astype(jnp.float32) + summed).astype(jnp.bfloat16)
    updated_f32 = updated.astype(jnp.float32)
    inv_rms = lax.rsqrt(jnp.mean(updated_f32 * updated_f32, axis=-1, keepdims=True) + epsilon)
    normed = (updated_f32 * inv_rms * norm_gain).astype(jnp.bfloat16)
    updated_cols = lax.dynamic_slice_in_dim(updated, col_start, col_width, 1)
    normed_cols = lax.dynamic_slice_in_dim(normed, col_start, col_width, 1)
    shared_pre = jnp.dot(normed, shared_gate, preferred_element_type=jnp.float32)
    shared_lin = jnp.dot(normed, shared_up, preferred_element_type=jnp.float32)
    shared_act = (jax.nn.silu(shared_pre) * shared_lin).astype(jnp.bfloat16)
    top_count = routes.shape[1]
    experts = lax.axis_size("sp")
    capacity = 2 * rows_here * top_count // experts
    flat_ids = routes.reshape(-1)
    one_hot = (flat_ids[:, None] == jnp.arange(experts, dtype=jnp.int32)[None, :]).astype(jnp.int32)
    rank_in = jnp.cumsum(one_hot, axis=0) - one_hot
    slot_dest = flat_ids * capacity + jnp.sum(rank_in * one_hot, axis=1)
    token_of = jnp.arange(rows_here * top_count, dtype=jnp.int32) // top_count
    slot_token = jnp.full((experts * capacity,), -1, jnp.int32).at[slot_dest].set(token_of)
    filled = slot_token >= 0
    safe_token = jnp.where(filled, slot_token, 0)
    outgoing = jnp.where(filled[:, None], normed_cols[safe_token], jnp.zeros((), jnp.bfloat16))
    pieces = lax.all_to_all(
        outgoing.reshape(experts, capacity, col_width),
        "sp",
        split_axis=0,
        concat_axis=0,
        tiled=True,
    )
    arrived = lax.all_gather(pieces, "tp", axis=2, tiled=True)
    expert_rows = arrived.reshape(-1, model_width)
    gate_pre = jnp.dot(expert_rows, expert_gate[0], preferred_element_type=jnp.float32)
    up_lin = jnp.dot(expert_rows, expert_up[0], preferred_element_type=jnp.float32)
    expert_act = (jax.nn.silu(gate_pre) * up_lin).astype(jnp.bfloat16)
    gathered_expert, gathered_shared = (
        lax.all_gather(expert_act, "tp", axis=1, tiled=True),
        lax.all_gather(shared_act, "tp", axis=1, tiled=True),
    )
    expert_out = jnp.dot(
        gathered_expert, expert_down[0], preferred_element_type=jnp.float32
    ).astype(jnp.bfloat16)
    returned = lax.all_to_all(
        expert_out.reshape(experts, capacity, col_width),
        "sp",
        split_axis=0,
        concat_axis=0,
        tiled=True,
    )
    returned = returned.reshape(experts * capacity, col_width)
    picked = returned[slot_dest].astype(jnp.float32).reshape(rows_here, top_count, col_width)
    routed = jnp.sum(picked * route_weight[:, :, None], axis=1)
    shared_cols = jnp.dot(gathered_shared, shared_down, preferred_element_type=jnp.float32)
    return (updated_cols.astype(jnp.float32) + shared_cols + routed).astype(jnp.bfloat16)


MESH = pl.DeviceIdType.MESH
PARTS = 4
OWN = (0, 1)
E, M, B = 0, 1, 2
ALONG = {
    (E, 1): (0, 1, 3),
    (E, 2): (0,),
    (E, 3): (1,),
    (M, 0): (0, 1, 2, 3),
    (M, 2): (0, 3),
    (M, 3): (2, 3),
}


def fused_kernel(
    dims,
    res_hbm,
    q_hbm,
    k_hbm,
    v_hbm,
    seg_hbm,
    routes_hbm,
    rw_hbm,
    sinks_hbm,
    wo_hbm,
    gain_hbm,
    eg_hbm,
    eu_hbm,
    ed_hbm,
    sg_hbm,
    su_hbm,
    sd_hbm,
    result,
    q_ref,
    k_ref,
    v_ref,
    seg_ref,
    routes_ref,
    rw_ref,
    sinks_ref,
    gain_ref,
    res_v,
    wo_v,
    gu_v,
    sgu_v,
    dn_v,
    sdn_v,
    kh,
    vh,
    mh,
    marks_own,
    marks_v,
    wx,
    att,
    b1s,
    b1r,
    b2s,
    b2r,
    keep,
    upd,
    norm_v,
    norm_h,
    act,
    tot,
    ret,
    rin,
    acc,
    w_sem,
    sent_s,
    halo_r,
    x_r,
    b_r,
    c_r,
    u_r,
    m_r,
    a_r,
    e_r,
):
    rows, cols, width, window, hidden, heads, group = dims
    bf16, f32 = jnp.bfloat16, jnp.float32
    s = lax.axis_index("sp")
    t = lax.axis_index("tp")
    core = t % 2
    chip = t // 2
    mate = t + 1 - 2 * core
    over = t + 2 - 4 * chip
    diag = 3 - t
    side = s // 2
    middle = ((s + 1) // 2) % 2
    is_mid = middle == 1
    is_end = middle == 0
    inner = s + 1 - 2 * side
    outer = (s + 3 + 2 * side) % 4

    def index_of(block):
        end, mid = block
        b = end + middle * (mid - end)
        return b + side * (3 - 2 * b)

    roles = (is_end, is_mid, None)
    sent = [0, 0, 0]

    def remote(src, dst, recv, sp, tp, role=B):
        return pltpu.make_async_remote_copy(
            src_ref=src,
            dst_ref=dst,
            send_sem=sent_s.at[role],
            recv_sem=recv,
            device_id={"sp": sp, "tp": tp},
            device_id_type=MESH,
        )

    def count(copy, role):
        width_of = 2 if copy.src_ref.dtype == bf16 else 4
        sent[role] += math.prod(copy.src_ref.shape) * width_of

    def go(copy, role=B):
        if role == B:
            copy.start()
        else:

            @pl.when(roles[role])
            def _():
                copy.start()

        count(copy, role)

    barrier = pltpu.get_barrier_semaphore()
    for sp, tp in ((s, mate), (s, over), (inner, t)):
        pl.semaphore_signal(barrier, inc=1, device_id={"sp": sp, "tp": tp}, device_id_type=MESH)

    @pl.when(is_mid)
    def _():
        pl.semaphore_signal(barrier, inc=1, device_id={"sp": outer, "tp": t}, device_id_type=MESH)

    own_cols = pl.ds(pl.multiple_of(t * cols, cols), cols)
    first_half = pl.ds(0, hidden)
    second_half = pl.ds(hidden, hidden)
    sources = (
        ((seg_hbm, seg_ref),),
        ((k_hbm, k_ref), (q_hbm, q_ref), (v_hbm, v_ref)),
        ((sinks_hbm, sinks_ref),),
        ((routes_hbm, routes_ref),),
        ((rw_hbm, rw_ref),),
        ((wo_hbm, wo_v),),
        ((res_hbm.at[:, own_cols], res_v),),
        ((gain_hbm, gain_ref),),
        ((eg_hbm.at[0], gu_v.at[:, first_half]), (eu_hbm.at[0], gu_v.at[:, second_half])),
        ((sg_hbm, sgu_v.at[:, first_half]), (su_hbm, sgu_v.at[:, second_half])),
        ((ed_hbm.at[0], dn_v), (sd_hbm, sdn_v)),
    )
    for i, group_of in enumerate(sources):
        for src, dst in group_of:
            pltpu.make_async_copy(src, dst, w_sem.at[i]).start()
    as_large = {1: upd.at[0, 0], 8: gu_v, 9: sgu_v, 10: gu_v}

    def loaded(*which):
        for i in which:
            whole = as_large[i] if i in as_large else sources[i][0][1]
            pltpu.make_async_copy(whole, whole, w_sem.at[i]).wait()

    tail = pl.ds(rows - window, window)
    up_sp = (s + 1) % 4
    halos = [
        remote(k_ref.at[tail], kh, halo_r.at[0], up_sp, t, 3),
        remote(v_ref.at[tail], vh, halo_r.at[1], up_sp, t, 3),
        remote(marks_v, mh, halo_r.at[2], up_sp, t, 3),
    ]

    @pl.when(s == 0)
    def _():
        kh[...] = jnp.zeros_like(kh)
        vh[...] = jnp.zeros_like(vh)
        mh[...] = jnp.full(mh.shape, -1.0, f32)

    loaded(0)
    marks_own[...] = jnp.broadcast_to(seg_ref[...].astype(f32), marks_own.shape)
    marks_v[...] = marks_own[:, tail]

    def down_rows(row):
        return jnp.transpose(jnp.broadcast_to(row, (window, window)))

    q_pos = lax.broadcasted_iota(jnp.int32, (window, window), 0)
    k_pos = lax.broadcasted_iota(jnp.int32, (window, window), 1)

    def attend(n):
        here = pl.ds(n * window, window)
        if n == 0:
            k_prev, v_prev, m_prev = kh, vh, mh[0:1, :]
            before = slice(None)
        else:
            before = pl.ds((n - 1) * window, window)
            k_prev, v_prev, m_prev = k_ref, v_ref, marks_own[0:1, before]
        m_own = marks_own[0:1, here]
        marks = down_rows(m_own)
        ok_prev = (k_pos > q_pos) & (marks == m_prev)
        ok_own = (k_pos <= q_pos) & (marks == m_own)
        contract = (((1,), (1,)), ((), ()))
        every = range(heads)
        kv = [slice((h // group) * HEAD_DIM, (h // group + 1) * HEAD_DIM) for h in every]
        scores = []
        for h in every:
            qh = q_ref[here, h * HEAD_DIM : (h + 1) * HEAD_DIM]
            pair = [
                lax.dot_general(qh, k, contract, preferred_element_type=f32) * HEAD_DIM ** (-0.5)
                for k in (k_prev[before, kv[h]], k_ref[here, kv[h]])
            ]
            scores.append((jnp.where(ok_prev, pair[0], -jnp.inf), jnp.where(ok_own, pair[1], -jnp.inf)))
        tops = [
            jnp.maximum(jnp.max(jnp.maximum(*scores[h]), axis=-1, keepdims=True), sinks_ref[h])
            for h in every
        ]
        terms = [tuple(jnp.exp(score - tops[h]) for score in scores[h]) for h in every]
        totals = [
            jnp.sum(terms[h][0] + terms[h][1], axis=-1, keepdims=True)
            + jnp.exp(sinks_ref[h] - tops[h])
            for h in every
        ]
        for h in every:
            inverse = 1.0 / totals[h]
            p_prev, p_own = ((term * inverse).astype(bf16) for term in terms[h])
            got = jnp.dot(p_prev, v_prev[before, kv[h]], preferred_element_type=f32) + jnp.dot(
                p_own, v_ref[here, kv[h]], preferred_element_type=f32
            )
            att[here, h * HEAD_DIM : (h + 1) * HEAD_DIM] = got.astype(bf16)

    def project(n, chunk):
        where = pl.ds(pl.multiple_of(chunk * cols, cols), cols)
        return jnp.dot(
            att[pl.ds(n * window, window), :], wo_v[:, where], preferred_element_type=f32
        )

    part_rows = rows // PARTS
    per_half = window // part_rows

    def parts_of(n):
        return range(n * per_half, (n + 1) * per_half)

    def part_span(p):
        return pl.ds(p * part_rows, part_rows)

    first = {}
    second = {}

    def reduce_in_chip(n):
        for far in (1, 0):
            chunk = (over if far else t) + 1 - 2 * core
            b1s[n, far] = project(n, chunk).astype(bf16)
            copy = remote(
                b1s.at[n, far], b1r.at[n, far], b_r.at[n, far], s, mate
            )
            go(copy)
            first[n, far] = copy

    def reduce_across(n):
        mine = project(n, over)
        first[n, 1].wait_recv()
        mine = mine + b1r[n, 1].astype(f32)
        for i, p in enumerate(parts_of(n)):
            b2s[p] = mine[i * part_rows : (i + 1) * part_rows].astype(bf16)
            copy = remote(b2s.at[p], b2r.at[p], c_r.at[p], s, over)
            go(copy)
            second[p] = copy

    def hold(n):
        here = pl.ds(n * window, window)
        mine = project(n, t) + res_v[here, :].astype(f32)
        first[n, 0].wait_recv()
        keep[here, :] = mine + b1r[n, 0].astype(f32)

    def piece(b, chunk, p):
        return upd.at[b, chunk, part_span(p)]

    def share(passed, b, chunk, p, sp, tp, role=B):
        place = piece(b, chunk, p)
        return remote(place, place, u_r.at[b, passed, p], sp, tp, role)

    def to_mate(b, chunk, p, role=B):
        place = piece(b, chunk, p)
        return remote(place, place, m_r.at[b, p // per_half], s, mate, role)

    def send_own(role, far, p, passed):
        wanted = (M, 0) if role == E else (E, 1) if far else (M, 2)
        if passed and p not in ALONG[wanted]:
            return
        chunk = over if passed else t
        go(share(passed, s, chunk, p, outer if far else inner, t, role), role)

    def publish(p):
        second[p].wait_recv()
        upd[s, t, part_span(p), :] = (keep[part_span(p), :] + b2r[p].astype(f32)).astype(bf16)
        go(share(1, s, t, p, s, over))
        go(to_mate(s, t, p))

    def own_over(p):
        share(1, s, over, p, s, over).wait_recv()
        go(to_mate(s, over, p))

    def onward(block):
        return inner if block == 0 else outer

    def take(role, block, p, passed):
        b = block + side * (3 - 2 * block)
        chunk = over if passed else t
        copies = []
        if role == M and (not passed or p in ALONG[(M, 3) if block == 0 else (E, block)]):
            copies.append(share(passed, b, chunk, p, onward(block), t, role))
        if not passed and p not in ALONG[role, block]:
            copies.append(share(1, b, chunk, p, s, over, role))
        copies.append(to_mate(b, chunk, p, role))

        @pl.when(roles[role])
        def _():
            share(passed, b, chunk, p, s, mate).wait_recv()
            for copy in copies:
                copy.start()

        for copy in copies:
            count(copy, role)

    def normalize(block, n, rows_out):
        b = index_of(block)
        landed = upd.at[b, pl.ds(0, 2), pl.ds(n * window, window)]
        remote(landed, landed, m_r.at[b, n], s, mate).wait_recv()
        step = 32

        def body(i, carry):
            here = pl.ds(pl.multiple_of(n * window + i * step, step), step)
            squares = jnp.zeros((step, 1), f32)
            for chunk in range(4):
                part = upd[b, chunk, here, :].astype(f32)
                squares = squares + jnp.sum(part * part, axis=-1, keepdims=True)
            inv = lax.rsqrt(squares / width + epsilon)
            for chunk in range(4):
                part = upd[b, chunk, here, :].astype(f32)
                span = slice(chunk * cols, (chunk + 1) * cols)
                rows_out[here, span] = (part * inv * gain_ref[0:1, span]).astype(bf16)
            return carry

        lax.fori_loop(0, window // step, body, 0)

    def slot_of(block):
        return 4 if block is None else index_of(block)

    def pass_on(slot, chunk, tp, n, role=B):
        place = act.at[slot, chunk, pl.ds(n * window, window)]
        flow = 0 if tp is over else 1
        return remote(place, place, a_r.at[slot, flow, n], s, tp, role)

    def activate(block, n, normed):
        slot = slot_of(block)
        here = pl.ds(n * window, window)
        weight = sgu_v if block is None else gu_v
        both = jnp.dot(normed[here, :], weight[...], preferred_element_type=f32)
        gate, lin = both[:, :hidden], both[:, hidden:]
        act[slot, t, here, :] = (gate / (1.0 + jnp.exp(-gate)) * lin).astype(bf16)
        go(pass_on(slot, t, over, n))
        go(pass_on(slot, t, mate, n))

    def relay_act(role, block, n):
        if role == B:
            slot = s if block == 0 else 4
            pass_on(slot, over, over, n).wait_recv()
            go(pass_on(slot, over, mate, n))
        else:
            slot = block + side * (3 - 2 * block)
            copy = pass_on(slot, over, mate, n, role)

            @pl.when(roles[role])
            def _():
                pass_on(slot, over, over, n).wait_recv()
                copy.start()

            count(copy, role)

    def contract_act(block, n):
        slot = slot_of(block)
        weight = sdn_v if block is None else dn_v
        landed = act.at[slot, pl.ds(0, 2), pl.ds(n * window, window)]
        remote(landed, landed, a_r.at[slot, 1, n], s, mate).wait_recv()
        total = None
        for chunk in range(4):
            part = jnp.dot(
                act[slot, chunk, pl.ds(n * window, window), :],
                weight[chunk * hidden : (chunk + 1) * hidden, :],
                preferred_element_type=f32,
            )
            total = part if total is None else total + part
        return total

    def weighted(block, n, place, other):
        here = pl.ds(n * window, window)
        total = contract_act(block, n)
        listed = wx[index_of(block), :, here]
        row = lax.broadcasted_iota(jnp.int32, listed.shape, 0)
        column = down_rows(jnp.sum(jnp.where(row == s, listed, 0.0), axis=0, keepdims=True))
        for c in range(0, cols, window):
            value = column * total[:, c : c + window]
            if other is not None:
                value = value + other(slice(c, c + window))
            place[here, c : c + window] = value

    def back(place, b, p, sp, role=B):
        here = part_span(p)
        return remote(ret.at[b, here], rin.at[place, here], e_r.at[place, p], sp, t, role)

    def give(block, n):
        weighted(block, n, tot.at[index_of(block)], None)

    def pass_back(role, block, p):
        b = block + side * (3 - 2 * block)
        here = part_span(p)
        place = 4 if (role, block) == (E, 1) else b
        copy = back(place, b, p, outer if (role, block) == (M, 0) else inner, role)

        @pl.when(roles[role])
        def _():
            value = tot[b, here, :]
            if role == M:
                back(b, b, p, inner).wait_recv()
                value = value + rin[b, here, :].astype(f32)
            ret[b, here, :] = value.astype(bf16)
            copy.start()

        count(copy, role)

    def keep_own(n):
        here = pl.ds(n * window, window)
        weighted(OWN, n, acc, lambda c: upd[s, t, here, c].astype(f32) + acc[here, c])

    def keep_shared(n):
        acc[pl.ds(n * window, window), :] = contract_act(None, n)

    def gather_in(p):
        here = part_span(p)
        back(s, s, p, inner).wait_recv()

        @pl.when(is_mid)
        def _():
            back(4, s, p, outer).wait_recv()

        result[here, :] = (
            acc[here, :] + rin[s, here, :].astype(f32) + rin[4, here, :].astype(f32)
        ).astype(bf16)

    def weights_on(b, sp, role=B):
        return remote(wx.at[b], wx.at[b], x_r.at[b], sp, t, role)

    def take_weights(role, block):
        copy = weights_on(block + side * (3 - 2 * block), onward(block), M)

        @pl.when(roles[role])
        def _():
            copy.wait_recv()
            if role == M:
                copy.start()

        if role == M:
            count(copy, M)

    def compute(block, n):
        normalize(block, n, norm_v)
        activate(block, n, norm_v)

    def norm_own(n):
        normalize(OWN, n, norm_h)

    def act_own(n):
        activate(OWN, n, norm_h)

    def act_shared(n):
        activate(None, n, norm_h)

    def enter():
        loaded(3, 4)
        wx[s] = jnp.zeros(wx.shape[1:], f32)
        for e in range(4):
            weight = jnp.zeros((1, rows), f32)
            for k in range(routes_ref.shape[0]):
                named = routes_ref[k : k + 1, :] == e
                weight = weight + jnp.where(named, rw_ref[k : k + 1, :], 0.0)
            wx[s, e : e + 1, :] = weight
        pl.semaphore_wait(barrier, 3 + middle)

        @pl.when(s < 3)
        def _():
            for copy in halos:
                copy.start()

        go(weights_on(s, inner))
        go(weights_on(s, outer, M), M)
        loaded(5)

    def clear():
        @pl.when(is_end)
        def _():
            rin[4] = jnp.zeros(rin.shape[1:], bf16)

    def halo():
        @pl.when(s > 0)
        def _():
            for copy in halos:
                copy.wait_recv()

    loaded(1, 2)
    attend(1)
    enter()
    reduce_in_chip(1)
    reduce_across(1)
    clear()
    halo()
    attend(0)
    loaded(6)
    take_weights(M, 0)
    reduce_in_chip(0)
    hold(1)
    reduce_across(0)
    publish(2)
    send_own(M, 0, 2, 0)
    take_weights(M, 2)
    send_own(E, 0, 2, 0)
    send_own(M, 1, 2, 0)
    hold(0)
    publish(3)
    loaded(7, 8, 9, 10)
    send_own(M, 0, 3, 0)
    send_own(E, 0, 3, 0)
    send_own(M, 1, 3, 0)
    take(M, 0, 2, 0)
    take_weights(M, 3)
    take(M, 2, 2, 0)
    publish(0)
    send_own(E, 0, 0, 0)
    take(M, 0, 3, 0)
    take(M, 2, 3, 0)
    take(M, 0, 0, 0)
    publish(1)
    take(M, 3, 2, 0)
    take(M, 0, 1, 0)
    send_own(M, 0, 1, 0)
    send_own(E, 0, 1, 0)
    send_own(M, 0, 0, 0)
    own_over(3)
    send_own(E, 0, 3, 1)
    take(M, 3, 3, 0)
    take(E, 1, 2, 0)
    take(M, 2, 2, 1)
    take_weights(E, 3)
    take(M, 3, 0, 0)
    own_over(0)
    own_over(2)
    send_own(M, 0, 3, 1)
    take(E, 2, 2, 0)
    send_own(E, 0, 2, 1)
    take(M, 0, 3, 1)
    take(E, 2, 3, 0)
    send_own(M, 0, 0, 1)
    take(M, 3, 1, 0)
    take(M, 0, 2, 1)
    take(E, 3, 2, 0)
    take(E, 1, 3, 0)
    take(E, 2, 2, 1)
    take(M, 2, 1, 0)
    send_own(M, 1, 3, 1)
    send_own(E, 0, 0, 1)
    take(E, 3, 3, 0)
    take(E, 2, 3, 1)
    own_over(1)
    take(E, 3, 0, 0)
    send_own(E, 0, 1, 1)
    compute((2, 0), 1)
    take(E, 3, 2, 1)
    norm_own(1)
    take(E, 1, 2, 1)
    norm_own(0)
    take(E, 3, 3, 1)
    take(M, 3, 1, 1)
    take(M, 2, 0, 0)
    take(E, 2, 1, 0)
    take(M, 2, 3, 1)
    compute((3, 2), 1)
    take(M, 0, 1, 1)
    take(M, 2, 1, 1)
    relay_act(M, 0, 1)
    take(M, 3, 0, 1)
    take_weights(E, 2)
    take(M, 2, 0, 1)
    take(E, 3, 1, 0)
    act_shared(0)
    take(M, 0, 0, 1)
    take(M, 3, 3, 1)
    take(E, 1, 3, 1)
    take(E, 3, 0, 1)
    relay_act(E, 2, 1)
    send_own(M, 1, 1, 1)
    take(E, 3, 1, 1)
    send_own(M, 1, 0, 0)
    send_own(M, 1, 1, 0)
    give((2, 0), 1)
    pass_back(E, 2, 3)
    take_weights(E, 1)
    compute((3, 3), 0)
    take(M, 3, 2, 1)
    pass_back(E, 2, 2)
    take(E, 2, 0, 0)
    take(E, 2, 1, 1)
    take(E, 2, 0, 1)
    send_own(M, 1, 0, 1)
    relay_act(E, 3, 1)
    relay_act(M, 2, 1)
    compute((1, 3), 1)
    give((3, 2), 1)
    pass_back(E, 3, 3)
    pass_back(E, 3, 2)
    compute((2, 0), 0)
    take(E, 1, 0, 0)
    relay_act(E, 3, 0)
    pass_back(M, 2, 3)
    act_shared(1)
    relay_act(M, 3, 0)
    relay_act(B, 1, 0)
    give((3, 3), 0)
    pass_back(E, 3, 0)
    pass_back(E, 3, 1)
    relay_act(M, 3, 1)
    take(E, 1, 1, 1)
    take(E, 1, 1, 0)
    relay_act(E, 1, 1)
    take(E, 1, 0, 1)
    give((1, 3), 1)
    relay_act(M, 0, 0)
    relay_act(E, 2, 0)
    pass_back(E, 1, 3)
    pass_back(M, 3, 3)
    compute((1, 2), 0)
    keep_shared(0)
    pass_back(M, 3, 2)
    relay_act(B, 1, 1)
    pass_back(M, 3, 0)
    give((2, 0), 0)
    pass_back(E, 2, 0)
    pass_back(E, 2, 1)
    pass_back(E, 1, 2)
    pass_back(M, 0, 3)
    pass_back(M, 3, 1)
    act_own(1)
    relay_act(M, 2, 0)
    relay_act(E, 1, 0)
    pass_back(M, 0, 2)
    pass_back(M, 2, 2)
    act_own(0)
    give((1, 2), 0)
    pass_back(M, 0, 0)
    pass_back(E, 1, 0)
    pass_back(M, 2, 0)
    pass_back(M, 0, 1)
    relay_act(B, 0, 1)
    pass_back(E, 1, 1)
    pass_back(M, 2, 1)
    keep_shared(1)
    relay_act(B, 0, 0)
    keep_own(1)
    keep_own(0)
    gather_in(2)
    gather_in(0)
    gather_in(3)
    gather_in(1)

    def settle(size, sem):
        for unit in (upd.at[0], upd.at[0, 0], piece(0, 0, 0), wx.at[0]):
            of_one = math.prod(unit.shape) * (4 if unit.dtype == f32 else 2)
            for _ in range(size // of_one):
                pltpu.make_async_copy(unit, unit, sem).wait()
            size = size % of_one

    settle(sent[B], sent_s.at[B])

    @pl.when(is_end)
    def _():
        settle(sent[E], sent_s.at[E])

    @pl.when(is_mid)
    def _():
        settle(sent[M], sent_s.at[M])

    @pl.when(s < 3)
    def _():
        for copy in halos:
            copy.wait_send()


def layer(
    residual,
    queries,
    keys,
    values,
    segments,
    routes,
    route_weight,
    sinks,
    out_weight,
    norm_gain,
    expert_gate,
    expert_up,
    expert_down,
    shared_gate,
    shared_up,
    shared_down,
):
    arguments = (
        residual,
        queries,
        keys,
        values,
        segments,
        routes,
        route_weight,
        sinks,
        out_weight,
        norm_gain,
        expert_gate,
        expert_up,
        expert_down,
        shared_gate,
        shared_up,
        shared_down,
    )
    rows, width = residual.shape
    n_sp, n_tp = lax.axis_size("sp"), lax.axis_size("tp")
    capacity = 2 * rows * routes.shape[1] // n_sp
    hidden = expert_gate.shape[2]
    if n_sp != 4 or n_tp != 4 or capacity < rows or rows != 2 * WINDOW or shared_gate.shape[1] != hidden:
        return shards(*arguments)
    cols = width // n_tp
    heads = queries.shape[1] // HEAD_DIM
    group = queries.shape[1] // keys.shape[1]
    kv_width = keys.shape[1]
    blocks = rows // WINDOW
    bf16, f32 = jnp.bfloat16, jnp.float32
    vmem = pl.BlockSpec(memory_space=pltpu.VMEM)
    anywhere = pl.BlockSpec(memory_space=pl.ANY)
    dma = pltpu.SemaphoreType.DMA
    piece = rows // PARTS
    return pl.pallas_call(
        functools.partial(fused_kernel, (rows, cols, width, WINDOW, hidden, heads, group)),
        out_shape=pltpu.VMEM((rows, cols), bf16),
        in_specs=[anywhere] * 16,
        out_specs=vmem,
        scratch_shapes=[
            pltpu.VMEM(queries.shape, bf16),
            pltpu.VMEM(keys.shape, bf16),
            pltpu.VMEM(values.shape, bf16),
            pltpu.VMEM((1, rows), jnp.int32),
            pltpu.VMEM(routes.shape[::-1], jnp.int32),
            pltpu.VMEM(routes.shape[::-1], f32),
            pltpu.SMEM(sinks.shape, f32),
            pltpu.VMEM((1, width), f32),
            pltpu.VMEM((rows, cols), bf16),
            pltpu.VMEM(out_weight.shape, bf16),
            pltpu.VMEM((width, 2 * hidden), bf16),
            pltpu.VMEM((width, 2 * hidden), bf16),
            pltpu.VMEM(expert_down.shape[1:], bf16),
            pltpu.VMEM(shared_down.shape, bf16),
            pltpu.VMEM((WINDOW, kv_width), bf16),
            pltpu.VMEM((WINDOW, kv_width), bf16),
            pltpu.VMEM((8, WINDOW), f32),
            pltpu.VMEM((8, rows), f32),
            pltpu.VMEM((8, WINDOW), f32),
            pltpu.VMEM((4, 8, rows), f32),
            pltpu.VMEM((rows, heads * HEAD_DIM), bf16),
            pltpu.VMEM((blocks, 2, WINDOW, cols), bf16),
            pltpu.VMEM((blocks, 2, WINDOW, cols), bf16),
            pltpu.VMEM((PARTS, piece, cols), bf16),
            pltpu.VMEM((PARTS, piece, cols), bf16),
            pltpu.VMEM((rows, cols), f32),
            pltpu.VMEM((4, 4, rows, cols), bf16),
            pltpu.VMEM((rows, width), bf16),
            pltpu.VMEM((rows, width), bf16),
            pltpu.VMEM((5, 4, rows, hidden), bf16),
            pltpu.VMEM((4, rows, cols), f32),
            pltpu.VMEM((4, rows, cols), bf16),
            pltpu.VMEM((5, rows, cols), bf16),
            pltpu.VMEM((rows, cols), f32),
            dma((11,)),
            dma((4,)),
            dma((3,)),
            dma((4,)),
            dma((blocks, 2)),
            dma((PARTS,)),
            dma((4, 2, PARTS)),
            dma((4, blocks)),
            dma((5, 2, blocks)),
            dma((5, PARTS)),
        ],
        compiler_params=pltpu.CompilerParams(collective_id=0, has_side_effects=True),
    )(
        residual,
        queries,
        keys,
        values,
        segments[None, :],
        routes.T,
        route_weight.T,
        sinks,
        out_weight,
        norm_gain[None, :],
        expert_gate,
        expert_up,
        expert_down,
        shared_gate,
        shared_up,
        shared_down,
    )


def solution(mesh):
    placed = (
        P(("grp", "sp"), None),
        P(("grp", "sp"), "tp"),
        P(("grp", "sp"), "tp"),
        P(("grp", "sp"), "tp"),
        P(("grp", "sp")),
        P(("grp", "sp"), None),
        P(("grp", "sp"), None),
        P("tp"),
        P("tp", None),
        P(),
        P("sp", None, "tp"),
        P("sp", None, "tp"),
        P("sp", None, "tp"),
        P(None, "tp"),
        P(None, "tp"),
        P(None, "tp"),
    )
    return jax.shard_map(
        layer, mesh=mesh, in_specs=placed, out_specs=P(("grp", "sp"), "tp"), check_vma=False
    )
```

```python
import functools
import math
import jax
import jax.numpy as jnp
from jax import lax
from jax.experimental import pallas as pl
from jax.experimental.pallas import tpu as pltpu
from jax.sharding import PartitionSpec as P

HEAD_DIM = 64
WINDOW = 128


epsilon = 1e-06


def passed_along(value, axis, steps):
    count = lax.axis_size(axis)
    leading, last = (max(0, -steps), min(count, count - steps))
    return lax.ppermute(value, axis, [(source, source + steps) for source in range(leading, last)])


def banded(prev_rows, own_rows, window_len):
    blocks = own_rows.shape[0] // window_len
    joined = jnp.concatenate([prev_rows, own_rows], axis=0)
    shaped = joined.reshape((blocks + 1, window_len) + own_rows.shape[1:])
    return jnp.concatenate([shaped[:-1], shaped[1:]], axis=1)


def shards(
    residual,
    queries,
    keys,
    values,
    segments,
    routes,
    route_weight,
    sinks,
    out_weight,
    norm_gain,
    expert_gate,
    expert_up,
    expert_down,
    shared_gate,
    shared_up,
    shared_down,
):
    rows_here = residual.shape[0]
    model_width = residual.shape[1]
    tp_count = lax.axis_size("tp")
    tp_index = lax.axis_index("tp")
    head_local = queries.shape[1] // HEAD_DIM
    kv_local = keys.shape[1] // HEAD_DIM
    group_size = head_local // kv_local
    window_len = WINDOW
    blocks = rows_here // window_len
    own_marks = (segments % 256 + 1).astype(jnp.bfloat16)
    prev_keys, prev_values, prev_marks = passed_along(
        (
            keys[rows_here - window_len :],
            values[rows_here - window_len :],
            own_marks[rows_here - window_len :],
        ),
        "sp",
        1,
    )
    key_band = banded(prev_keys, keys, window_len).reshape(
        blocks, 2 * window_len, kv_local, HEAD_DIM
    )
    value_band = banded(prev_values, values, window_len).reshape(
        blocks, 2 * window_len, kv_local, HEAD_DIM
    )
    mark_band = banded(prev_marks, own_marks, window_len).astype(jnp.float32)
    query_marks = own_marks.reshape(blocks, window_len).astype(jnp.float32)
    query_blocks = queries.reshape(blocks, window_len, kv_local, group_size, HEAD_DIM)
    scores = jnp.einsum(
        "nqhgd,nkhd->nhgqk", query_blocks, key_band, preferred_element_type=jnp.float32
    ) * HEAD_DIM ** (-0.5)
    offsets = jnp.arange(window_len)[:, None] + window_len - jnp.arange(2 * window_len)[None, :]
    allowed = (
        (offsets >= 0) & (offsets < window_len) & (query_marks[:, :, None] == mark_band[:, None, :])
    )
    sink_logits = sinks.reshape(kv_local, group_size)[None, :, :, None]
    masked = jnp.where(allowed[:, None, None], scores, -jnp.inf)
    top_score = jnp.maximum(jnp.max(masked, axis=-1), sink_logits)
    exp_terms = jnp.where(allowed[:, None, None], jnp.exp(scores - top_score[..., None]), 0.0)
    denominator = jnp.sum(exp_terms, axis=-1) + jnp.exp(sink_logits - top_score)
    probabilities = (exp_terms / denominator[..., None]).astype(jnp.bfloat16)
    attended = jnp.einsum(
        "nhgqk,nkhd->nqhgd", probabilities, value_band, preferred_element_type=jnp.float32
    )
    attended = attended.astype(jnp.bfloat16).reshape(rows_here, head_local * HEAD_DIM)
    partial_value = jnp.dot(attended, out_weight, preferred_element_type=jnp.float32)
    col_width = model_width // tp_count
    col_start = tp_index * col_width
    summed = lax.psum(partial_value, "tp")
    updated = (residual.astype(jnp.float32) + summed).astype(jnp.bfloat16)
    updated_f32 = updated.astype(jnp.float32)
    inv_rms = lax.rsqrt(jnp.mean(updated_f32 * updated_f32, axis=-1, keepdims=True) + epsilon)
    normed = (updated_f32 * inv_rms * norm_gain).astype(jnp.bfloat16)
    updated_cols = lax.dynamic_slice_in_dim(updated, col_start, col_width, 1)
    normed_cols = lax.dynamic_slice_in_dim(normed, col_start, col_width, 1)
    shared_pre = jnp.dot(normed, shared_gate, preferred_element_type=jnp.float32)
    shared_lin = jnp.dot(normed, shared_up, preferred_element_type=jnp.float32)
    shared_act = (jax.nn.silu(shared_pre) * shared_lin).astype(jnp.bfloat16)
    top_count = routes.shape[1]
    experts = lax.axis_size("sp")
    capacity = 2 * rows_here * top_count // experts
    flat_ids = routes.reshape(-1)
    one_hot = (flat_ids[:, None] == jnp.arange(experts, dtype=jnp.int32)[None, :]).astype(jnp.int32)
    rank_in = jnp.cumsum(one_hot, axis=0) - one_hot
    slot_dest = flat_ids * capacity + jnp.sum(rank_in * one_hot, axis=1)
    token_of = jnp.arange(rows_here * top_count, dtype=jnp.int32) // top_count
    slot_token = jnp.full((experts * capacity,), -1, jnp.int32).at[slot_dest].set(token_of)
    filled = slot_token >= 0
    safe_token = jnp.where(filled, slot_token, 0)
    outgoing = jnp.where(filled[:, None], normed_cols[safe_token], jnp.zeros((), jnp.bfloat16))
    pieces = lax.all_to_all(
        outgoing.reshape(experts, capacity, col_width),
        "sp",
        split_axis=0,
        concat_axis=0,
        tiled=True,
    )
    arrived = lax.all_gather(pieces, "tp", axis=2, tiled=True)
    expert_rows = arrived.reshape(-1, model_width)
    gate_pre = jnp.dot(expert_rows, expert_gate[0], preferred_element_type=jnp.float32)
    up_lin = jnp.dot(expert_rows, expert_up[0], preferred_element_type=jnp.float32)
    expert_act = (jax.nn.silu(gate_pre) * up_lin).astype(jnp.bfloat16)
    gathered_expert, gathered_shared = (
        lax.all_gather(expert_act, "tp", axis=1, tiled=True),
        lax.all_gather(shared_act, "tp", axis=1, tiled=True),
    )
    expert_out = jnp.dot(
        gathered_expert, expert_down[0], preferred_element_type=jnp.float32
    ).astype(jnp.bfloat16)
    returned = lax.all_to_all(
        expert_out.reshape(experts, capacity, col_width),
        "sp",
        split_axis=0,
        concat_axis=0,
        tiled=True,
    )
    returned = returned.reshape(experts * capacity, col_width)
    picked = returned[slot_dest].astype(jnp.float32).reshape(rows_here, top_count, col_width)
    routed = jnp.sum(picked * route_weight[:, :, None], axis=1)
    shared_cols = jnp.dot(gathered_shared, shared_down, preferred_element_type=jnp.float32)
    return (updated_cols.astype(jnp.float32) + shared_cols + routed).astype(jnp.bfloat16)


MESH = pl.DeviceIdType.MESH
PARTS = 4
OWN = (0, 1)
E, M, B = 0, 1, 2
ALONG = {
    (E, 1): (0, 1, 3),
    (E, 2): (0,),
    (E, 3): (1,),
    (M, 0): (0, 1, 2, 3),
    (M, 2): (0, 3),
    (M, 3): (2, 3),
}


def fused_kernel(
    dims,
    res_hbm,
    q_hbm,
    k_hbm,
    v_hbm,
    seg_hbm,
    routes_hbm,
    rw_hbm,
    sinks_hbm,
    wo_hbm,
    gain_hbm,
    eg_hbm,
    eu_hbm,
    ed_hbm,
    sg_hbm,
    su_hbm,
    sd_hbm,
    result,
    q_ref,
    k_ref,
    v_ref,
    seg_ref,
    routes_ref,
    rw_ref,
    sinks_ref,
    gain_ref,
    res_v,
    wo_v,
    gu_v,
    sgu_v,
    dn_v,
    sdn_v,
    kh,
    vh,
    mh,
    marks_own,
    marks_v,
    wx,
    att,
    b1s,
    b1r,
    b2s,
    b2r,
    keep,
    upd,
    norm_v,
    norm_h,
    act,
    tot,
    ret,
    rin,
    acc,
    w_sem,
    sent_s,
    halo_r,
    x_r,
    b_r,
    u_r,
    m_r,
    a_r,
    e_r,
):
    rows, cols, width, window, hidden, heads, group = dims
    bf16, f32 = jnp.bfloat16, jnp.float32
    s = lax.axis_index("sp")
    t = lax.axis_index("tp")
    core = t % 2
    chip = t // 2
    mate = t + 1 - 2 * core
    over = t + 2 - 4 * chip
    diag = 3 - t
    side = s // 2
    middle = ((s + 1) // 2) % 2
    is_mid = middle == 1
    is_end = middle == 0
    inner = s + 1 - 2 * side
    outer = (s + 3 + 2 * side) % 4

    def index_of(block):
        end, mid = block
        b = end + middle * (mid - end)
        return b + side * (3 - 2 * b)

    roles = (is_end, is_mid, None)
    sent = [0, 0, 0]

    def remote(src, dst, recv, sp, tp, role=B):
        return pltpu.make_async_remote_copy(
            src_ref=src,
            dst_ref=dst,
            send_sem=sent_s.at[role],
            recv_sem=recv,
            device_id={"sp": sp, "tp": tp},
            device_id_type=MESH,
        )

    def count(copy, role):
        width_of = 2 if copy.src_ref.dtype == bf16 else 4
        sent[role] += math.prod(copy.src_ref.shape) * width_of

    def go(copy, role=B):
        if role == B:
            copy.start()
        else:

            @pl.when(roles[role])
            def _():
                copy.start()

        count(copy, role)

    barrier = pltpu.get_barrier_semaphore()
    for sp, tp in ((s, mate), (s, over), (inner, t)):
        pl.semaphore_signal(barrier, inc=1, device_id={"sp": sp, "tp": tp}, device_id_type=MESH)

    @pl.when(is_mid)
    def _():
        pl.semaphore_signal(barrier, inc=1, device_id={"sp": outer, "tp": t}, device_id_type=MESH)

    own_cols = pl.ds(pl.multiple_of(t * cols, cols), cols)
    first_half = pl.ds(0, hidden)
    second_half = pl.ds(hidden, hidden)
    sources = (
        ((seg_hbm, seg_ref),),
        ((k_hbm, k_ref), (q_hbm, q_ref), (v_hbm, v_ref)),
        ((sinks_hbm, sinks_ref),),
        ((routes_hbm, routes_ref),),
        ((rw_hbm, rw_ref),),
        ((wo_hbm, wo_v),),
        ((res_hbm.at[:, own_cols], res_v),),
        ((gain_hbm, gain_ref),),
        ((eg_hbm.at[0], gu_v.at[:, first_half]), (eu_hbm.at[0], gu_v.at[:, second_half])),
        ((sg_hbm, sgu_v.at[:, first_half]), (su_hbm, sgu_v.at[:, second_half])),
        ((ed_hbm.at[0], dn_v), (sd_hbm, sdn_v)),
    )
    for i, group_of in enumerate(sources):
        for src, dst in group_of:
            pltpu.make_async_copy(src, dst, w_sem.at[i]).start()
    as_large = {1: upd.at[0, 0], 8: gu_v, 9: sgu_v, 10: gu_v}

    def loaded(*which):
        for i in which:
            whole = as_large[i] if i in as_large else sources[i][0][1]
            pltpu.make_async_copy(whole, whole, w_sem.at[i]).wait()

    tail = pl.ds(rows - window, window)
    up_sp = (s + 1) % 4
    halos = [
        remote(k_ref.at[tail], kh, halo_r.at[0], up_sp, t, 3),
        remote(v_ref.at[tail], vh, halo_r.at[1], up_sp, t, 3),
        remote(marks_v, mh, halo_r.at[2], up_sp, t, 3),
    ]

    @pl.when(s == 0)
    def _():
        kh[...] = jnp.zeros_like(kh)
        vh[...] = jnp.zeros_like(vh)
        mh[...] = jnp.full(mh.shape, -1.0, f32)

    loaded(0)
    marks_own[...] = jnp.broadcast_to(seg_ref[...].astype(f32), marks_own.shape)
    marks_v[...] = marks_own[:, tail]

    def down_rows(row):
        return jnp.transpose(jnp.broadcast_to(row, (window, window)))

    q_pos = lax.broadcasted_iota(jnp.int32, (window, window), 0)
    k_pos = lax.broadcasted_iota(jnp.int32, (window, window), 1)

    def attend(n):
        here = pl.ds(n * window, window)
        if n == 0:
            k_prev, v_prev, m_prev = kh, vh, mh[0:1, :]
            before = slice(None)
        else:
            before = pl.ds((n - 1) * window, window)
            k_prev, v_prev, m_prev = k_ref, v_ref, marks_own[0:1, before]
        m_own = marks_own[0:1, here]
        marks = down_rows(m_own)
        ok_prev = (k_pos > q_pos) & (marks == m_prev)
        ok_own = (k_pos <= q_pos) & (marks == m_own)
        contract = (((1,), (1,)), ((), ()))
        every = range(heads)
        kv = [slice((h // group) * HEAD_DIM, (h // group + 1) * HEAD_DIM) for h in every]
        scores = []
        for h in every:
            qh = q_ref[here, h * HEAD_DIM : (h + 1) * HEAD_DIM]
            pair = [
                lax.dot_general(qh, k, contract, preferred_element_type=f32) * HEAD_DIM ** (-0.5)
                for k in (k_prev[before, kv[h]], k_ref[here, kv[h]])
            ]
            scores.append((jnp.where(ok_prev, pair[0], -jnp.inf), jnp.where(ok_own, pair[1], -jnp.inf)))
        tops = [
            jnp.maximum(jnp.max(jnp.maximum(*scores[h]), axis=-1, keepdims=True), sinks_ref[h])
            for h in every
        ]
        terms = [tuple(jnp.exp(score - tops[h]) for score in scores[h]) for h in every]
        totals = [
            jnp.sum(terms[h][0] + terms[h][1], axis=-1, keepdims=True)
            + jnp.exp(sinks_ref[h] - tops[h])
            for h in every
        ]
        for h in every:
            inverse = 1.0 / totals[h]
            p_prev, p_own = ((term * inverse).astype(bf16) for term in terms[h])
            got = jnp.dot(p_prev, v_prev[before, kv[h]], preferred_element_type=f32) + jnp.dot(
                p_own, v_ref[here, kv[h]], preferred_element_type=f32
            )
            att[here, h * HEAD_DIM : (h + 1) * HEAD_DIM] = got.astype(bf16)

    def project(n, chunk):
        where = pl.ds(pl.multiple_of(chunk * cols, cols), cols)
        return jnp.dot(
            att[pl.ds(n * window, window), :], wo_v[:, where], preferred_element_type=f32
        )

    part_rows = rows // PARTS
    per_half = window // part_rows

    def parts_of(n):
        return range(n * per_half, (n + 1) * per_half)

    def part_span(p):
        return pl.ds(p * part_rows, part_rows)

    first = {}
    second = {}

    def reduce_in_chip(n):
        for far in (1, 0):
            chunk = (over if far else t) + 1 - 2 * core
            b1s[n, far] = project(n, chunk).astype(bf16)
            copy = remote(
                b1s.at[n, far], b1r.at[n, far], b_r.at[n, far], s, mate
            )
            go(copy)
            first[n, far] = copy

    def reduce_across(n):
        mine = project(n, over)
        first[n, 1].wait_recv()
        mine = mine + b1r[n, 1].astype(f32)
        for i, p in enumerate(parts_of(n)):
            b2s[p] = mine[i * part_rows : (i + 1) * part_rows].astype(bf16)
            copy = remote(b2s.at[p], b2r.at[p], u_r.at[s, 0, p], s, over)
            go(copy)
            second[p] = copy

    def hold(n):
        here = pl.ds(n * window, window)
        mine = project(n, t) + res_v[here, :].astype(f32)
        first[n, 0].wait_recv()
        keep[here, :] = mine + b1r[n, 0].astype(f32)

    def piece(b, chunk, p):
        return upd.at[b, chunk, part_span(p)]

    def share(passed, b, chunk, p, sp, tp, role=B):
        place = piece(b, chunk, p)
        return remote(place, place, u_r.at[b, passed, p], sp, tp, role)

    def to_mate(b, chunk, p, role=B):
        place = piece(b, chunk, p)
        return remote(place, place, m_r.at[b, p // per_half], s, mate, role)

    def send_own(role, far, p, passed):
        wanted = (M, 0) if role == E else (E, 1) if far else (M, 2)
        if passed and p not in ALONG[wanted]:
            return
        chunk = over if passed else t
        go(share(passed, s, chunk, p, outer if far else inner, t, role), role)

    def publish(p):
        second[p].wait_recv()
        upd[s, t, part_span(p), :] = (keep[part_span(p), :] + b2r[p].astype(f32)).astype(bf16)
        go(share(1, s, t, p, s, over))
        go(to_mate(s, t, p))

    def own_over(p):
        share(1, s, over, p, s, over).wait_recv()
        go(to_mate(s, over, p))

    def onward(block):
        return inner if block == 0 else outer

    def take(role, block, p, passed):
        b = block + side * (3 - 2 * block)
        chunk = over if passed else t
        copies = []
        if role == M and (not passed or p in ALONG[(M, 3) if block == 0 else (E, block)]):
            copies.append(share(passed, b, chunk, p, onward(block), t, role))
        if not passed and p not in ALONG[role, block]:
            copies.append(share(1, b, chunk, p, s, over, role))
        copies.append(to_mate(b, chunk, p, role))

        @pl.when(roles[role])
        def _():
            share(passed, b, chunk, p, s, mate).wait_recv()
            for copy in copies:
                copy.start()

        for copy in copies:
            count(copy, role)

    def normalize(block, n, rows_out):
        b = index_of(block)
        landed = upd.at[b, pl.ds(0, 2), pl.ds(n * window, window)]
        remote(landed, landed, m_r.at[b, n], s, mate).wait_recv()
        step = 32

        def body(i, carry):
            here = pl.ds(pl.multiple_of(n * window + i * step, step), step)
            squares = jnp.zeros((step, 1), f32)
            for chunk in range(4):
                part = upd[b, chunk, here, :].astype(f32)
                squares = squares + jnp.sum(part * part, axis=-1, keepdims=True)
            inv = lax.rsqrt(squares / width + epsilon)
            for chunk in range(4):
                part = upd[b, chunk, here, :].astype(f32)
                span = slice(chunk * cols, (chunk + 1) * cols)
                rows_out[here, span] = (part * inv * gain_ref[0:1, span]).astype(bf16)
            return carry

        lax.fori_loop(0, window // step, body, 0)

    def slot_of(block):
        return 4 if block is None else index_of(block)

    def pass_on(slot, chunk, tp, n, role=B):
        place = act.at[slot, chunk, pl.ds(n * window, window)]
        flow = 0 if tp is over else 1
        return remote(place, place, a_r.at[slot, flow, n], s, tp, role)

    def activate(block, n, normed):
        slot = slot_of(block)
        here = pl.ds(n * window, window)
        weight = sgu_v if block is None else gu_v
        both = jnp.dot(normed[here, :], weight[...], preferred_element_type=f32)
        gate, lin = both[:, :hidden], both[:, hidden:]
        act[slot, t, here, :] = (gate / (1.0 + jnp.exp(-gate)) * lin).astype(bf16)
        go(pass_on(slot, t, over, n))
        go(pass_on(slot, t, mate, n))

    def relay_act(role, block, n):
        if role == B:
            slot = s if block == 0 else 4
            pass_on(slot, over, over, n).wait_recv()
            go(pass_on(slot, over, mate, n))
        else:
            slot = block + side * (3 - 2 * block)
            copy = pass_on(slot, over, mate, n, role)

            @pl.when(roles[role])
            def _():
                pass_on(slot, over, over, n).wait_recv()
                copy.start()

            count(copy, role)

    def contract_act(block, n):
        slot = slot_of(block)
        weight = sdn_v if block is None else dn_v
        landed = act.at[slot, pl.ds(0, 2), pl.ds(n * window, window)]
        remote(landed, landed, a_r.at[slot, 1, n], s, mate).wait_recv()
        total = None
        for chunk in range(4):
            part = jnp.dot(
                act[slot, chunk, pl.ds(n * window, window), :],
                weight[chunk * hidden : (chunk + 1) * hidden, :],
                preferred_element_type=f32,
            )
            total = part if total is None else total + part
        return total

    def weighted(block, n, place, other):
        here = pl.ds(n * window, window)
        total = contract_act(block, n)
        listed = wx[index_of(block), :, here]
        row = lax.broadcasted_iota(jnp.int32, listed.shape, 0)
        column = down_rows(jnp.sum(jnp.where(row == s, listed, 0.0), axis=0, keepdims=True))
        for c in range(0, cols, window):
            value = column * total[:, c : c + window]
            if other is not None:
                value = value + other(slice(c, c + window))
            place[here, c : c + window] = value

    def back(place, b, p, sp, role=B):
        here = part_span(p)
        return remote(ret.at[b, here], rin.at[place, here], e_r.at[b, p], sp, t, role)

    def give(block, n):
        weighted(block, n, tot.at[index_of(block)], None)

    def pass_back(role, block, p):
        b = block + side * (3 - 2 * block)
        here = part_span(p)
        place = 4 if (role, block) == (E, 1) else b
        copy = back(place, b, p, outer if (role, block) == (M, 0) else inner, role)

        @pl.when(roles[role])
        def _():
            value = tot[b, here, :]
            if role == M:
                back(b, b, p, inner).wait_recv()
                value = value + rin[b, here, :].astype(f32)
            ret[b, here, :] = value.astype(bf16)
            copy.start()

        count(copy, role)

    def keep_own(n):
        here = pl.ds(n * window, window)
        weighted(OWN, n, acc, lambda c: upd[s, t, here, c].astype(f32) + acc[here, c])

    def keep_shared(n):
        acc[pl.ds(n * window, window), :] = contract_act(None, n)

    def gather_in(p):
        here = part_span(p)
        both = rin.at[pl.ds(0, 2), here]

        @pl.when(is_end)
        def _():
            back(s, s, p, inner).wait_recv()

        @pl.when(is_mid)
        def _():
            remote(both, both, e_r.at[s, p], outer, t).wait_recv()

        result[here, :] = (
            acc[here, :] + rin[s, here, :].astype(f32) + rin[4, here, :].astype(f32)
        ).astype(bf16)

    def weights_on(b, sp, role=B):
        return remote(wx.at[b], wx.at[b], x_r.at[b], sp, t, role)

    def take_weights(role, block):
        copy = weights_on(block + side * (3 - 2 * block), onward(block), M)

        @pl.when(roles[role])
        def _():
            copy.wait_recv()
            if role == M:
                copy.start()

        if role == M:
            count(copy, M)

    def compute(block, n):
        normalize(block, n, norm_v)
        activate(block, n, norm_v)

    def norm_own(n):
        normalize(OWN, n, norm_h)

    def act_own(n):
        activate(OWN, n, norm_h)

    def act_shared(n):
        activate(None, n, norm_h)

    def enter():
        loaded(3, 4)
        wx[s] = jnp.zeros(wx.shape[1:], f32)
        for e in range(4):
            weight = jnp.zeros((1, rows), f32)
            for k in range(routes_ref.shape[0]):
                named = routes_ref[k : k + 1, :] == e
                weight = weight + jnp.where(named, rw_ref[k : k + 1, :], 0.0)
            wx[s, e : e + 1, :] = weight
        pl.semaphore_wait(barrier, 3 + middle)

        @pl.when(s < 3)
        def _():
            for copy in halos:
                copy.start()

        go(weights_on(s, inner))
        go(weights_on(s, outer, M), M)
        loaded(5)

    def clear():
        @pl.when(is_end)
        def _():
            rin[4] = jnp.zeros(rin.shape[1:], bf16)

    def halo():
        @pl.when(s > 0)
        def _():
            for copy in halos:
                copy.wait_recv()

    loaded(1, 2)
    attend(1)
    enter()
    reduce_in_chip(1)
    reduce_across(1)
    clear()
    halo()
    attend(0)
    loaded(6)
    take_weights(M, 0)
    reduce_in_chip(0)
    hold(1)
    reduce_across(0)
    publish(2)
    send_own(M, 0, 2, 0)
    take_weights(M, 2)
    send_own(E, 0, 2, 0)
    send_own(M, 1, 2, 0)
    hold(0)
    publish(3)
    loaded(7, 8, 9, 10)
    send_own(M, 0, 3, 0)
    send_own(E, 0, 3, 0)
    send_own(M, 1, 3, 0)
    take(M, 0, 2, 0)
    take_weights(M, 3)
    take(M, 2, 2, 0)
    publish(0)
    send_own(E, 0, 0, 0)
    take(M, 0, 3, 0)
    take(M, 2, 3, 0)
    take(M, 0, 0, 0)
    publish(1)
    take(M, 3, 2, 0)
    take(M, 0, 1, 0)
    send_own(M, 0, 1, 0)
    send_own(E, 0, 1, 0)
    send_own(M, 0, 0, 0)
    own_over(3)
    send_own(E, 0, 3, 1)
    take(M, 3, 3, 0)
    take(E, 1, 2, 0)
    take(M, 2, 2, 1)
    take_weights(E, 3)
    take(M, 3, 0, 0)
    own_over(0)
    own_over(2)
    send_own(M, 0, 3, 1)
    take(E, 2, 2, 0)
    send_own(E, 0, 2, 1)
    take(M, 0, 3, 1)
    take(E, 2, 3, 0)
    send_own(M, 0, 0, 1)
    take(M, 3, 1, 0)
    take(M, 0, 2, 1)
    take(E, 3, 2, 0)
    take(E, 1, 3, 0)
    take(E, 2, 2, 1)
    take(M, 2, 1, 0)
    send_own(M, 1, 3, 1)
    send_own(E, 0, 0, 1)
    take(E, 3, 3, 0)
    take(E, 2, 3, 1)
    own_over(1)
    take(E, 3, 0, 0)
    send_own(E, 0, 1, 1)
    compute((2, 0), 1)
    take(E, 3, 2, 1)
    norm_own(1)
    take(E, 1, 2, 1)
    norm_own(0)
    take(E, 3, 3, 1)
    take(M, 3, 1, 1)
    take(M, 2, 0, 0)
    take(E, 2, 1, 0)
    take(M, 2, 3, 1)
    compute((3, 2), 1)
    take(M, 0, 1, 1)
    take(M, 2, 1, 1)
    relay_act(M, 0, 1)
    take(M, 3, 0, 1)
    take_weights(E, 2)
    take(M, 2, 0, 1)
    take(E, 3, 1, 0)
    act_shared(0)
    take(M, 0, 0, 1)
    take(M, 3, 3, 1)
    take(E, 1, 3, 1)
    take(E, 3, 0, 1)
    relay_act(E, 2, 1)
    send_own(M, 1, 1, 1)
    take(E, 3, 1, 1)
    send_own(M, 1, 0, 0)
    send_own(M, 1, 1, 0)
    give((2, 0), 1)
    pass_back(E, 2, 3)
    take_weights(E, 1)
    compute((3, 3), 0)
    take(M, 3, 2, 1)
    pass_back(E, 2, 2)
    take(E, 2, 0, 0)
    take(E, 2, 1, 1)
    take(E, 2, 0, 1)
    send_own(M, 1, 0, 1)
    relay_act(E, 3, 1)
    relay_act(M, 2, 1)
    compute((1, 3), 1)
    give((3, 2), 1)
    pass_back(E, 3, 3)
    pass_back(E, 3, 2)
    compute((2, 0), 0)
    take(E, 1, 0, 0)
    relay_act(E, 3, 0)
    pass_back(M, 2, 3)
    act_shared(1)
    relay_act(M, 3, 0)
    relay_act(B, 1, 0)
    give((3, 3), 0)
    pass_back(E, 3, 0)
    pass_back(E, 3, 1)
    relay_act(M, 3, 1)
    take(E, 1, 1, 1)
    take(E, 1, 1, 0)
    relay_act(E, 1, 1)
    take(E, 1, 0, 1)
    give((1, 3), 1)
    relay_act(M, 0, 0)
    relay_act(E, 2, 0)
    pass_back(E, 1, 3)
    pass_back(M, 3, 3)
    compute((1, 2), 0)
    keep_shared(0)
    pass_back(M, 3, 2)
    relay_act(B, 1, 1)
    pass_back(M, 3, 0)
    give((2, 0), 0)
    pass_back(E, 2, 0)
    pass_back(E, 2, 1)
    pass_back(E, 1, 2)
    pass_back(M, 0, 3)
    pass_back(M, 3, 1)
    act_own(1)
    relay_act(M, 2, 0)
    relay_act(E, 1, 0)
    pass_back(M, 0, 2)
    pass_back(M, 2, 2)
    act_own(0)
    give((1, 2), 0)
    pass_back(M, 0, 0)
    pass_back(E, 1, 0)
    pass_back(M, 2, 0)
    pass_back(M, 0, 1)
    relay_act(B, 0, 1)
    pass_back(E, 1, 1)
    pass_back(M, 2, 1)
    keep_shared(1)
    relay_act(B, 0, 0)
    keep_own(1)
    keep_own(0)
    gather_in(2)
    gather_in(0)
    gather_in(3)
    gather_in(1)

    def settle(size, sem):
        for unit in (upd.at[0], upd.at[0, 0], piece(0, 0, 0), wx.at[0]):
            of_one = math.prod(unit.shape) * (4 if unit.dtype == f32 else 2)
            for _ in range(size // of_one):
                pltpu.make_async_copy(unit, unit, sem).wait()
            size = size % of_one

    settle(sent[B], sent_s.at[B])

    @pl.when(is_end)
    def _():
        settle(sent[E], sent_s.at[E])

    @pl.when(is_mid)
    def _():
        settle(sent[M], sent_s.at[M])

    @pl.when(s < 3)
    def _():
        for copy in halos:
            copy.wait_send()


def layer(
    residual,
    queries,
    keys,
    values,
    segments,
    routes,
    route_weight,
    sinks,
    out_weight,
    norm_gain,
    expert_gate,
    expert_up,
    expert_down,
    shared_gate,
    shared_up,
    shared_down,
):
    arguments = (
        residual,
        queries,
        keys,
        values,
        segments,
        routes,
        route_weight,
        sinks,
        out_weight,
        norm_gain,
        expert_gate,
        expert_up,
        expert_down,
        shared_gate,
        shared_up,
        shared_down,
    )
    rows, width = residual.shape
    n_sp, n_tp = lax.axis_size("sp"), lax.axis_size("tp")
    capacity = 2 * rows * routes.shape[1] // n_sp
    hidden = expert_gate.shape[2]
    if n_sp != 4 or n_tp != 4 or capacity < rows or rows != 2 * WINDOW or shared_gate.shape[1] != hidden:
        return shards(*arguments)
    cols = width // n_tp
    heads = queries.shape[1] // HEAD_DIM
    group = queries.shape[1] // keys.shape[1]
    kv_width = keys.shape[1]
    blocks = rows // WINDOW
    bf16, f32 = jnp.bfloat16, jnp.float32
    vmem = pl.BlockSpec(memory_space=pltpu.VMEM)
    anywhere = pl.BlockSpec(memory_space=pl.ANY)
    dma = pltpu.SemaphoreType.DMA
    piece = rows // PARTS
    return pl.pallas_call(
        functools.partial(fused_kernel, (rows, cols, width, WINDOW, hidden, heads, group)),
        out_shape=pltpu.VMEM((rows, cols), bf16),
        in_specs=[anywhere] * 16,
        out_specs=vmem,
        scratch_shapes=[
            pltpu.VMEM(queries.shape, bf16),
            pltpu.VMEM(keys.shape, bf16),
            pltpu.VMEM(values.shape, bf16),
            pltpu.VMEM((1, rows), jnp.int32),
            pltpu.VMEM(routes.shape[::-1], jnp.int32),
            pltpu.VMEM(routes.shape[::-1], f32),
            pltpu.SMEM(sinks.shape, f32),
            pltpu.VMEM((1, width), f32),
            pltpu.VMEM((rows, cols), bf16),
            pltpu.VMEM(out_weight.shape, bf16),
            pltpu.VMEM((width, 2 * hidden), bf16),
            pltpu.VMEM((width, 2 * hidden), bf16),
            pltpu.VMEM(expert_down.shape[1:], bf16),
            pltpu.VMEM(shared_down.shape, bf16),
            pltpu.VMEM((WINDOW, kv_width), bf16),
            pltpu.VMEM((WINDOW, kv_width), bf16),
            pltpu.VMEM((8, WINDOW), f32),
            pltpu.VMEM((8, rows), f32),
            pltpu.VMEM((8, WINDOW), f32),
            pltpu.VMEM((4, 8, rows), f32),
            pltpu.VMEM((rows, heads * HEAD_DIM), bf16),
            pltpu.VMEM((blocks, 2, WINDOW, cols), bf16),
            pltpu.VMEM((blocks, 2, WINDOW, cols), bf16),
            pltpu.VMEM((PARTS, piece, cols), bf16),
            pltpu.VMEM((PARTS, piece, cols), bf16),
            pltpu.VMEM((rows, cols), f32),
            pltpu.VMEM((4, 4, rows, cols), bf16),
            pltpu.VMEM((rows, width), bf16),
            pltpu.VMEM((rows, width), bf16),
            pltpu.VMEM((5, 4, rows, hidden), bf16),
            pltpu.VMEM((4, rows, cols), f32),
            pltpu.VMEM((4, rows, cols), bf16),
            pltpu.VMEM((5, rows, cols), bf16),
            pltpu.VMEM((rows, cols), f32),
            dma((11,)),
            dma((4,)),
            dma((3,)),
            dma((4,)),
            dma((blocks, 2)),
            dma((4, 2, PARTS)),
            dma((4, blocks)),
            dma((5, 2, blocks)),
            dma((4, PARTS)),
        ],
        compiler_params=pltpu.CompilerParams(collective_id=0, has_side_effects=True),
    )(
        residual,
        queries,
        keys,
        values,
        segments[None, :],
        routes.T,
        route_weight.T,
        sinks,
        out_weight,
        norm_gain[None, :],
        expert_gate,
        expert_up,
        expert_down,
        shared_gate,
        shared_up,
        shared_down,
    )


def solution(mesh):
    placed = (
        P(("grp", "sp"), None),
        P(("grp", "sp"), "tp"),
        P(("grp", "sp"), "tp"),
        P(("grp", "sp"), "tp"),
        P(("grp", "sp")),
        P(("grp", "sp"), None),
        P(("grp", "sp"), None),
        P("tp"),
        P("tp", None),
        P(),
        P("sp", None, "tp"),
        P("sp", None, "tp"),
        P("sp", None, "tp"),
        P(None, "tp"),
        P(None, "tp"),
        P(None, "tp"),
    )
    return jax.shard_map(
        layer, mesh=mesh, in_specs=placed, out_specs=P(("grp", "sp"), "tp"), check_vma=False
    )
```

```python
import functools
import math
import jax
import jax.numpy as jnp
from jax import lax
from jax.experimental import pallas as pl
from jax.experimental.pallas import tpu as pltpu
from jax.sharding import PartitionSpec as P

HEAD_DIM = 64
WINDOW = 128


epsilon = 1e-06


def passed_along(value, axis, steps):
    count = lax.axis_size(axis)
    leading, last = (max(0, -steps), min(count, count - steps))
    return lax.ppermute(value, axis, [(source, source + steps) for source in range(leading, last)])


def banded(prev_rows, own_rows, window_len):
    blocks = own_rows.shape[0] // window_len
    joined = jnp.concatenate([prev_rows, own_rows], axis=0)
    shaped = joined.reshape((blocks + 1, window_len) + own_rows.shape[1:])
    return jnp.concatenate([shaped[:-1], shaped[1:]], axis=1)


def shards(
    residual,
    queries,
    keys,
    values,
    segments,
    routes,
    route_weight,
    sinks,
    out_weight,
    norm_gain,
    expert_gate,
    expert_up,
    expert_down,
    shared_gate,
    shared_up,
    shared_down,
):
    rows_here = residual.shape[0]
    model_width = residual.shape[1]
    tp_count = lax.axis_size("tp")
    tp_index = lax.axis_index("tp")
    head_local = queries.shape[1] // HEAD_DIM
    kv_local = keys.shape[1] // HEAD_DIM
    group_size = head_local // kv_local
    window_len = WINDOW
    blocks = rows_here // window_len
    own_marks = (segments % 256 + 1).astype(jnp.bfloat16)
    prev_keys, prev_values, prev_marks = passed_along(
        (
            keys[rows_here - window_len :],
            values[rows_here - window_len :],
            own_marks[rows_here - window_len :],
        ),
        "sp",
        1,
    )
    key_band = banded(prev_keys, keys, window_len).reshape(
        blocks, 2 * window_len, kv_local, HEAD_DIM
    )
    value_band = banded(prev_values, values, window_len).reshape(
        blocks, 2 * window_len, kv_local, HEAD_DIM
    )
    mark_band = banded(prev_marks, own_marks, window_len).astype(jnp.float32)
    query_marks = own_marks.reshape(blocks, window_len).astype(jnp.float32)
    query_blocks = queries.reshape(blocks, window_len, kv_local, group_size, HEAD_DIM)
    scores = jnp.einsum(
        "nqhgd,nkhd->nhgqk", query_blocks, key_band, preferred_element_type=jnp.float32
    ) * HEAD_DIM ** (-0.5)
    offsets = jnp.arange(window_len)[:, None] + window_len - jnp.arange(2 * window_len)[None, :]
    allowed = (
        (offsets >= 0) & (offsets < window_len) & (query_marks[:, :, None] == mark_band[:, None, :])
    )
    sink_logits = sinks.reshape(kv_local, group_size)[None, :, :, None]
    masked = jnp.where(allowed[:, None, None], scores, -jnp.inf)
    top_score = jnp.maximum(jnp.max(masked, axis=-1), sink_logits)
    exp_terms = jnp.where(allowed[:, None, None], jnp.exp(scores - top_score[..., None]), 0.0)
    denominator = jnp.sum(exp_terms, axis=-1) + jnp.exp(sink_logits - top_score)
    probabilities = (exp_terms / denominator[..., None]).astype(jnp.bfloat16)
    attended = jnp.einsum(
        "nhgqk,nkhd->nqhgd", probabilities, value_band, preferred_element_type=jnp.float32
    )
    attended = attended.astype(jnp.bfloat16).reshape(rows_here, head_local * HEAD_DIM)
    partial_value = jnp.dot(attended, out_weight, preferred_element_type=jnp.float32)
    col_width = model_width // tp_count
    col_start = tp_index * col_width
    summed = lax.psum(partial_value, "tp")
    updated = (residual.astype(jnp.float32) + summed).astype(jnp.bfloat16)
    updated_f32 = updated.astype(jnp.float32)
    inv_rms = lax.rsqrt(jnp.mean(updated_f32 * updated_f32, axis=-1, keepdims=True) + epsilon)
    normed = (updated_f32 * inv_rms * norm_gain).astype(jnp.bfloat16)
    updated_cols = lax.dynamic_slice_in_dim(updated, col_start, col_width, 1)
    normed_cols = lax.dynamic_slice_in_dim(normed, col_start, col_width, 1)
    shared_pre = jnp.dot(normed, shared_gate, preferred_element_type=jnp.float32)
    shared_lin = jnp.dot(normed, shared_up, preferred_element_type=jnp.float32)
    shared_act = (jax.nn.silu(shared_pre) * shared_lin).astype(jnp.bfloat16)
    top_count = routes.shape[1]
    experts = lax.axis_size("sp")
    capacity = 2 * rows_here * top_count // experts
    flat_ids = routes.reshape(-1)
    one_hot = (flat_ids[:, None] == jnp.arange(experts, dtype=jnp.int32)[None, :]).astype(jnp.int32)
    rank_in = jnp.cumsum(one_hot, axis=0) - one_hot
    slot_dest = flat_ids * capacity + jnp.sum(rank_in * one_hot, axis=1)
    token_of = jnp.arange(rows_here * top_count, dtype=jnp.int32) // top_count
    slot_token = jnp.full((experts * capacity,), -1, jnp.int32).at[slot_dest].set(token_of)
    filled = slot_token >= 0
    safe_token = jnp.where(filled, slot_token, 0)
    outgoing = jnp.where(filled[:, None], normed_cols[safe_token], jnp.zeros((), jnp.bfloat16))
    pieces = lax.all_to_all(
        outgoing.reshape(experts, capacity, col_width),
        "sp",
        split_axis=0,
        concat_axis=0,
        tiled=True,
    )
    arrived = lax.all_gather(pieces, "tp", axis=2, tiled=True)
    expert_rows = arrived.reshape(-1, model_width)
    gate_pre = jnp.dot(expert_rows, expert_gate[0], preferred_element_type=jnp.float32)
    up_lin = jnp.dot(expert_rows, expert_up[0], preferred_element_type=jnp.float32)
    expert_act = (jax.nn.silu(gate_pre) * up_lin).astype(jnp.bfloat16)
    gathered_expert, gathered_shared = (
        lax.all_gather(expert_act, "tp", axis=1, tiled=True),
        lax.all_gather(shared_act, "tp", axis=1, tiled=True),
    )
    expert_out = jnp.dot(
        gathered_expert, expert_down[0], preferred_element_type=jnp.float32
    ).astype(jnp.bfloat16)
    returned = lax.all_to_all(
        expert_out.reshape(experts, capacity, col_width),
        "sp",
        split_axis=0,
        concat_axis=0,
        tiled=True,
    )
    returned = returned.reshape(experts * capacity, col_width)
    picked = returned[slot_dest].astype(jnp.float32).reshape(rows_here, top_count, col_width)
    routed = jnp.sum(picked * route_weight[:, :, None], axis=1)
    shared_cols = jnp.dot(gathered_shared, shared_down, preferred_element_type=jnp.float32)
    return (updated_cols.astype(jnp.float32) + shared_cols + routed).astype(jnp.bfloat16)


MESH = pl.DeviceIdType.MESH
PARTS = 4
OWN = (0, 1)
E, M, B = 0, 1, 2
ALONG = {
    (E, 1): (0, 1, 2),
    (E, 2): (1,),
    (E, 3): (1,),
    (M, 0): (0, 1, 2, 3),
    (M, 2): (1, 2),
    (M, 3): (2, 3),
}


def fused_kernel(
    dims,
    res_hbm,
    q_hbm,
    k_hbm,
    v_hbm,
    seg_hbm,
    routes_hbm,
    rw_hbm,
    sinks_hbm,
    wo_hbm,
    gain_hbm,
    eg_hbm,
    eu_hbm,
    ed_hbm,
    sg_hbm,
    su_hbm,
    sd_hbm,
    result,
    q_ref,
    k_ref,
    v_ref,
    seg_ref,
    routes_ref,
    rw_ref,
    sinks_ref,
    gain_ref,
    res_v,
    wo_v,
    gu_v,
    sgu_v,
    dn_v,
    sdn_v,
    kh,
    vh,
    mh,
    marks_own,
    marks_v,
    wx,
    att,
    b1s,
    b1r,
    b2s,
    b2r,
    keep,
    upd,
    norm_v,
    norm_h,
    act,
    tot,
    ret,
    rin,
    acc,
    w_sem,
    sent_s,
    halo_r,
    x_r,
    b_r,
    u_r,
    m_r,
    a_r,
    e_r,
):
    rows, cols, width, window, hidden, heads, group = dims
    bf16, f32 = jnp.bfloat16, jnp.float32
    s = lax.axis_index("sp")
    t = lax.axis_index("tp")
    core = t % 2
    chip = t // 2
    mate = t + 1 - 2 * core
    over = t + 2 - 4 * chip
    diag = 3 - t
    side = s // 2
    middle = ((s + 1) // 2) % 2
    is_mid = middle == 1
    is_end = middle == 0
    inner = s + 1 - 2 * side
    outer = (s + 3 + 2 * side) % 4

    def index_of(block):
        end, mid = block
        b = end + middle * (mid - end)
        return b + side * (3 - 2 * b)

    roles = (is_end, is_mid, None)
    sent = [0, 0, 0]

    def remote(src, dst, recv, sp, tp, role=B):
        return pltpu.make_async_remote_copy(
            src_ref=src,
            dst_ref=dst,
            send_sem=sent_s.at[role],
            recv_sem=recv,
            device_id={"sp": sp, "tp": tp},
            device_id_type=MESH,
        )

    def count(copy, role):
        width_of = 2 if copy.src_ref.dtype == bf16 else 4
        sent[role] += math.prod(copy.src_ref.shape) * width_of

    def go(copy, role=B):
        if role == B:
            copy.start()
        else:

            @pl.when(roles[role])
            def _():
                copy.start()

        count(copy, role)

    barrier = pltpu.get_barrier_semaphore()
    for sp, tp in ((s, mate), (s, over), (inner, t)):
        pl.semaphore_signal(barrier, inc=1, device_id={"sp": sp, "tp": tp}, device_id_type=MESH)

    @pl.when(is_mid)
    def _():
        pl.semaphore_signal(barrier, inc=1, device_id={"sp": outer, "tp": t}, device_id_type=MESH)

    own_cols = pl.ds(pl.multiple_of(t * cols, cols), cols)
    first_half = pl.ds(0, hidden)
    second_half = pl.ds(hidden, hidden)
    sources = (
        ((seg_hbm, seg_ref),),
        ((k_hbm, k_ref), (q_hbm, q_ref), (v_hbm, v_ref)),
        ((sinks_hbm, sinks_ref),),
        ((routes_hbm, routes_ref),),
        ((rw_hbm, rw_ref),),
        ((wo_hbm, wo_v),),
        ((res_hbm.at[:, own_cols], res_v),),
        ((gain_hbm, gain_ref),),
        ((eg_hbm.at[0], gu_v.at[:, first_half]), (eu_hbm.at[0], gu_v.at[:, second_half])),
        ((sg_hbm, sgu_v.at[:, first_half]), (su_hbm, sgu_v.at[:, second_half])),
        ((ed_hbm.at[0], dn_v), (sd_hbm, sdn_v)),
    )
    for i, group_of in enumerate(sources):
        for src, dst in group_of:
            pltpu.make_async_copy(src, dst, w_sem.at[i]).start()
    as_large = {1: upd.at[0, 0], 8: gu_v, 9: sgu_v, 10: gu_v}

    def loaded(*which):
        for i in which:
            whole = as_large[i] if i in as_large else sources[i][0][1]
            pltpu.make_async_copy(whole, whole, w_sem.at[i]).wait()

    tail = pl.ds(rows - window, window)
    up_sp = (s + 1) % 4
    halos = [
        remote(k_ref.at[tail], kh, halo_r.at[0], up_sp, t, 3),
        remote(v_ref.at[tail], vh, halo_r.at[1], up_sp, t, 3),
        remote(marks_v, mh, halo_r.at[2], up_sp, t, 3),
    ]

    @pl.when(s == 0)
    def _():
        kh[...] = jnp.zeros_like(kh)
        vh[...] = jnp.zeros_like(vh)
        mh[...] = jnp.full(mh.shape, -1.0, f32)

    loaded(0)
    marks_own[...] = jnp.broadcast_to(seg_ref[...].astype(f32), marks_own.shape)
    marks_v[...] = marks_own[:, tail]

    def down_rows(row):
        return jnp.transpose(jnp.broadcast_to(row, (window, window)))

    q_pos = lax.broadcasted_iota(jnp.int32, (window, window), 0)
    k_pos = lax.broadcasted_iota(jnp.int32, (window, window), 1)

    def attend(n):
        here = pl.ds(n * window, window)
        if n == 0:
            k_prev, v_prev, m_prev = kh, vh, mh[0:1, :]
            before = slice(None)
        else:
            before = pl.ds((n - 1) * window, window)
            k_prev, v_prev, m_prev = k_ref, v_ref, marks_own[0:1, before]
        m_own = marks_own[0:1, here]
        marks = down_rows(m_own)
        ok_prev = (k_pos > q_pos) & (marks == m_prev)
        ok_own = (k_pos <= q_pos) & (marks == m_own)
        contract = (((1,), (1,)), ((), ()))
        every = range(heads)
        kv = [slice((h // group) * HEAD_DIM, (h // group + 1) * HEAD_DIM) for h in every]
        scores = []
        for h in every:
            qh = q_ref[here, h * HEAD_DIM : (h + 1) * HEAD_DIM]
            pair = [
                lax.dot_general(qh, k, contract, preferred_element_type=f32) * HEAD_DIM ** (-0.5)
                for k in (k_prev[before, kv[h]], k_ref[here, kv[h]])
            ]
            scores.append((jnp.where(ok_prev, pair[0], -jnp.inf), jnp.where(ok_own, pair[1], -jnp.inf)))
        tops = [
            jnp.maximum(jnp.max(jnp.maximum(*scores[h]), axis=-1, keepdims=True), sinks_ref[h])
            for h in every
        ]
        terms = [tuple(jnp.exp(score - tops[h]) for score in scores[h]) for h in every]
        totals = [
            jnp.sum(terms[h][0] + terms[h][1], axis=-1, keepdims=True)
            + jnp.exp(sinks_ref[h] - tops[h])
            for h in every
        ]
        for h in every:
            inverse = 1.0 / totals[h]
            p_prev, p_own = ((term * inverse).astype(bf16) for term in terms[h])
            got = jnp.dot(p_prev, v_prev[before, kv[h]], preferred_element_type=f32) + jnp.dot(
                p_own, v_ref[here, kv[h]], preferred_element_type=f32
            )
            att[here, h * HEAD_DIM : (h + 1) * HEAD_DIM] = got.astype(bf16)

    def project(n, chunk):
        where = pl.ds(pl.multiple_of(chunk * cols, cols), cols)
        return jnp.dot(
            att[pl.ds(n * window, window), :], wo_v[:, where], preferred_element_type=f32
        )

    part_rows = rows // PARTS
    per_half = window // part_rows

    def parts_of(n):
        return range(n * per_half, (n + 1) * per_half)

    def part_span(p):
        return pl.ds(p * part_rows, part_rows)

    first = {}
    second = {}

    def reduce_in_chip(n):
        for far in (1, 0):
            chunk = (over if far else t) + 1 - 2 * core
            b1s[n, far] = project(n, chunk).astype(bf16)
            copy = remote(
                b1s.at[n, far], b1r.at[n, far], b_r.at[n, far], s, mate
            )
            go(copy)
            first[n, far] = copy

    def reduce_across(n):
        mine = project(n, over)
        first[n, 1].wait_recv()
        mine = mine + b1r[n, 1].astype(f32)
        for i, p in enumerate(parts_of(n)):
            b2s[p] = mine[i * part_rows : (i + 1) * part_rows].astype(bf16)
            copy = remote(b2s.at[p], b2r.at[p], u_r.at[s, 0, p], s, over)
            go(copy)
            second[p] = copy

    def hold(n):
        here = pl.ds(n * window, window)
        mine = project(n, t) + res_v[here, :].astype(f32)
        first[n, 0].wait_recv()
        keep[here, :] = mine + b1r[n, 0].astype(f32)

    def piece(b, chunk, p):
        return upd.at[b, chunk, part_span(p)]

    def share(passed, b, chunk, p, sp, tp, role=B):
        place = piece(b, chunk, p)
        return remote(place, place, u_r.at[b, passed, p], sp, tp, role)

    def to_mate(b, chunk, p, role=B):
        place = piece(b, chunk, p)
        return remote(place, place, m_r.at[b, p // per_half], s, mate, role)

    def send_own(role, far, p, passed):
        wanted = (M, 0) if role == E else (E, 1) if far else (M, 2)
        if passed and p not in ALONG[wanted]:
            return
        chunk = over if passed else t
        go(share(passed, s, chunk, p, outer if far else inner, t, role), role)

    def publish(p):
        second[p].wait_recv()
        upd[s, t, part_span(p), :] = (keep[part_span(p), :] + b2r[p].astype(f32)).astype(bf16)
        go(share(1, s, t, p, s, over))
        go(to_mate(s, t, p))

    def own_over(p):
        share(1, s, over, p, s, over).wait_recv()
        go(to_mate(s, over, p))

    def onward(block):
        return inner if block == 0 else outer

    def take(role, block, p, passed):
        b = block + side * (3 - 2 * block)
        chunk = over if passed else t
        copies = []
        if role == M and (not passed or p in ALONG[(M, 3) if block == 0 else (E, block)]):
            copies.append(share(passed, b, chunk, p, onward(block), t, role))
        if not passed and p not in ALONG[role, block]:
            copies.append(share(1, b, chunk, p, s, over, role))
        copies.append(to_mate(b, chunk, p, role))

        @pl.when(roles[role])
        def _():
            share(passed, b, chunk, p, s, mate).wait_recv()
            for copy in copies:
                copy.start()

        for copy in copies:
            count(copy, role)

    def normalize(block, n, rows_out):
        b = index_of(block)
        landed = upd.at[b, pl.ds(0, 2), pl.ds(n * window, window)]
        remote(landed, landed, m_r.at[b, n], s, mate).wait_recv()
        step = 32

        def body(i, carry):
            here = pl.ds(pl.multiple_of(n * window + i * step, step), step)
            squares = jnp.zeros((step, 1), f32)
            for chunk in range(4):
                part = upd[b, chunk, here, :].astype(f32)
                squares = squares + jnp.sum(part * part, axis=-1, keepdims=True)
            inv = lax.rsqrt(squares / width + epsilon)
            for chunk in range(4):
                part = upd[b, chunk, here, :].astype(f32)
                span = slice(chunk * cols, (chunk + 1) * cols)
                rows_out[here, span] = (part * inv * gain_ref[0:1, span]).astype(bf16)
            return carry

        lax.fori_loop(0, window // step, body, 0)

    def slot_of(block):
        return 4 if block is None else index_of(block)

    def pass_on(slot, chunk, tp, n, role=B):
        place = act.at[slot, chunk, pl.ds(n * window, window)]
        flow = 0 if tp is over else 1
        return remote(place, place, a_r.at[slot, flow, n], s, tp, role)

    def activate(block, n, normed):
        slot = slot_of(block)
        here = pl.ds(n * window, window)
        weight = sgu_v if block is None else gu_v
        both = jnp.dot(normed[here, :], weight[...], preferred_element_type=f32)
        gate, lin = both[:, :hidden], both[:, hidden:]
        act[slot, t, here, :] = (gate / (1.0 + jnp.exp(-gate)) * lin).astype(bf16)
        go(pass_on(slot, t, over, n))
        go(pass_on(slot, t, mate, n))

    def relay_act(role, block, n):
        if role == B:
            slot = s if block == 0 else 4
            pass_on(slot, over, over, n).wait_recv()
            go(pass_on(slot, over, mate, n))
        else:
            slot = block + side * (3 - 2 * block)
            copy = pass_on(slot, over, mate, n, role)

            @pl.when(roles[role])
            def _():
                pass_on(slot, over, over, n).wait_recv()
                copy.start()

            count(copy, role)

    def contract_act(block, n):
        slot = slot_of(block)
        weight = sdn_v if block is None else dn_v
        landed = act.at[slot, pl.ds(0, 2), pl.ds(n * window, window)]
        remote(landed, landed, a_r.at[slot, 1, n], s, mate).wait_recv()
        total = None
        for chunk in range(4):
            part = jnp.dot(
                act[slot, chunk, pl.ds(n * window, window), :],
                weight[chunk * hidden : (chunk + 1) * hidden, :],
                preferred_element_type=f32,
            )
            total = part if total is None else total + part
        return total

    def weighted(block, n, place, other):
        here = pl.ds(n * window, window)
        total = contract_act(block, n)
        listed = wx[index_of(block), :, here]
        row = lax.broadcasted_iota(jnp.int32, listed.shape, 0)
        column = down_rows(jnp.sum(jnp.where(row == s, listed, 0.0), axis=0, keepdims=True))
        for c in range(0, cols, window):
            value = column * total[:, c : c + window]
            if other is not None:
                value = value + other(slice(c, c + window))
            place[here, c : c + window] = value

    def back(place, b, p, sp, role=B):
        here = part_span(p)
        return remote(ret.at[b, here], rin.at[place, here], e_r.at[b, p], sp, t, role)

    def give(block, n):
        weighted(block, n, tot.at[index_of(block)], None)

    def pass_back(role, block, p):
        b = block + side * (3 - 2 * block)
        here = part_span(p)
        place = 4 if (role, block) == (E, 1) else b
        copy = back(place, b, p, outer if (role, block) == (M, 0) else inner, role)

        @pl.when(roles[role])
        def _():
            value = tot[b, here, :]
            if role == M:
                back(b, b, p, inner).wait_recv()
                value = value + rin[b, here, :].astype(f32)
            ret[b, here, :] = value.astype(bf16)
            copy.start()

        count(copy, role)

    def keep_own(n):
        here = pl.ds(n * window, window)
        weighted(OWN, n, acc, lambda c: upd[s, t, here, c].astype(f32) + acc[here, c])

    def keep_shared(n):
        acc[pl.ds(n * window, window), :] = contract_act(None, n)

    def gather_in(p):
        here = part_span(p)
        both = rin.at[pl.ds(0, 2), here]

        @pl.when(is_end)
        def _():
            back(s, s, p, inner).wait_recv()

        @pl.when(is_mid)
        def _():
            remote(both, both, e_r.at[s, p], outer, t).wait_recv()

        result[here, :] = (
            acc[here, :] + rin[s, here, :].astype(f32) + rin[4, here, :].astype(f32)
        ).astype(bf16)

    def weights_on(b, sp, role=B):
        return remote(wx.at[b], wx.at[b], x_r.at[b], sp, t, role)

    def take_weights(role, block):
        copy = weights_on(block + side * (3 - 2 * block), onward(block), M)

        @pl.when(roles[role])
        def _():
            copy.wait_recv()
            if role == M:
                copy.start()

        if role == M:
            count(copy, M)

    def compute(block, n):
        normalize(block, n, norm_v)
        activate(block, n, norm_v)

    def norm_own(n):
        normalize(OWN, n, norm_h)

    def act_own(n):
        activate(OWN, n, norm_h)

    def act_shared(n):
        activate(None, n, norm_h)

    def enter():
        loaded(3, 4)
        wx[s] = jnp.zeros(wx.shape[1:], f32)
        for e in range(4):
            weight = jnp.zeros((1, rows), f32)
            for k in range(routes_ref.shape[0]):
                named = routes_ref[k : k + 1, :] == e
                weight = weight + jnp.where(named, rw_ref[k : k + 1, :], 0.0)
            wx[s, e : e + 1, :] = weight
        pl.semaphore_wait(barrier, 3 + middle)

        @pl.when(s < 3)
        def _():
            for copy in halos:
                copy.start()

        go(weights_on(s, inner))
        go(weights_on(s, outer, M), M)
        loaded(5)

    def clear():
        @pl.when(is_end)
        def _():
            rin[4] = jnp.zeros(rin.shape[1:], bf16)

    def halo():
        @pl.when(s > 0)
        def _():
            for copy in halos:
                copy.wait_recv()

    loaded(1, 2)
    attend(1)
    enter()
    reduce_in_chip(1)
    reduce_across(1)
    halo()
    attend(0)
    reduce_in_chip(0)
    loaded(6)
    hold(1)
    take_weights(M, 0)
    reduce_across(0)
    clear()
    publish(2)
    send_own(M, 0, 2, 0)
    send_own(E, 0, 2, 0)
    send_own(M, 1, 2, 0)
    take_weights(M, 2)
    publish(3)
    send_own(M, 0, 3, 0)
    send_own(M, 1, 3, 0)
    loaded(7, 8, 9, 10)
    send_own(E, 0, 3, 0)
    take(M, 0, 2, 0)
    take_weights(M, 3)
    take(M, 2, 2, 0)
    take(M, 0, 3, 0)
    hold(0)
    publish(0)
    send_own(E, 0, 0, 0)
    take(M, 2, 3, 0)
    publish(1)
    send_own(E, 0, 1, 0)
    take(M, 0, 0, 0)
    take(M, 3, 2, 0)
    take(M, 0, 1, 0)
    take(M, 3, 3, 0)
    take_weights(E, 3)
    send_own(M, 0, 0, 0)
    take(M, 3, 0, 0)
    own_over(3)
    own_over(2)
    send_own(E, 0, 3, 1)
    take(E, 2, 2, 0)
    own_over(0)
    send_own(M, 1, 2, 1)
    send_own(E, 0, 2, 1)
    take(M, 0, 3, 1)
    take(E, 2, 3, 0)
    take(E, 3, 2, 0)
    take(M, 3, 1, 0)
    norm_own(1)
    take(E, 2, 2, 1)
    take(E, 1, 2, 0)
    send_own(M, 0, 2, 1)
    own_over(1)
    take(M, 0, 2, 1)
    take(E, 3, 3, 0)
    take(E, 2, 3, 1)
    send_own(M, 0, 1, 1)
    take(E, 1, 3, 0)
    send_own(M, 0, 1, 0)
    take(M, 2, 0, 0)
    send_own(E, 0, 0, 1)
    compute((2, 0), 1)
    take(E, 3, 2, 1)
    take(M, 3, 1, 1)
    send_own(E, 0, 1, 1)
    take(E, 3, 0, 0)
    take(M, 2, 3, 1)
    send_own(M, 1, 1, 0)
    norm_own(0)
    take(E, 3, 3, 1)
    take(M, 2, 2, 1)
    take_weights(E, 2)
    compute((3, 2), 1)
    take(E, 3, 1, 1)
    take(E, 2, 0, 0)
    take(M, 3, 2, 1)
    take(M, 3, 3, 1)
    take(M, 2, 1, 1)
    relay_act(E, 2, 1)
    take(E, 3, 1, 0)
    take(E, 1, 3, 1)
    relay_act(M, 0, 1)
    take(E, 3, 0, 1)
    take(M, 0, 1, 1)
    take(M, 3, 0, 1)
    take(M, 2, 1, 0)
    take(E, 1, 2, 1)
    give((2, 0), 1)
    send_own(M, 1, 1, 1)
    pass_back(E, 2, 3)
    compute((3, 3), 0)
    take(M, 2, 0, 1)
    pass_back(E, 2, 2)
    take(E, 2, 1, 1)
    relay_act(E, 3, 1)
    take(M, 0, 0, 1)
    send_own(M, 1, 0, 1)
    compute((1, 3), 1)
    take(E, 2, 0, 1)
    take(E, 2, 1, 0)
    send_own(M, 1, 0, 0)
    relay_act(M, 2, 1)
    give((3, 2), 1)
    pass_back(E, 3, 2)
    take_weights(E, 1)
    compute((2, 0), 0)
    relay_act(M, 3, 0)
    pass_back(E, 3, 3)
    relay_act(E, 3, 0)
    act_shared(0)
    take(E, 1, 1, 0)
    relay_act(M, 3, 1)
    take(E, 1, 0, 1)
    pass_back(M, 2, 3)
    give((3, 3), 0)
    pass_back(E, 3, 1)
    take(E, 1, 1, 1)
    pass_back(E, 3, 0)
    relay_act(E, 1, 1)
    take(E, 1, 0, 0)
    act_own(0)
    give((1, 3), 1)
    pass_back(M, 3, 2)
    pass_back(E, 1, 3)
    compute((1, 2), 0)
    relay_act(M, 0, 0)
    pass_back(M, 3, 3)
    relay_act(E, 2, 0)
    act_own(1)
    pass_back(M, 3, 1)
    give((2, 0), 0)
    pass_back(E, 2, 0)
    pass_back(M, 0, 2)
    act_shared(1)
    relay_act(B, 0, 0)
    pass_back(E, 2, 1)
    pass_back(M, 3, 0)
    pass_back(M, 0, 3)
    relay_act(M, 2, 0)
    pass_back(E, 1, 2)
    relay_act(E, 1, 0)
    pass_back(M, 2, 2)
    pass_back(M, 0, 1)
    give((1, 2), 0)
    relay_act(B, 0, 1)
    pass_back(M, 2, 0)
    pass_back(M, 0, 0)
    pass_back(M, 2, 1)
    pass_back(E, 1, 1)
    pass_back(E, 1, 0)
    relay_act(B, 1, 0)
    keep_shared(0)
    keep_own(0)
    relay_act(B, 1, 1)
    keep_shared(1)
    keep_own(1)
    gather_in(3)
    gather_in(1)
    gather_in(2)
    gather_in(0)

    def settle(size, sem):
        for unit in (upd.at[0], upd.at[0, 0], piece(0, 0, 0), wx.at[0]):
            of_one = math.prod(unit.shape) * (4 if unit.dtype == f32 else 2)
            for _ in range(size // of_one):
                pltpu.make_async_copy(unit, unit, sem).wait()
            size = size % of_one

    settle(sent[B], sent_s.at[B])

    @pl.when(is_end)
    def _():
        settle(sent[E], sent_s.at[E])

    @pl.when(is_mid)
    def _():
        settle(sent[M], sent_s.at[M])

    @pl.when(s < 3)
    def _():
        for copy in halos:
            copy.wait_send()


def layer(
    residual,
    queries,
    keys,
    values,
    segments,
    routes,
    route_weight,
    sinks,
    out_weight,
    norm_gain,
    expert_gate,
    expert_up,
    expert_down,
    shared_gate,
    shared_up,
    shared_down,
):
    arguments = (
        residual,
        queries,
        keys,
        values,
        segments,
        routes,
        route_weight,
        sinks,
        out_weight,
        norm_gain,
        expert_gate,
        expert_up,
        expert_down,
        shared_gate,
        shared_up,
        shared_down,
    )
    rows, width = residual.shape
    n_sp, n_tp = lax.axis_size("sp"), lax.axis_size("tp")
    capacity = 2 * rows * routes.shape[1] // n_sp
    hidden = expert_gate.shape[2]
    if n_sp != 4 or n_tp != 4 or capacity < rows or rows != 2 * WINDOW or shared_gate.shape[1] != hidden:
        return shards(*arguments)
    cols = width // n_tp
    heads = queries.shape[1] // HEAD_DIM
    group = queries.shape[1] // keys.shape[1]
    kv_width = keys.shape[1]
    blocks = rows // WINDOW
    bf16, f32 = jnp.bfloat16, jnp.float32
    vmem = pl.BlockSpec(memory_space=pltpu.VMEM)
    anywhere = pl.BlockSpec(memory_space=pl.ANY)
    dma = pltpu.SemaphoreType.DMA
    piece = rows // PARTS
    return pl.pallas_call(
        functools.partial(fused_kernel, (rows, cols, width, WINDOW, hidden, heads, group)),
        out_shape=pltpu.VMEM((rows, cols), bf16),
        in_specs=[anywhere] * 16,
        out_specs=vmem,
        scratch_shapes=[
            pltpu.VMEM(queries.shape, bf16),
            pltpu.VMEM(keys.shape, bf16),
            pltpu.VMEM(values.shape, bf16),
            pltpu.VMEM((1, rows), jnp.int32),
            pltpu.VMEM(routes.shape[::-1], jnp.int32),
            pltpu.VMEM(routes.shape[::-1], f32),
            pltpu.SMEM(sinks.shape, f32),
            pltpu.VMEM((1, width), f32),
            pltpu.VMEM((rows, cols), bf16),
            pltpu.VMEM(out_weight.shape, bf16),
            pltpu.VMEM((width, 2 * hidden), bf16),
            pltpu.VMEM((width, 2 * hidden), bf16),
            pltpu.VMEM(expert_down.shape[1:], bf16),
            pltpu.VMEM(shared_down.shape, bf16),
            pltpu.VMEM((WINDOW, kv_width), bf16),
            pltpu.VMEM((WINDOW, kv_width), bf16),
            pltpu.VMEM((8, WINDOW), f32),
            pltpu.VMEM((8, rows), f32),
            pltpu.VMEM((8, WINDOW), f32),
            pltpu.VMEM((4, 8, rows), f32),
            pltpu.VMEM((rows, heads * HEAD_DIM), bf16),
            pltpu.VMEM((blocks, 2, WINDOW, cols), bf16),
            pltpu.VMEM((blocks, 2, WINDOW, cols), bf16),
            pltpu.VMEM((PARTS, piece, cols), bf16),
            pltpu.VMEM((PARTS, piece, cols), bf16),
            pltpu.VMEM((rows, cols), f32),
            pltpu.VMEM((4, 4, rows, cols), bf16),
            pltpu.VMEM((rows, width), bf16),
            pltpu.VMEM((rows, width), bf16),
            pltpu.VMEM((5, 4, rows, hidden), bf16),
            pltpu.VMEM((4, rows, cols), f32),
            pltpu.VMEM((4, rows, cols), bf16),
            pltpu.VMEM((5, rows, cols), bf16),
            pltpu.VMEM((rows, cols), f32),
            dma((11,)),
            dma((4,)),
            dma((3,)),
            dma((4,)),
            dma((blocks, 2)),
            dma((4, 2, PARTS)),
            dma((4, blocks)),
            dma((5, 2, blocks)),
            dma((4, PARTS)),
        ],
        compiler_params=pltpu.CompilerParams(collective_id=0, has_side_effects=True),
    )(
        residual,
        queries,
        keys,
        values,
        segments[None, :],
        routes.T,
        route_weight.T,
        sinks,
        out_weight,
        norm_gain[None, :],
        expert_gate,
        expert_up,
        expert_down,
        shared_gate,
        shared_up,
        shared_down,
    )


def solution(mesh):
    placed = (
        P(("grp", "sp"), None),
        P(("grp", "sp"), "tp"),
        P(("grp", "sp"), "tp"),
        P(("grp", "sp"), "tp"),
        P(("grp", "sp")),
        P(("grp", "sp"), None),
        P(("grp", "sp"), None),
        P("tp"),
        P("tp", None),
        P(),
        P("sp", None, "tp"),
        P("sp", None, "tp"),
        P("sp", None, "tp"),
        P(None, "tp"),
        P(None, "tp"),
        P(None, "tp"),
    )
    return jax.shard_map(
        layer, mesh=mesh, in_specs=placed, out_specs=P(("grp", "sp"), "tp"), check_vma=False
    )
```
